32 devices in a mesh: sp: 8 (over z, y), tp: 4 (over x, core).
Axes of the slice: x: 2, y: 2, z: 4, core: 2. Of those that a mesh axis runs over, the one named last changes fastest.
Arguments:
- tokens: bfloat16 [4096, 2048], P(('sp', 'tp')), may hold values from -6 to 6
- pooling_input_weight: bfloat16 [2048, 1024], P('sp', 'tp'), may hold values from -0.125 to 0.125
- query_matrix: bfloat16 [2048, 512], P('sp', 'tp'), may hold values from -0.125 to 0.125
- key_matrix: bfloat16 [2048, 512], P('sp', 'tp'), may hold values from -0.125 to 0.125
- value_matrix: bfloat16 [2048, 1024], P('sp', 'tp'), may hold values from -0.125 to 0.125
- decay_inner_weight: bfloat16 [2048, 64], replicated, may hold values from -0.125 to 0.125
- decay_outer_weight: bfloat16 [2, 32, 512], replicated, may hold values from -1 to 1
- channel_decay_bias: float32 [2, 512], replicated, may hold values from -0.3 to 12
- spike_log_decay: float32 [8, 4096], P('tp', 'sp'), may hold values from -0.72 to 0
- starting_state: float32 [2, 8, 64, 128], P(None, 'tp'), may hold values from -96 to 96
- pooling_group_map: bfloat16 [4, 256, 256], replicated, may hold values from -0.375 to 0.375
- pooling_output_weight: bfloat16 [1024, 2048], P('tp', 'sp'), may hold values from -0.125 to 0.125
- attention_output_weight: bfloat16 [1024, 2048], P('tp', 'sp'), may hold values from -0.125 to 0.125
Outputs:
- mixed: bfloat16 [4096, 2048], P(('sp', 'tp'))
The draws below stay inside these ranges and needn't reach their ends.
All inputs are finite; a program needn't handle non-finite values.
Results may differ from the reference program's by a relative error of at most 0.015.
Values may be sent and summed in bfloat16 or wider, within the bound.
A program may use at most 64 MiB of HBM per device.

```python
import math
import jax
import jax.numpy as jnp
from jax import lax

D = 2048
WINDOWS = 4
POOL_CH = 256
HEAD_COUNT = 8
KEY_CHANNELS = 64
DV = 128
RANK = 32
BLOCK = 64
TOKEN_COUNT = 4096
D_POOL = 1024
QK = 512
VW = 1024
N_SP = 8
N_TP = 4


def draw_tokens(key, part):
    noise_key, direction_key = jax.random.split(jax.random.fold_in(key, 37))
    noise = jax.random.normal(noise_key, (TOKEN_COUNT, D), jnp.float32)
    direction = jax.random.normal(direction_key, (D,), jnp.float32)
    ramp = -1.0 + 2.0 * jnp.arange(TOKEN_COUNT, dtype=jnp.float32) / jnp.float32(TOKEN_COUNT - 1)
    values = noise + 1.5 * ramp[:, None] * direction[None, :]
    return jnp.clip(values, -6.0, 6.0).astype(jnp.bfloat16)


def draw_channel_decay_bias(key, part):
    pick_key, jitter_key = jax.random.split(jax.random.fold_in(key, 11))
    chance = 0.5
    slower = jax.random.bernoulli(pick_key, chance, (2, HEAD_COUNT))
    slow_level = jnp.maximum(jnp.log(jnp.float32(TOKEN_COUNT) / 3.2), 3.0)
    jitter = jax.random.uniform(jitter_key, (2, HEAD_COUNT, KEY_CHANNELS), jnp.float32, -1.0, 1.0)
    levels = jnp.where(slower[:, :, None], slow_level, 0.7) + jitter
    return levels.reshape(2, HEAD_COUNT * KEY_CHANNELS).astype(jnp.float32)


def draw_spike_log_decay(key, part):
    factor_key, location_seed, depth_key = jax.random.split(jax.random.fold_in(key, 23), 3)
    low_factor = 0.5
    high_factor = 4.0
    block_count = TOKEN_COUNT // BLOCK
    factors = jnp.exp(jax.random.uniform(factor_key, (HEAD_COUNT, block_count), jnp.float32, math.log(low_factor), math.log(high_factor)))
    steady = -(0.2 / TOKEN_COUNT) * jnp.repeat(factors, BLOCK, axis=1)
    spike_locations = jax.random.randint(location_seed, (HEAD_COUNT, 2), 0, TOKEN_COUNT)
    spike_depth = jnp.log(jax.random.uniform(depth_key, (HEAD_COUNT, 2), jnp.float32, 0.5, 0.8))
    token_positions = jnp.arange(TOKEN_COUNT, dtype=jnp.int32)
    spike_events = token_positions[None, :, None] == spike_locations[:, None, :]
    abrupt_change = jnp.min(jnp.where(spike_events, spike_depth[:, None, :], 0.0), axis=2)
    return (steady + abrupt_change).astype(jnp.float32)


def level_of(key, dims, shards, smallest, largest):
    loudness, own = 1.0, jax.random.fold_in(key, 6)
    for dim, blocks in shards:
        draws = jnp.exp(jax.random.uniform(jax.random.fold_in(own, dim), (blocks,), jnp.float32, smallest / len(shards), largest / len(shards)))
        loudness = loudness * jnp.repeat(draws, dims[dim] // blocks).reshape([-1 if axis == dim else 1 for axis in range(len(dims))])
    return loudness


def scatter_about(rng, extent, scale, most, pieces=(), kind=jnp.bfloat16):
    result = scale * jax.random.normal(rng, extent, jnp.float32)
    if pieces:
        result = result * level_of(rng, extent, pieces, -0.22, 0.18)
    return jnp.clip(result, -most, most).astype(kind)


def setup_inputs(seed: int = 0) -> dict:
    keys = jax.random.split(jax.random.key(seed), 14)
    return {
        "tokens": draw_tokens(jax.random.fold_in(keys[13], 71), 0),
        "pooling_input_weight": scatter_about(keys[1], (D, D_POOL), D ** -0.5, 0.125, ((0, 8), (1, 4))),
        "query_matrix": scatter_about(keys[2], (D, QK), D ** -0.5, 0.125, ((0, 8), (1, 4))),
        "key_matrix": scatter_about(keys[3], (D, QK), D ** -0.5, 0.125, ((0, 8), (1, 4))),
        "value_matrix": scatter_about(keys[4], (D, VW), D ** -0.5, 0.125, ((0, 8), (1, 4))),
        "decay_inner_weight": scatter_about(keys[5], (D, 2 * RANK), D ** -0.5, 0.125),
        "decay_outer_weight": scatter_about(keys[6], (2, RANK, QK), RANK ** -0.5, 1.0),
        "channel_decay_bias": draw_channel_decay_bias(jax.random.fold_in(keys[13], 71), 0),
        "spike_log_decay": draw_spike_log_decay(jax.random.fold_in(keys[13], 71), 0),
        "starting_state": scatter_about(keys[9], (2, HEAD_COUNT, KEY_CHANNELS, DV), (2 * N_SP), 96.0, ((1, 4),), jnp.float32),
        "pooling_group_map": scatter_about(keys[10], (WINDOWS, POOL_CH, POOL_CH), POOL_CH ** -0.5, 0.375),
        "pooling_output_weight": scatter_about(keys[11], (D_POOL, D), (D_POOL + VW) ** -0.5, 0.125, ((0, 4), (1, 8))),
        "attention_output_weight": scatter_about(keys[12], (VW, D), (D_POOL + VW) ** -0.5, 0.125, ((0, 4), (1, 8))),
    }


eps_value = 1e-06
gate_norm_factor = 16.0
highest = lax.Precision.HIGHEST
rim_width = 8

def normalize(token_rows):
    floats = token_rows.astype(jnp.float32)
    scaled = floats * lax.rsqrt(lax.optimization_barrier(jnp.mean(floats * floats, axis=-1, keepdims=True)) + eps_value)
    return scaled.astype(jnp.bfloat16)

def project(normed, weight):
    return jnp.dot(normed, weight, preferred_element_type=jnp.float32).astype(jnp.bfloat16)

def pooling(pool_input, pooling_group_map):
    sequence_length = pool_input.shape[0]
    floats = pool_input.astype(jnp.float32)
    padded = jnp.pad(floats, ((rim_width, rim_width), (0, 0)))
    position = jnp.arange(sequence_length, dtype=jnp.int32)
    outputs = []
    for group_id in range(WINDOWS):
        window = 2 ** (group_id + 1)
        half_width = window // 2
        columns = padded[:, group_id * POOL_CH:(group_id + 1) * POOL_CH]
        window_sum = jnp.zeros((sequence_length, POOL_CH), jnp.float32)
        for offset in range(-half_width, window - half_width):
            window_sum = window_sum + columns[rim_width + offset:rim_width + offset + sequence_length]
        low_end = jnp.clip(position - half_width, 0, sequence_length - 1)
        high_end = jnp.clip(position - half_width + window - 1, 0, sequence_length - 1)
        counted = (high_end - low_end + 1).astype(jnp.float32)[:, None]
        own_values = floats[:, group_id * POOL_CH:(group_id + 1) * POOL_CH]
        pooled = (window_sum / counted - own_values).astype(jnp.bfloat16)
        outputs.append(jnp.dot(pooled, pooling_group_map[group_id], preferred_element_type=jnp.float32).astype(jnp.bfloat16))
    return jnp.concatenate(outputs, axis=1)

def within_blocks(queries, cumulative, key_rows, value_rows, lower):
    row_ids = lax.broadcasted_iota(jnp.int32, (BLOCK, BLOCK), 0)
    col_ids = lax.broadcasted_iota(jnp.int32, (BLOCK, BLOCK), 1)
    allowed = col_ids <= row_ids if lower else col_ids > row_ids
    scaled_q = queries * jnp.exp(cumulative)
    scaled_k = key_rows * jnp.exp(-cumulative)
    scores = jnp.einsum('hnid,hnjd->hnij', scaled_q, scaled_k, precision=highest)
    scores = jnp.where(allowed, scores, 0.0)
    return (scaled_q, jnp.einsum('hnij,hnjv->hniv', scores, value_rows, precision=highest))

def block_updates(key_rows, value_rows, cumulative, edge):
    weighted = key_rows * jnp.exp(edge[:, :, None, :] - cumulative)
    return jnp.einsum('hncd,hncv->hndv', weighted, value_rows, precision=highest)

def run_states(edge, updates, start_memory, backward):

    def advance(memory, element):
        decay_now, update_now = element
        return (jnp.exp(decay_now)[..., None] * memory + update_now, memory)
    _, before = lax.scan(advance, start_memory, (jnp.moveaxis(edge, 1, 0), jnp.moveaxis(updates, 1, 0)), reverse=backward)
    return before

def reference(tokens, pooling_input_weight, query_matrix, key_matrix, value_matrix, decay_inner_weight, decay_outer_weight, channel_decay_bias, spike_log_decay, starting_state, pooling_group_map, pooling_output_weight, attention_output_weight):
    normed = normalize(tokens)
    sequence_length = tokens.shape[0]
    blocks = sequence_length // BLOCK
    pool_output = pooling(project(normed, pooling_input_weight), pooling_group_map)

    def split_heads(token_level, width):
        return token_level.astype(jnp.float32).reshape(blocks, BLOCK, HEAD_COUNT, width).transpose(2, 0, 1, 3)
    queries = split_heads(project(normed, query_matrix), KEY_CHANNELS) * KEY_CHANNELS ** (-0.5)
    key_rows = split_heads(project(normed, key_matrix), KEY_CHANNELS)
    value_rows = split_heads(project(normed, value_matrix), DV)
    low_rank = project(normed, decay_inner_weight)
    spike_amounts = spike_log_decay.T[:, :, None]

    def log_decay(direction):
        preactivation = jnp.dot(low_rank[:, direction * RANK:(direction + 1) * RANK], decay_outer_weight[direction], preferred_element_type=jnp.float32) + channel_decay_bias[direction]
        token_level = (jax.nn.log_sigmoid(preactivation) / gate_norm_factor).reshape(sequence_length, HEAD_COUNT, KEY_CHANNELS) + spike_amounts
        return token_level.reshape(blocks, BLOCK, HEAD_COUNT, KEY_CHANNELS).transpose(2, 0, 1, 3)
    cum_fwd = jnp.cumsum(log_decay(0), axis=2)
    cum_bwd = jnp.flip(jnp.cumsum(jnp.flip(log_decay(1), 2), axis=2), 2)
    scaled_fwd, inner_fwd = within_blocks(queries, cum_fwd, key_rows, value_rows, True)
    scaled_bwd, inner_bwd = within_blocks(queries, cum_bwd, key_rows, value_rows, False)
    edge_fwd = cum_fwd[:, :, -1, :]
    edge_bwd = cum_bwd[:, :, 0, :]
    before_fwd = run_states(edge_fwd, block_updates(key_rows, value_rows, cum_fwd, edge_fwd), starting_state[0], False)
    before_bwd = run_states(edge_bwd, block_updates(key_rows, value_rows, cum_bwd, edge_bwd), starting_state[1], True)
    out_fwd = inner_fwd + jnp.einsum('hnid,nhdv->hniv', scaled_fwd, before_fwd, precision=highest)
    out_bwd = inner_bwd + jnp.einsum('hnid,nhdv->hniv', scaled_bwd, before_bwd, precision=highest)
    joined = out_fwd + out_bwd
    normal_scale = lax.rsqrt(lax.optimization_barrier(jnp.mean(joined * joined, axis=-1, keepdims=True)) + eps_value)
    attention_output = (joined * normal_scale).astype(jnp.bfloat16).transpose(1, 2, 0, 3).reshape(sequence_length, HEAD_COUNT * DV)
    pool_rows = D_POOL // N_TP
    attention_rows = VW // N_TP
    mixed = jnp.zeros((sequence_length, D), jnp.float32)
    for group_id in range(N_TP):
        part_one = jnp.dot(pool_output[:, group_id * pool_rows:(group_id + 1) * pool_rows], pooling_output_weight[group_id * pool_rows:(group_id + 1) * pool_rows], preferred_element_type=jnp.float32)
        part_two = jnp.dot(attention_output[:, group_id * attention_rows:(group_id + 1) * attention_rows], attention_output_weight[group_id * attention_rows:(group_id + 1) * attention_rows], preferred_element_type=jnp.float32)
        rounded = lax.optimization_barrier((part_one + part_two).astype(jnp.bfloat16))
        mixed = mixed + rounded.astype(jnp.float32)
    return mixed.astype(jnp.bfloat16)
```

```python
import functools

import jax
import jax.numpy as jnp
from jax import lax
from jax.experimental import pallas as pl
from jax.experimental.pallas import tpu as pltpu
from jax.sharding import PartitionSpec as P

KEY_CHANNELS = 64
DV = 128
RANK = 32
BLOCK = 64


eps_value = 1e-06
gate_norm_factor = 16.0
highest = lax.Precision.HIGHEST
rim_width = 8


def extended(value, sides, width):
    for axis, dim in sides:
        devices, length = (lax.axis_size(axis), value.shape[dim])
        up = [(i, (i + 1) % devices) for i in range(devices - 1)]
        down = [(j, i) for i, j in up]
        last = lax.slice_in_dim(value, length - width, length, axis=dim)
        leading = lax.slice_in_dim(value, 0, width, axis=dim)
        before = lax.ppermute(last, axis, up)
        after = lax.ppermute(leading, axis, down)
        value = jnp.concatenate([before, value, after], axis=dim)
    return value


def entering_2(value, axis, join, neutral, backward):
    count = lax.axis_size(axis)
    place = lax.axis_index(axis)
    ahead = count - 1 - place if backward else place
    gathered = jax.tree.map(
        lambda a, kind: lax.all_gather(a.astype(kind), axis),
        value,
        jax.tree.map(lambda a: jnp.bfloat16 if a.dtype == jnp.float32 else a.dtype, value),
    )
    state = jax.tree.map(lambda a, e: jnp.zeros_like(a) + jnp.asarray(e, a.dtype), value, neutral)

    def one(lap, state):
        source = count - 1 - lap if backward else lap
        return join(
            state,
            jax.tree.map(
                lambda a, own: lax.dynamic_index_in_dim(a, source, 0, False).astype(own.dtype),
                gathered,
                value,
            ),
        )

    return lax.fori_loop(0, ahead, one, state)


def normalize(token_rows):
    floats = token_rows.astype(jnp.float32)
    scaled = floats * lax.rsqrt(jnp.mean(floats * floats, axis=-1, keepdims=True) + eps_value)
    return scaled.astype(jnp.bfloat16)


def chain_combine(earlier, later):
    return (earlier[0] + later[0], jnp.exp(later[0])[..., None] * earlier[1] + later[1])


def local_chain(decays, updates, backward):

    def advance(carried, element):
        log_total, memory = carried
        decay_now, update_now = element
        return (
            (log_total + decay_now, jnp.exp(decay_now)[..., None] * memory + update_now),
            (log_total, memory),
        )

    begin = (jnp.zeros_like(decays[0]), jnp.zeros_like(updates[0]))
    return lax.scan(advance, begin, (decays, updates), reverse=backward)


def within_blocks(queries, cumulative, key_rows, value_rows, lower):
    row_ids = lax.broadcasted_iota(jnp.int32, (BLOCK, BLOCK), 0)
    col_ids = lax.broadcasted_iota(jnp.int32, (BLOCK, BLOCK), 1)
    allowed = col_ids <= row_ids if lower else col_ids > row_ids
    scaled_q = queries * jnp.exp(cumulative)
    scaled_k = key_rows * jnp.exp(-cumulative)
    scores = jnp.einsum("hnid,hnjd->hnij", scaled_q, scaled_k, precision=highest)
    scores = jnp.where(allowed, scores, 0.0)
    return (scaled_q, jnp.einsum("hnij,hnjv->hniv", scores, value_rows, precision=highest))


def block_updates(key_rows, value_rows, cumulative, edge):
    weighted = key_rows * jnp.exp(edge[:, :, None, :] - cumulative)
    return jnp.einsum("hncd,hncv->hndv", weighted, value_rows, precision=highest)


def carried_term(scaled_q, before, entering):
    log_before, memory_before = before
    block_memory = jnp.exp(log_before)[..., None] * entering[None] + memory_before
    return jnp.einsum("hnid,nhdv->hniv", scaled_q, block_memory, precision=highest)


def shards(
    tokens,
    pooling_input_weight,
    query_matrix,
    key_matrix,
    value_matrix,
    decay_inner_weight,
    decay_outer_weight,
    channel_decay_bias,
    spike_log_decay,
    starting_state,
    pooling_group_map,
    pooling_output_weight,
    attention_output_weight,
):
    sp_index = lax.axis_index("sp")
    tp_index = lax.axis_index("tp")
    normed = normalize(tokens)
    pool_cols = pooling_input_weight.shape[1]
    qk_cols = query_matrix.shape[1]
    value_cols = value_matrix.shape[1]
    local_weight = jnp.concatenate(
        [pooling_input_weight, query_matrix, key_matrix, value_matrix], axis=1
    )
    whole_weight = lax.all_gather(local_weight, "sp", axis=0, tiled=True)
    row_piece = lax.all_gather(normed, "tp", axis=0, tiled=True)
    main_part = jnp.dot(row_piece, whole_weight, preferred_element_type=jnp.float32).astype(
        jnp.bfloat16
    )
    rank_part = jnp.dot(row_piece, decay_inner_weight, preferred_element_type=jnp.float32).astype(
        jnp.bfloat16
    )
    projected = jnp.concatenate([main_part, rank_part], axis=1)
    sequence_length = projected.shape[0]
    blocks = sequence_length // BLOCK
    heads_here = qk_cols // KEY_CHANNELS
    pool_input = projected[:, :pool_cols]
    query_part = projected[:, pool_cols : pool_cols + qk_cols]
    key_part = projected[:, pool_cols + qk_cols : pool_cols + 2 * qk_cols]
    value_part = projected[:, pool_cols + 2 * qk_cols : pool_cols + 2 * qk_cols + value_cols]
    low_rank = projected[:, pool_cols + 2 * qk_cols + value_cols :]
    window = jnp.left_shift(jnp.int32(2), tp_index)
    half_width = window // 2
    padded = extended(pool_input, (("sp", 0),), rim_width)
    floats = padded.astype(jnp.float32)
    window_sum = jnp.zeros((sequence_length, pool_cols), jnp.float32)
    for offset in range(-rim_width, rim_width):
        inside = ((offset >= -half_width) & (offset < window - half_width)).astype(jnp.float32)
        window_sum = (
            window_sum + inside * floats[rim_width + offset : rim_width + offset + sequence_length]
        )
    seq_length = sequence_length * lax.axis_size("sp")
    position = sp_index * sequence_length + jnp.arange(sequence_length, dtype=jnp.int32)
    low_end = jnp.clip(position - half_width, 0, seq_length - 1)
    high_end = jnp.clip(position - half_width + window - 1, 0, seq_length - 1)
    counted = (high_end - low_end + 1).astype(jnp.float32)[:, None]
    pooled = (window_sum / counted - floats[rim_width : rim_width + sequence_length]).astype(
        jnp.bfloat16
    )
    mix_here = lax.dynamic_index_in_dim(pooling_group_map, tp_index, 0, keepdims=False)
    pool_output = jnp.dot(pooled, mix_here, preferred_element_type=jnp.float32).astype(jnp.bfloat16)

    def split_heads(token_level, width):
        return (
            token_level.astype(jnp.float32)
            .reshape(blocks, BLOCK, heads_here, width)
            .transpose(2, 0, 1, 3)
        )

    queries = split_heads(query_part, KEY_CHANNELS) * KEY_CHANNELS ** (-0.5)
    key_rows = split_heads(key_part, KEY_CHANNELS)
    value_rows = split_heads(value_part, DV)
    up_here = lax.dynamic_slice_in_dim(decay_outer_weight, tp_index * qk_cols, qk_cols, 2)
    bias_here = lax.dynamic_slice_in_dim(channel_decay_bias, tp_index * qk_cols, qk_cols, 1)
    spike_amounts = spike_log_decay.T[:, :, None]

    def log_decay(direction):
        preactivation = (
            jnp.dot(
                low_rank[:, direction * RANK : (direction + 1) * RANK],
                up_here[direction],
                preferred_element_type=jnp.float32,
            )
            + bias_here[direction]
        )
        token_level = (jax.nn.log_sigmoid(preactivation) / gate_norm_factor).reshape(
            sequence_length, heads_here, KEY_CHANNELS
        ) + spike_amounts
        return token_level.reshape(blocks, BLOCK, heads_here, KEY_CHANNELS).transpose(2, 0, 1, 3)

    cum_fwd = jnp.cumsum(log_decay(0), axis=2)
    cum_bwd = jnp.flip(jnp.cumsum(jnp.flip(log_decay(1), 2), axis=2), 2)
    scaled_fwd, inner_fwd = within_blocks(queries, cum_fwd, key_rows, value_rows, True)
    scaled_bwd, inner_bwd = within_blocks(queries, cum_bwd, key_rows, value_rows, False)
    edge_fwd = cum_fwd[:, :, -1, :]
    edge_bwd = cum_bwd[:, :, 0, :]
    updates_fwd = block_updates(key_rows, value_rows, cum_fwd, edge_fwd)
    updates_bwd = block_updates(key_rows, value_rows, cum_bwd, edge_bwd)
    total_fwd, before_fwd = local_chain(
        jnp.moveaxis(edge_fwd, 1, 0), jnp.moveaxis(updates_fwd, 1, 0), False
    )
    total_bwd, before_bwd = local_chain(
        jnp.moveaxis(edge_bwd, 1, 0), jnp.moveaxis(updates_bwd, 1, 0), True
    )
    neutral = (jnp.zeros_like(total_fwd[0]), jnp.zeros_like(total_fwd[1]))
    prefix_fwd = entering_2(total_fwd, "sp", chain_combine, neutral, False)
    prefix_bwd = entering_2(total_bwd, "sp", chain_combine, neutral, True)
    entering_fwd = jnp.exp(prefix_fwd[0])[..., None] * starting_state[0] + prefix_fwd[1]
    entering_bwd = jnp.exp(prefix_bwd[0])[..., None] * starting_state[1] + prefix_bwd[1]
    out_fwd = inner_fwd + carried_term(scaled_fwd, before_fwd, entering_fwd)
    out_bwd = inner_bwd + carried_term(scaled_bwd, before_bwd, entering_bwd)
    joined = out_fwd + out_bwd
    normal_scale = lax.rsqrt(jnp.mean(joined * joined, axis=-1, keepdims=True) + eps_value)
    attention_output = (
        (joined * normal_scale)
        .astype(jnp.bfloat16)
        .transpose(1, 2, 0, 3)
        .reshape(sequence_length, heads_here * DV)
    )
    whole_pool, whole_attention = (
        lax.all_gather(pooling_output_weight, "sp", axis=1, tiled=True),
        lax.all_gather(attention_output_weight, "sp", axis=1, tiled=True),
    )
    part_one = jnp.dot(pool_output, whole_pool, preferred_element_type=jnp.float32)
    part_two = jnp.dot(attention_output, whole_attention, preferred_element_type=jnp.float32)
    return lax.psum_scatter(
        (part_one + part_two).astype(jnp.bfloat16), "tp", scatter_dimension=0, tiled=True
    )


MESH = pl.DeviceIdType.MESH
CHUNKS = 4
TOK_CHUNKS = 4
RIM = 16
QKV, POOL, OUT = range(3)


def nt(a, b):
    return lax.dot_general(a, b, (((1,), (1,)), ((), ())), preferred_element_type=jnp.float32)


def tn(a, b):
    return lax.dot_general(a, b, (((0,), (0,)), ((), ())), preferred_element_type=jnp.float32)


def nn(a, b):
    return jnp.dot(a, b, preferred_element_type=jnp.float32)


def fused(
    n,
    tokens,
    w_pool,
    w_query,
    w_key,
    w_value,
    inner,
    outer,
    bias,
    spikes,
    start,
    group_map,
    w_pool_out,
    w_att_out,
    result,
    xraw,
    normed,
    wqkv,
    wpl,
    obuf,
    pbuf,
    qkv,
    ld,
    qbuf,
    upd,
    edges,
    before_b,
    acc,
    act,
    msg,
    inbox,
    gmap,
    sib_out,
    sib_in,
    x_part,
    x_out,
    x_in,
    own,
    local_sem,
    tok_send,
    tok_recv,
    ring_send,
    ring_recv,
    halo_send,
    halo_recv,
    st_send,
    st_recv,
    sib_send,
    sib_recv,
    x_send,
    x_recv,
):
    me = lax.axis_index("sp")
    tp = lax.axis_index("tp")
    m = tokens.shape[0]
    tps = normed.shape[0] // m
    seq = normed.shape[0]
    rows = w_pool.shape[0]
    pc, qc, vc = w_pool.shape[1], w_query.shape[1], w_value.shape[1]
    ocols = obuf.shape[2]
    blocks = seq // BLOCK
    half = n // 2
    f32, bf16 = jnp.float32, jnp.bfloat16

    odd = lax.rem(me, 2)
    pos = jnp.where(odd == 0, me // 2, n - 1 - me // 2)

    def at_pos(p):
        p = lax.rem(p + 2 * n, n)
        return jnp.where(p < half, 2 * p, 2 * (n - 1 - p) + 1)

    nexts = (at_pos(pos + 1), at_pos(pos - 1))
    origins = {k: at_pos(pos + k) for k in range(-half, half + 1)}

    sibling = tp + 1 - 2 * lax.rem(tp, 2)
    across = lax.rem(tp + 2, tps)
    across_sibling = lax.rem(sibling + 2, tps)

    locals_ = []

    def local(src, dst):
        copy = pltpu.make_async_copy(src, dst, local_sem.at[len(locals_)])
        copy.start()
        locals_.append(copy)
        return copy

    my_rows = pl.ds(pl.multiple_of(me * rows, rows), rows)
    my_tok = pl.ds(pl.multiple_of(tp * m, m), m)
    w_copies = [
        local(w_query, wqkv.at[my_rows, pl.ds(0, qc)]),
        local(w_key, wqkv.at[my_rows, pl.ds(qc, qc)]),
        local(w_value, wqkv.at[my_rows, pl.ds(2 * qc, vc)]),
    ]
    t_copy = local(tokens, xraw.at[my_tok])
    late_copies = [
        local(w_pool, wpl.at[my_rows]),
        local(w_pool_out, obuf.at[me, pl.ds(0, pc)]),
        local(w_att_out, obuf.at[me, pl.ds(pc, vc)]),
        local(group_map.at[tp], gmap),
    ]

    barrier = pltpu.get_barrier_semaphore()
    for d in range(1, n):
        pl.semaphore_signal(
            barrier, inc=1, device_id={"sp": lax.rem(me + d, n)}, device_id_type=MESH
        )
    for d in range(1, tps):
        pl.semaphore_signal(
            barrier, inc=1, device_id={"tp": lax.rem(tp + d, tps)}, device_id_type=MESH
        )
    pl.semaphore_wait(barrier, n - 1 + tps - 1)

    def hops_of(d, c):
        return half if (c < CHUNKS // 2) == (d == 0) else half - 1

    def ring_copy(group, d, c, s, landed):
        shift = s + 1 if landed else s
        origin = origins[-shift if d == 0 else shift]
        if group == OUT:
            step = (pc + vc) // CHUNKS
            part = obuf.at[origin, pl.ds(c * step, step)]
        else:
            step = rows // CHUNKS
            at = pl.ds(pl.multiple_of(origin * rows + c * step, step), step)
            part = wqkv.at[at] if group == QKV else wpl.at[at]
        return pltpu.make_async_remote_copy(
            src_ref=part,
            dst_ref=part,
            send_sem=ring_send.at[group, d, c, s],
            recv_sem=ring_recv.at[group, d, c, s],
            device_id={"sp": nexts[d]},
            device_id_type=MESH,
        )

    def ring_event(group, s, i):
        for d in range(2):
            c = i if d == 0 else (i + CHUNKS // 2) % CHUNKS
            hops = hops_of(d, c)
            if 0 < s <= hops:
                ring_copy(group, d, c, s - 1, True).wait_recv()
            if s < hops:
                ring_copy(group, d, c, s, False).start()

    order = event_order(half)
    done = 0

    def pump(count=1):
        nonlocal done
        for event in order[done : done + count]:
            ring_event(*event)
        done = min(done + count, len(order))

    def pump_to(event):
        pump(order.index(event) + 1 - done)

    def token_copy(kind, c=0):
        step = m // TOK_CHUNKS
        if kind == 0:
            slot, part, peer = 0, my_tok, sibling
        elif kind == 1:
            slot, peer = 1 + c, across
            part = pl.ds(pl.multiple_of(tp * m + c * step, step), step)
        else:
            slot, peer = 1 + TOK_CHUNKS + c, sibling
            part = pl.ds(pl.multiple_of(across * m + c * step, step), step)
        return pltpu.make_async_remote_copy(
            src_ref=xraw.at[part],
            dst_ref=xraw.at[part],
            send_sem=tok_send.at[slot],
            recv_sem=tok_recv.at[slot],
            device_id={"tp": peer},
            device_id_type=MESH,
        )

    def normalize_rows(source, c, count):
        piece = pl.ds(pl.multiple_of(source * m + c * count, count), count)
        floats = xraw[piece, :].astype(f32)
        scale = lax.rsqrt(jnp.mean(floats * floats, axis=-1, keepdims=True) + eps_value)
        normed[piece, :] = (floats * scale).astype(bf16)

    t_copy.wait()
    for c in range(TOK_CHUNKS):
        token_copy(1, c).start()
    token_copy(0).start()
    for copy in w_copies:
        copy.wait()
    pump(CHUNKS)
    for copy in late_copies:
        copy.wait()
    normalize_rows(tp, 0, m)
    token_copy(0).wait_recv()
    normalize_rows(sibling, 0, m)
    pump(1)
    for c in range(TOK_CHUNKS):
        token_copy(1, c).wait_recv()
        token_copy(2, c).start()
        normalize_rows(across, c, m // TOK_CHUNKS)
        if c > 0:
            token_copy(2, c - 1).wait_recv()
            normalize_rows(across_sibling, c - 1, m // TOK_CHUNKS)
        pump(2)
    token_copy(2, TOK_CHUNKS - 1).wait_recv()
    normalize_rows(across_sibling, TOK_CHUNKS - 1, m // TOK_CHUNKS)

    low = nt(normed[...], inner[...]).astype(bf16)
    cols = pl.ds(pl.multiple_of(tp * qc, qc), qc)
    lane2 = lax.broadcasted_iota(jnp.int32, (1, 2 * qc), 1)
    heads = spikes.shape[0]
    padded = jnp.concatenate([spikes[...], jnp.zeros((8 - heads, seq), f32)], axis=0)
    chosen = (
        lax.broadcasted_iota(jnp.int32, (8, qc), 1) // KEY_CHANNELS
        == lax.broadcasted_iota(jnp.int32, (8, qc), 0)
    ).astype(f32)
    spread = lax.dot_general(
        padded, chosen, (((0,), (0,)), ((), ())), precision=highest, preferred_element_type=f32
    )
    for direction in range(2):
        pre = nn(
            low[:, direction * RANK : (direction + 1) * RANK], outer[direction, :, cols]
        ) + bias[direction : direction + 1, cols]
        ld[:, direction * qc : (direction + 1) * qc] = (
            jnp.minimum(pre, 0.0) - jnp.log1p(jnp.exp(-jnp.abs(pre)))
        ) / gate_norm_factor + spread

    pump_to((QKV, half, CHUNKS // 2 - 1))
    qkv[...] = nn(normed[...], wqkv[...]).astype(bf16)
    pump(1)

    row_ids = lax.broadcasted_iota(jnp.int32, (BLOCK, BLOCK), 0)
    col_ids = lax.broadcasted_iota(jnp.int32, (BLOCK, BLOCK), 1)
    lower = (col_ids <= row_ids).astype(f32)
    upper = (col_ids >= row_ids).astype(f32)
    first = lax.broadcasted_iota(jnp.int32, (1, qc), 1) < KEY_CHANNELS
    k0 = first.astype(f32)
    k1 = 1.0 - k0
    first2 = lax.rem(lane2, qc) < KEY_CHANNELS
    v0 = (lax.broadcasted_iota(jnp.int32, (1, vc), 1) < DV).astype(f32)
    v1 = 1.0 - v0
    allowed = (
        lax.rem(lax.broadcasted_iota(jnp.int32, (BLOCK, qc), 1), BLOCK)
        <= lax.broadcasted_iota(jnp.int32, (BLOCK, qc), 0)
    )

    for b in range(blocks):
        at = pl.ds(b * BLOCK, BLOCK)
        cum_f = jnp.dot(lower, ld[at, :qc], precision=highest, preferred_element_type=f32)
        cum_b = jnp.dot(upper, ld[at, qc:], precision=highest, preferred_element_type=f32)
        q = qkv[at, :qc].astype(f32) * KEY_CHANNELS ** (-0.5)
        k = qkv[at, qc : 2 * qc].astype(f32)
        v = qkv[at, 2 * qc :]
        vf = v.astype(f32)
        qf = (q * jnp.exp(cum_f)).astype(bf16)
        qb = (q * jnp.exp(cum_b)).astype(bf16)
        kf = k * jnp.exp(-cum_f)
        kb = k * jnp.exp(-cum_b)
        edge_f = cum_f[BLOCK - 1 : BLOCK, :]
        edge_b = cum_b[0:1, :]
        weighted = jnp.concatenate(
            [k * jnp.exp(edge_f - cum_f), k * jnp.exp(edge_b - cum_b)], axis=1
        ).astype(bf16)
        qbuf[at, :qc] = qf
        qbuf[at, qc:] = qb
        edges[b : b + 1, :] = jnp.concatenate([edge_f, edge_b], axis=1)
        scores_f = nt(qf, jnp.concatenate([kf * k0, kf * k1], axis=0).astype(bf16))
        scores_b = nt(qb, jnp.concatenate([kb * k0, kb * k1], axis=0).astype(bf16))
        scores = jnp.where(allowed, scores_f, scores_b).astype(bf16)
        both = jnp.concatenate([vf * v0, vf * v1], axis=0).astype(bf16)
        acc[at, :] = nn(scores, both)
        full = tn(v, weighted)
        upd[b] = jnp.where(first2, full[:DV], full[DV:])
        if b % 4 == 3:
            pump(1)

    total_f = jnp.zeros((DV, qc), f32)
    total_b = jnp.zeros((DV, qc), f32)
    for b in range(blocks):
        total_f = jnp.exp(edges[b : b + 1, :qc]) * total_f + upd[b, :, :qc]
    for b in reversed(range(blocks)):
        total_b = jnp.exp(edges[b : b + 1, qc:]) * total_b + upd[b, :, qc:]
    logs = jnp.sum(edges[...], axis=0, keepdims=True)
    ids = lax.broadcasted_iota(jnp.int32, (RIM, qc), 0)
    for direction, total in ((0, total_f), (1, total_b)):
        msg[direction, pl.ds(0, DV), :] = total.astype(bf16)
        log = logs[:, direction * qc : (direction + 1) * qc]
        hi = log.astype(bf16).astype(f32)
        lo = log - hi
        msg[direction, pl.ds(DV, RIM), :] = jnp.where(
            ids == 0, hi, jnp.where(ids == 1, lo, 0.0)
        ).astype(bf16)

    def state_copy(d):
        peer = lax.rem(me + d, n)
        return pltpu.make_async_remote_copy(
            src_ref=msg.at[jnp.where(peer > me, 0, 1)],
            dst_ref=inbox.at[me],
            send_sem=st_send.at[d - 1],
            recv_sem=st_recv.at[d - 1],
            device_id={"sp": peer},
            device_id_type=MESH,
        )

    def state_landed(source):
        d = lax.rem(me - source + n, n)
        return pltpu.make_async_remote_copy(
            src_ref=msg.at[0],
            dst_ref=inbox.at[source],
            send_sem=st_send.at[d - 1],
            recv_sem=st_recv.at[d - 1],
            device_id={"sp": source},
            device_id_type=MESH,
        )

    for d in range(1, n):
        state_copy(d).start()

    pump_to((POOL, half, CHUNKS // 2 - 1))
    pbuf[pl.ds(RIM, seq), :] = nn(normed[...], wpl[...]).astype(bf16)

    def halo(side):
        src = pl.ds(seq, RIM) if side == 0 else pl.ds(RIM, RIM)
        dst = pl.ds(0, RIM) if side == 0 else pl.ds(RIM + seq, RIM)
        peer = jnp.minimum(me + 1, n - 1) if side == 0 else jnp.maximum(me - 1, 0)
        return pltpu.make_async_remote_copy(
            src_ref=pbuf.at[src],
            dst_ref=pbuf.at[dst],
            send_sem=halo_send.at[side],
            recv_sem=halo_recv.at[side],
            device_id={"sp": peer},
            device_id_type=MESH,
        )

    @pl.when(me < n - 1)
    def _():
        halo(0).start()

    @pl.when(me > 0)
    def _():
        halo(1).start()

    @pl.when(me == 0)
    def _():
        pbuf[pl.ds(0, RIM), :] = jnp.zeros((RIM, pc), bf16)

    @pl.when(me == n - 1)
    def _():
        pbuf[pl.ds(RIM + seq, RIM), :] = jnp.zeros((RIM, pc), bf16)

    pump(1)

    def join(source, state):
        state_landed(source).wait_recv()
        tail = inbox[source, pl.ds(DV, RIM), :].astype(f32)
        log = tail[0:1, :] + tail[1:2, :]
        return jnp.exp(log) * state + inbox[source, pl.ds(0, DV), :].astype(f32)

    state_f = lax.fori_loop(0, me, join, start[0].T)
    state_b = lax.fori_loop(0, n - 1 - me, lambda i, st: join(n - 1 - i, st), start[1].T)
    for b in reversed(range(blocks)):
        before_b[b] = state_b
        state_b = jnp.exp(edges[b : b + 1, qc:]) * state_b + upd[b, :, qc:]
    for b in range(blocks):
        at = pl.ds(b * BLOCK, BLOCK)
        back = before_b[b]
        memory = jnp.concatenate(
            [
                jnp.concatenate([state_f * k0, back * k0], axis=1),
                jnp.concatenate([state_f * k1, back * k1], axis=1),
            ],
            axis=0,
        ).astype(bf16)
        joined = acc[at, :] + nt(qbuf[at, :], memory)
        for h in range(vc // DV):
            o = joined[:, h * DV : (h + 1) * DV]
            scale = lax.rsqrt(jnp.mean(o * o, axis=-1, keepdims=True) + eps_value)
            act[at, pc + h * DV : pc + (h + 1) * DV] = (o * scale).astype(bf16)
        if b + 1 < blocks:
            state_f = jnp.exp(edges[b : b + 1, :qc]) * state_f + upd[b, :, :qc]
    pump(1)

    @pl.when(me > 0)
    def _():
        halo(0).wait_recv()

    @pl.when(me < n - 1)
    def _():
        halo(1).wait_recv()

    window = jnp.left_shift(jnp.int32(2), tp)
    half_width = window // 2
    tile = 2 * BLOCK
    offset = (
        lax.broadcasted_iota(jnp.int32, (tile, tile + 2 * RIM), 1)
        - RIM
        - lax.broadcasted_iota(jnp.int32, (tile, tile + 2 * RIM), 0)
    )
    band = ((offset >= -half_width) & (offset < window - half_width)).astype(f32).astype(bf16)
    seq_length = seq * n
    for b in range(seq // tile):
        sums = nn(band, pbuf[pl.ds(b * tile, tile + 2 * RIM), :])
        position = me * seq + b * tile + lax.broadcasted_iota(jnp.int32, (tile, 1), 0)
        low_end = jnp.clip(position - half_width, 0, seq_length - 1)
        high_end = jnp.clip(position - half_width + window - 1, 0, seq_length - 1)
        counted = (high_end - low_end + 1).astype(f32)
        pooled = (sums / counted - pbuf[pl.ds(RIM + b * tile, tile), :].astype(f32)).astype(bf16)
        act[pl.ds(b * tile, tile), :pc] = nn(pooled, gmap[...]).astype(bf16)

    block_at = [0]
    for k in range(1, half):
        block_at += [-k, k]
    block_at.append(half)

    def rows_of(dest):
        return pl.ds(pl.multiple_of(dest * m, m), m)

    def sib_copy(i):
        return pltpu.make_async_remote_copy(
            src_ref=sib_out.at[i],
            dst_ref=sib_in.at[i],
            send_sem=sib_send.at[i],
            recv_sem=sib_recv.at[i],
            device_id={"tp": sibling},
            device_id_type=MESH,
        )

    def x_copy(i):
        return pltpu.make_async_remote_copy(
            src_ref=x_out.at[i],
            dst_ref=x_in.at[i],
            send_sem=x_send.at[i],
            recv_sem=x_recv.at[i],
            device_id={"tp": across},
            device_id_type=MESH,
        )

    def produce(i):
        weights = obuf[origins[block_at[i]]]
        sib_out[i, pl.ds(0, m)] = nn(act[rows_of(across_sibling), :], weights).astype(bf16)
        sib_out[i, pl.ds(m, m)] = nn(act[rows_of(sibling), :], weights).astype(bf16)
        sib_copy(i).start()
        x_part[i] = nn(act[rows_of(across), :], weights)
        own[i] = nn(act[rows_of(tp), :], weights)

    def cross(i):
        sib_copy(i).wait_recv()
        x_out[i] = (x_part[i] + sib_in[i, pl.ds(0, m)].astype(f32)).astype(bf16)
        x_copy(i).start()

    def finish(i):
        x_copy(i).wait_recv()
        at = pl.ds(pl.multiple_of(origins[block_at[i]] * ocols, ocols), ocols)
        result[:, at] = (
            own[i] + sib_in[i, pl.ds(m, m)].astype(f32) + x_in[i].astype(f32)
        ).astype(bf16)

    produce(0)
    for s in range(1, half):
        pump_to((OUT, s, CHUNKS - 1))
        produce(2 * s - 1)
        cross(2 * s - 2)
        produce(2 * s)
        cross(2 * s - 1)
        if s > 1:
            finish(2 * s - 4)
            finish(2 * s - 3)
    pump(len(order))
    produce(n - 1)
    cross(n - 2)
    cross(n - 1)
    for i in range(n - 4, n):
        finish(i)

    token_copy(0).wait_send()
    for c in range(TOK_CHUNKS):
        token_copy(1, c).wait_send()
        token_copy(2, c).wait_send()
    for group in range(3):
        for d in range(2):
            for c in range(CHUNKS):
                for s in range(hops_of(d, c)):
                    ring_copy(group, d, c, s, False).wait_send()

    @pl.when(me < n - 1)
    def _():
        halo(0).wait_send()

    @pl.when(me > 0)
    def _():
        halo(1).wait_send()

    for d in range(1, n):
        state_copy(d).wait_send()
    for i in range(n):
        sib_copy(i).wait_send()
        x_copy(i).wait_send()


def event_order(half):
    lead, rest = range(CHUNKS // 2), range(CHUNKS // 2, CHUNKS)
    events = [(QKV, s, i) for s in range(half - 1) for i in range(CHUNKS)]
    events += [(QKV, half - 1, i) for i in lead]
    events += [(POOL, 0, i) for i in range(CHUNKS)]
    events += [(QKV, half - 1, i) for i in rest]
    events += [(QKV, half, i) for i in lead]
    events += [(OUT, 0, 0)]
    for s in range(1, half - 1):
        events += [(POOL, s, i) for i in range(CHUNKS)] + [(OUT, 0, s)] * (s < CHUNKS)
    events += [(POOL, half - 1, i) for i in lead]
    events += [(OUT, 0, i) for i in range(half - 1, CHUNKS)]
    events += [(POOL, half - 1, i) for i in rest]
    events += [(POOL, half, i) for i in lead]
    for s in range(1, half - 1):
        events += [(OUT, s, i) for i in range(CHUNKS)]
    events += [(OUT, half - 1, i) for i in range(CHUNKS)]
    events += [(OUT, half, i) for i in lead]
    return events


def one_kernel(
    n,
    tps,
    tokens,
    pooling_input_weight,
    query_matrix,
    key_matrix,
    value_matrix,
    decay_inner_weight,
    decay_outer_weight,
    channel_decay_bias,
    spike_log_decay,
    starting_state,
    pooling_group_map,
    pooling_output_weight,
    attention_output_weight,
):
    m, width = tokens.shape
    seq = m * tps
    pc, qc, vc = (a.shape[1] for a in (pooling_input_weight, query_matrix, value_matrix))
    ocols = pooling_output_weight.shape[1]
    blocks = seq // BLOCK
    f32, bf16 = jnp.float32, jnp.bfloat16
    vmem = pl.BlockSpec(memory_space=pltpu.VMEM)
    hbm = pl.BlockSpec(memory_space=pl.ANY)
    dma = pltpu.SemaphoreType.DMA
    return pl.pallas_call(
        functools.partial(fused, n),
        out_shape=jax.ShapeDtypeStruct((m, n * ocols), bf16),
        in_specs=[hbm] * 5 + [vmem] * 5 + [hbm] * 3,
        out_specs=vmem,
        scratch_shapes=[
            pltpu.VMEM((seq, width), bf16),
            pltpu.VMEM((seq, width), bf16),
            pltpu.VMEM((width, 2 * qc + vc), bf16),
            pltpu.VMEM((width, pc), bf16),
            pltpu.VMEM((n, pc + vc, ocols), bf16),
            pltpu.VMEM((seq + 2 * RIM, pc), bf16),
            pltpu.VMEM((seq, 2 * qc + vc), bf16),
            pltpu.VMEM((seq, 2 * qc), f32),
            pltpu.VMEM((seq, 2 * qc), bf16),
            pltpu.VMEM((blocks, DV, 2 * qc), f32),
            pltpu.VMEM((blocks, 2 * qc), f32),
            pltpu.VMEM((blocks, DV, qc), f32),
            pltpu.VMEM((seq, vc), f32),
            pltpu.VMEM((seq, pc + vc), bf16),
            pltpu.VMEM((2, DV + RIM, qc), bf16),
            pltpu.VMEM((n, DV + RIM, qc), bf16),
            pltpu.VMEM((pc, pc), bf16),
            pltpu.VMEM((n, 2 * m, ocols), bf16),
            pltpu.VMEM((n, 2 * m, ocols), bf16),
            pltpu.VMEM((n, m, ocols), f32),
            pltpu.VMEM((n, m, ocols), bf16),
            pltpu.VMEM((n, m, ocols), bf16),
            pltpu.VMEM((n, m, ocols), f32),
            dma((8,)),
            dma((1 + 2 * TOK_CHUNKS,)),
            dma((1 + 2 * TOK_CHUNKS,)),
            dma((3, 2, CHUNKS, n // 2)),
            dma((3, 2, CHUNKS, n // 2)),
            dma((2,)),
            dma((2,)),
            dma((n - 1,)),
            dma((n - 1,)),
            dma((n,)),
            dma((n,)),
            dma((n,)),
            dma((n,)),
        ],
        compiler_params=pltpu.CompilerParams(
            collective_id=0, has_side_effects=True, vmem_limit_bytes=60 * 2**20
        ),
    )(
        tokens,
        pooling_input_weight,
        query_matrix,
        key_matrix,
        value_matrix,
        decay_inner_weight.T,
        decay_outer_weight,
        channel_decay_bias,
        spike_log_decay,
        starting_state.reshape(2, qc, DV),
        pooling_group_map,
        pooling_output_weight,
        attention_output_weight,
    )


def solution(mesh):
    in_specs = (
        P(("sp", "tp"), None),
        P("sp", "tp"),
        P("sp", "tp"),
        P("sp", "tp"),
        P("sp", "tp"),
        P(),
        P(),
        P(),
        P("tp", "sp"),
        P(None, "tp", None, None),
        P(),
        P("tp", "sp"),
        P("tp", "sp"),
    )
    out_specs = P(("sp", "tp"), None)
    n, tps = mesh.shape["sp"], mesh.shape["tp"]
    fits = n % 4 == 0 and n <= 16 and tps == 4
    local = functools.partial(one_kernel, n, tps) if fits else shards
    return jax.shard_map(local, mesh=mesh, in_specs=in_specs, out_specs=out_specs, check_vma=False)
```

```python
import functools

import jax
import jax.numpy as jnp
from jax import lax
from jax.experimental import pallas as pl
from jax.experimental.pallas import tpu as pltpu
from jax.sharding import PartitionSpec as P

KEY_CHANNELS = 64
DV = 128
RANK = 32
BLOCK = 64


eps_value = 1e-06
gate_norm_factor = 16.0
highest = lax.Precision.HIGHEST
rim_width = 8


def extended(value, sides, width):
    for axis, dim in sides:
        devices, length = (lax.axis_size(axis), value.shape[dim])
        up = [(i, (i + 1) % devices) for i in range(devices - 1)]
        down = [(j, i) for i, j in up]
        last = lax.slice_in_dim(value, length - width, length, axis=dim)
        leading = lax.slice_in_dim(value, 0, width, axis=dim)
        before = lax.ppermute(last, axis, up)
        after = lax.ppermute(leading, axis, down)
        value = jnp.concatenate([before, value, after], axis=dim)
    return value


def entering_2(value, axis, join, neutral, backward):
    count = lax.axis_size(axis)
    place = lax.axis_index(axis)
    ahead = count - 1 - place if backward else place
    gathered = jax.tree.map(
        lambda a, kind: lax.all_gather(a.astype(kind), axis),
        value,
        jax.tree.map(lambda a: jnp.bfloat16 if a.dtype == jnp.float32 else a.dtype, value),
    )
    state = jax.tree.map(lambda a, e: jnp.zeros_like(a) + jnp.asarray(e, a.dtype), value, neutral)

    def one(lap, state):
        source = count - 1 - lap if backward else lap
        return join(
            state,
            jax.tree.map(
                lambda a, own: lax.dynamic_index_in_dim(a, source, 0, False).astype(own.dtype),
                gathered,
                value,
            ),
        )

    return lax.fori_loop(0, ahead, one, state)


def normalize(token_rows):
    floats = token_rows.astype(jnp.float32)
    scaled = floats * lax.rsqrt(jnp.mean(floats * floats, axis=-1, keepdims=True) + eps_value)
    return scaled.astype(jnp.bfloat16)


def chain_combine(earlier, later):
    return (earlier[0] + later[0], jnp.exp(later[0])[..., None] * earlier[1] + later[1])


def local_chain(decays, updates, backward):

    def advance(carried, element):
        log_total, memory = carried
        decay_now, update_now = element
        return (
            (log_total + decay_now, jnp.exp(decay_now)[..., None] * memory + update_now),
            (log_total, memory),
        )

    begin = (jnp.zeros_like(decays[0]), jnp.zeros_like(updates[0]))
    return lax.scan(advance, begin, (decays, updates), reverse=backward)


def within_blocks(queries, cumulative, key_rows, value_rows, lower):
    row_ids = lax.broadcasted_iota(jnp.int32, (BLOCK, BLOCK), 0)
    col_ids = lax.broadcasted_iota(jnp.int32, (BLOCK, BLOCK), 1)
    allowed = col_ids <= row_ids if lower else col_ids > row_ids
    scaled_q = queries * jnp.exp(cumulative)
    scaled_k = key_rows * jnp.exp(-cumulative)
    scores = jnp.einsum("hnid,hnjd->hnij", scaled_q, scaled_k, precision=highest)
    scores = jnp.where(allowed, scores, 0.0)
    return (scaled_q, jnp.einsum("hnij,hnjv->hniv", scores, value_rows, precision=highest))


def block_updates(key_rows, value_rows, cumulative, edge):
    weighted = key_rows * jnp.exp(edge[:, :, None, :] - cumulative)
    return jnp.einsum("hncd,hncv->hndv", weighted, value_rows, precision=highest)


def carried_term(scaled_q, before, entering):
    log_before, memory_before = before
    block_memory = jnp.exp(log_before)[..., None] * entering[None] + memory_before
    return jnp.einsum("hnid,nhdv->hniv", scaled_q, block_memory, precision=highest)


def shards(
    tokens,
    pooling_input_weight,
    query_matrix,
    key_matrix,
    value_matrix,
    decay_inner_weight,
    decay_outer_weight,
    channel_decay_bias,
    spike_log_decay,
    starting_state,
    pooling_group_map,
    pooling_output_weight,
    attention_output_weight,
):
    sp_index = lax.axis_index("sp")
    tp_index = lax.axis_index("tp")
    normed = normalize(tokens)
    pool_cols = pooling_input_weight.shape[1]
    qk_cols = query_matrix.shape[1]
    value_cols = value_matrix.shape[1]
    local_weight = jnp.concatenate(
        [pooling_input_weight, query_matrix, key_matrix, value_matrix], axis=1
    )
    whole_weight = lax.all_gather(local_weight, "sp", axis=0, tiled=True)
    row_piece = lax.all_gather(normed, "tp", axis=0, tiled=True)
    main_part = jnp.dot(row_piece, whole_weight, preferred_element_type=jnp.float32).astype(
        jnp.bfloat16
    )
    rank_part = jnp.dot(row_piece, decay_inner_weight, preferred_element_type=jnp.float32).astype(
        jnp.bfloat16
    )
    projected = jnp.concatenate([main_part, rank_part], axis=1)
    sequence_length = projected.shape[0]
    blocks = sequence_length // BLOCK
    heads_here = qk_cols // KEY_CHANNELS
    pool_input = projected[:, :pool_cols]
    query_part = projected[:, pool_cols : pool_cols + qk_cols]
    key_part = projected[:, pool_cols + qk_cols : pool_cols + 2 * qk_cols]
    value_part = projected[:, pool_cols + 2 * qk_cols : pool_cols + 2 * qk_cols + value_cols]
    low_rank = projected[:, pool_cols + 2 * qk_cols + value_cols :]
    window = jnp.left_shift(jnp.int32(2), tp_index)
    half_width = window // 2
    padded = extended(pool_input, (("sp", 0),), rim_width)
    floats = padded.astype(jnp.float32)
    window_sum = jnp.zeros((sequence_length, pool_cols), jnp.float32)
    for offset in range(-rim_width, rim_width):
        inside = ((offset >= -half_width) & (offset < window - half_width)).astype(jnp.float32)
        window_sum = (
            window_sum + inside * floats[rim_width + offset : rim_width + offset + sequence_length]
        )
    seq_length = sequence_length * lax.axis_size("sp")
    position = sp_index * sequence_length + jnp.arange(sequence_length, dtype=jnp.int32)
    low_end = jnp.clip(position - half_width, 0, seq_length - 1)
    high_end = jnp.clip(position - half_width + window - 1, 0, seq_length - 1)
    counted = (high_end - low_end + 1).astype(jnp.float32)[:, None]
    pooled = (window_sum / counted - floats[rim_width : rim_width + sequence_length]).astype(
        jnp.bfloat16
    )
    mix_here = lax.dynamic_index_in_dim(pooling_group_map, tp_index, 0, keepdims=False)
    pool_output = jnp.dot(pooled, mix_here, preferred_element_type=jnp.float32).astype(jnp.bfloat16)

    def split_heads(token_level, width):
        return (
            token_level.astype(jnp.float32)
            .reshape(blocks, BLOCK, heads_here, width)
            .transpose(2, 0, 1, 3)
        )

    queries = split_heads(query_part, KEY_CHANNELS) * KEY_CHANNELS ** (-0.5)
    key_rows = split_heads(key_part, KEY_CHANNELS)
    value_rows = split_heads(value_part, DV)
    up_here = lax.dynamic_slice_in_dim(decay_outer_weight, tp_index * qk_cols, qk_cols, 2)
    bias_here = lax.dynamic_slice_in_dim(channel_decay_bias, tp_index * qk_cols, qk_cols, 1)
    spike_amounts = spike_log_decay.T[:, :, None]

    def log_decay(direction):
        preactivation = (
            jnp.dot(
                low_rank[:, direction * RANK : (direction + 1) * RANK],
                up_here[direction],
                preferred_element_type=jnp.float32,
            )
            + bias_here[direction]
        )
        token_level = (jax.nn.log_sigmoid(preactivation) / gate_norm_factor).reshape(
            sequence_length, heads_here, KEY_CHANNELS
        ) + spike_amounts
        return token_level.reshape(blocks, BLOCK, heads_here, KEY_CHANNELS).transpose(2, 0, 1, 3)

    cum_fwd = jnp.cumsum(log_decay(0), axis=2)
    cum_bwd = jnp.flip(jnp.cumsum(jnp.flip(log_decay(1), 2), axis=2), 2)
    scaled_fwd, inner_fwd = within_blocks(queries, cum_fwd, key_rows, value_rows, True)
    scaled_bwd, inner_bwd = within_blocks(queries, cum_bwd, key_rows, value_rows, False)
    edge_fwd = cum_fwd[:, :, -1, :]
    edge_bwd = cum_bwd[:, :, 0, :]
    updates_fwd = block_updates(key_rows, value_rows, cum_fwd, edge_fwd)
    updates_bwd = block_updates(key_rows, value_rows, cum_bwd, edge_bwd)
    total_fwd, before_fwd = local_chain(
        jnp.moveaxis(edge_fwd, 1, 0), jnp.moveaxis(updates_fwd, 1, 0), False
    )
    total_bwd, before_bwd = local_chain(
        jnp.moveaxis(edge_bwd, 1, 0), jnp.moveaxis(updates_bwd, 1, 0), True
    )
    neutral = (jnp.zeros_like(total_fwd[0]), jnp.zeros_like(total_fwd[1]))
    prefix_fwd = entering_2(total_fwd, "sp", chain_combine, neutral, False)
    prefix_bwd = entering_2(total_bwd, "sp", chain_combine, neutral, True)
    entering_fwd = jnp.exp(prefix_fwd[0])[..., None] * starting_state[0] + prefix_fwd[1]
    entering_bwd = jnp.exp(prefix_bwd[0])[..., None] * starting_state[1] + prefix_bwd[1]
    out_fwd = inner_fwd + carried_term(scaled_fwd, before_fwd, entering_fwd)
    out_bwd = inner_bwd + carried_term(scaled_bwd, before_bwd, entering_bwd)
    joined = out_fwd + out_bwd
    normal_scale = lax.rsqrt(jnp.mean(joined * joined, axis=-1, keepdims=True) + eps_value)
    attention_output = (
        (joined * normal_scale)
        .astype(jnp.bfloat16)
        .transpose(1, 2, 0, 3)
        .reshape(sequence_length, heads_here * DV)
    )
    whole_pool, whole_attention = (
        lax.all_gather(pooling_output_weight, "sp", axis=1, tiled=True),
        lax.all_gather(attention_output_weight, "sp", axis=1, tiled=True),
    )
    part_one = jnp.dot(pool_output, whole_pool, preferred_element_type=jnp.float32)
    part_two = jnp.dot(attention_output, whole_attention, preferred_element_type=jnp.float32)
    return lax.psum_scatter(
        (part_one + part_two).astype(jnp.bfloat16), "tp", scatter_dimension=0, tiled=True
    )


MESH = pl.DeviceIdType.MESH
CHUNKS = 4
TOK_CHUNKS = 4
RIM = 16
QKV, POOL, OUT = range(3)
PUMPS = (3, 4)


def nt(a, b):
    return lax.dot_general(a, b, (((1,), (1,)), ((), ())), preferred_element_type=jnp.float32)


def tn(a, b):
    return lax.dot_general(a, b, (((0,), (0,)), ((), ())), preferred_element_type=jnp.float32)


def nn(a, b):
    return jnp.dot(a, b, preferred_element_type=jnp.float32)


def fused(
    n,
    tokens,
    w_pool,
    w_query,
    w_key,
    w_value,
    inner_in,
    outer_in,
    bias_in,
    spikes_in,
    start_in,
    group_map,
    w_pool_out,
    w_att_out,
    result,
    inner,
    outer,
    bias,
    spikes,
    start,
    xraw,
    normed,
    wqkv,
    wpl,
    obuf,
    pbuf,
    qkv,
    ld,
    qbuf,
    upd,
    edges,
    before_b,
    acc,
    act,
    total,
    pair_out,
    pair_in,
    msg,
    inbox,
    back_out,
    back_in,
    entry,
    gmap,
    sib_out,
    sib_in,
    x_part,
    x_out,
    x_in,
    own,
    local_sem,
    tok_send,
    tok_recv,
    ring_send,
    ring_recv,
    halo_send,
    halo_recv,
    pair_send,
    pair_recv,
    st_send,
    st_recv,
    sib_send,
    sib_recv,
    x_send,
    x_recv,
):
    me = lax.axis_index("sp")
    tp = lax.axis_index("tp")
    m = tokens.shape[0]
    tps = normed.shape[0] // m
    seq = normed.shape[0]
    rows = w_pool.shape[0]
    pc, qc, vc = w_pool.shape[1], w_query.shape[1], w_value.shape[1]
    ocols = obuf.shape[2]
    blocks = seq // BLOCK
    half = n // 2
    f32, bf16 = jnp.float32, jnp.bfloat16

    odd = lax.rem(me, 2)
    pos = jnp.where(odd == 0, me // 2, n - 1 - me // 2)

    def at_pos(p):
        p = lax.rem(p + 2 * n, n)
        return jnp.where(p < half, 2 * p, 2 * (n - 1 - p) + 1)

    nexts = (at_pos(pos + 1), at_pos(pos - 1))
    origins = {k: at_pos(pos + k) for k in range(-half, half + 1)}

    sibling = tp + 1 - 2 * lax.rem(tp, 2)
    across = lax.rem(tp + 2, tps)
    across_sibling = lax.rem(sibling + 2, tps)

    locals_ = []

    def local(src, dst):
        copy = pltpu.make_async_copy(src, dst, local_sem.at[len(locals_)])
        copy.start()
        locals_.append(copy)
        return copy

    barrier = pltpu.get_barrier_semaphore()
    for peer in nexts:
        pl.semaphore_signal(barrier, inc=1, device_id={"sp": peer}, device_id_type=MESH)
    for peer in (sibling, across):
        pl.semaphore_signal(barrier, inc=1, device_id={"tp": peer}, device_id_type=MESH)

    my_rows = pl.ds(pl.multiple_of(me * rows, rows), rows)
    my_tok = pl.ds(pl.multiple_of(tp * m, m), m)
    w_copies = [
        local(w_query, wqkv.at[my_rows, pl.ds(0, qc)]),
        local(w_key, wqkv.at[my_rows, pl.ds(qc, qc)]),
        local(w_value, wqkv.at[my_rows, pl.ds(2 * qc, vc)]),
    ]
    t_copy = local(tokens, xraw.at[my_tok])
    late_copies = [
        local(w_pool, wpl.at[my_rows]),
        local(w_pool_out, obuf.at[me, pl.ds(0, pc)]),
        local(w_att_out, obuf.at[me, pl.ds(pc, vc)]),
        local(group_map.at[tp], gmap),
        local(inner_in, inner),
        local(outer_in, outer),
        local(bias_in, bias),
        local(spikes_in, spikes),
        local(start_in, start),
    ]
    pl.semaphore_wait(barrier, 4)

    def hops_of(d, c):
        return half if (c < CHUNKS // 2) == (d == 0) else half - 1

    def ring_copy(group, d, c, s, landed):
        shift = s + 1 if landed else s
        origin = origins[-shift if d == 0 else shift]
        if group == OUT:
            step = (pc + vc) // CHUNKS
            part = obuf.at[origin, pl.ds(c * step, step)]
        else:
            step = rows // CHUNKS
            at = pl.ds(pl.multiple_of(origin * rows + c * step, step), step)
            part = wqkv.at[at] if group == QKV else wpl.at[at]
        return pltpu.make_async_remote_copy(
            src_ref=part,
            dst_ref=part,
            send_sem=ring_send.at[group, d, c, s],
            recv_sem=ring_recv.at[group, d, c, s],
            device_id={"sp": nexts[d]},
            device_id_type=MESH,
        )

    def ring_event(group, s, i):
        for d in range(2):
            c = i if d == 0 else (i + CHUNKS // 2) % CHUNKS
            hops = hops_of(d, c)
            if 0 < s <= hops:
                ring_copy(group, d, c, s - 1, True).wait_recv()
            if s < hops:
                ring_copy(group, d, c, s, False).start()

    order = event_order(half)
    done = 0

    def pump(count=1):
        nonlocal done
        for event in order[done : done + count]:
            ring_event(*event)
        done = min(done + count, len(order))

    def pump_to(event):
        pump(order.index(event) + 1 - done)

    def token_copy(kind, c=0):
        step = m // TOK_CHUNKS
        if kind == 0:
            slot, part, peer = 0, my_tok, sibling
        elif kind == 1:
            slot, peer = 1 + c, across
            part = pl.ds(pl.multiple_of(tp * m + c * step, step), step)
        else:
            slot, peer = 1 + TOK_CHUNKS + c, sibling
            part = pl.ds(pl.multiple_of(across * m + c * step, step), step)
        return pltpu.make_async_remote_copy(
            src_ref=xraw.at[part],
            dst_ref=xraw.at[part],
            send_sem=tok_send.at[slot],
            recv_sem=tok_recv.at[slot],
            device_id={"tp": peer},
            device_id_type=MESH,
        )

    def normalize_rows(source, c, count):
        piece = pl.ds(pl.multiple_of(source * m + c * count, count), count)
        floats = xraw[piece, :].astype(f32)
        scale = lax.rsqrt(jnp.mean(floats * floats, axis=-1, keepdims=True) + eps_value)
        normed[piece, :] = (floats * scale).astype(bf16)

    t_copy.wait()
    for c in range(TOK_CHUNKS):
        token_copy(1, c).start()
    token_copy(0).start()
    for copy in w_copies:
        copy.wait()
    pump(CHUNKS)
    for copy in late_copies:
        copy.wait()
    normalize_rows(tp, 0, m)
    token_copy(0).wait_recv()
    normalize_rows(sibling, 0, m)
    pump(1)
    for c in range(TOK_CHUNKS):
        token_copy(1, c).wait_recv()
        token_copy(2, c).start()
        normalize_rows(across, c, m // TOK_CHUNKS)
        if c > 0:
            token_copy(2, c - 1).wait_recv()
            normalize_rows(across_sibling, c - 1, m // TOK_CHUNKS)
        pump(2)
    token_copy(2, TOK_CHUNKS - 1).wait_recv()
    normalize_rows(across_sibling, TOK_CHUNKS - 1, m // TOK_CHUNKS)

    low = nt(normed[...], inner[...]).astype(bf16)
    cols = pl.ds(pl.multiple_of(tp * qc, qc), qc)
    lane2 = lax.broadcasted_iota(jnp.int32, (1, 2 * qc), 1)
    heads = spikes.shape[0]
    padded = jnp.concatenate([spikes[...], jnp.zeros((8 - heads, seq), f32)], axis=0)
    chosen = (
        lax.broadcasted_iota(jnp.int32, (8, qc), 1) // KEY_CHANNELS
        == lax.broadcasted_iota(jnp.int32, (8, qc), 0)
    ).astype(f32)
    spread = lax.dot_general(
        padded, chosen, (((0,), (0,)), ((), ())), precision=highest, preferred_element_type=f32
    )
    for direction in range(2):
        pre = nn(
            low[:, direction * RANK : (direction + 1) * RANK], outer[direction, :, cols]
        ) + bias[direction : direction + 1, cols]
        ld[:, direction * qc : (direction + 1) * qc] = (
            jnp.minimum(pre, 0.0) - jnp.log1p(jnp.exp(-jnp.abs(pre)))
        ) / gate_norm_factor + spread

    pump_to((QKV, half, CHUNKS // 2 - 1))
    qkv[...] = nn(normed[...], wqkv[...]).astype(bf16)
    pump(1)

    row_ids = lax.broadcasted_iota(jnp.int32, (BLOCK, BLOCK), 0)
    col_ids = lax.broadcasted_iota(jnp.int32, (BLOCK, BLOCK), 1)
    lower = (col_ids <= row_ids).astype(f32)
    upper = (col_ids >= row_ids).astype(f32)
    first = lax.broadcasted_iota(jnp.int32, (1, qc), 1) < KEY_CHANNELS
    k0 = first.astype(f32)
    k1 = 1.0 - k0
    first2 = lax.rem(lane2, qc) < KEY_CHANNELS
    v0 = (lax.broadcasted_iota(jnp.int32, (1, vc), 1) < DV).astype(f32)
    v1 = 1.0 - v0
    allowed = (
        lax.rem(lax.broadcasted_iota(jnp.int32, (BLOCK, qc), 1), BLOCK)
        <= lax.broadcasted_iota(jnp.int32, (BLOCK, qc), 0)
    )

    for b in range(blocks):
        at = pl.ds(b * BLOCK, BLOCK)
        cum_f = jnp.dot(lower, ld[at, :qc], precision=highest, preferred_element_type=f32)
        cum_b = jnp.dot(upper, ld[at, qc:], precision=highest, preferred_element_type=f32)
        q = qkv[at, :qc].astype(f32) * KEY_CHANNELS ** (-0.5)
        k = qkv[at, qc : 2 * qc].astype(f32)
        v = qkv[at, 2 * qc :]
        vf = v.astype(f32)
        qf = (q * jnp.exp(cum_f)).astype(bf16)
        qb = (q * jnp.exp(cum_b)).astype(bf16)
        kf = k * jnp.exp(-cum_f)
        kb = k * jnp.exp(-cum_b)
        edge_f = cum_f[BLOCK - 1 : BLOCK, :]
        edge_b = cum_b[0:1, :]
        weighted = jnp.concatenate(
            [k * jnp.exp(edge_f - cum_f), k * jnp.exp(edge_b - cum_b)], axis=1
        ).astype(bf16)
        qbuf[at, :qc] = qf
        qbuf[at, qc:] = qb
        edges[b : b + 1, :] = jnp.concatenate([edge_f, edge_b], axis=1)
        scores_f = nt(qf, jnp.concatenate([kf * k0, kf * k1], axis=0).astype(bf16))
        scores_b = nt(qb, jnp.concatenate([kb * k0, kb * k1], axis=0).astype(bf16))
        scores = jnp.where(allowed, scores_f, scores_b).astype(bf16)
        both = jnp.concatenate([vf * v0, vf * v1], axis=0).astype(bf16)
        acc[at, :] = nn(scores, both)
        full = tn(v, weighted)
        upd[b] = jnp.where(first2, full[:DV], full[DV:])
        if b % 4 == 3:
            pump(1)

    total_f = jnp.zeros((DV, qc), f32)
    total_b = jnp.zeros((DV, qc), f32)
    for b in range(blocks):
        total_f = jnp.exp(edges[b : b + 1, :qc]) * total_f + upd[b, :, :qc]
    for b in reversed(range(blocks)):
        total_b = jnp.exp(edges[b : b + 1, qc:]) * total_b + upd[b, :, qc:]
    logs = jnp.sum(edges[...], axis=0, keepdims=True)
    log_f, log_b = logs[:, :qc], logs[:, qc:]
    total[0] = total_f
    total[1] = total_b
    plane, planes = me // 2, n // 2
    hd = DV // 2
    my_half = pl.ds(pl.multiple_of(odd * hd, hd), hd)
    other_half = pl.ds(pl.multiple_of((1 - odd) * hd, hd), hd)
    ids = lax.broadcasted_iota(jnp.int32, (RIM, qc), 0)

    def packed(*values):
        filled = jnp.zeros((RIM, qc), f32)
        for i, value in enumerate(values):
            hi = value.astype(bf16).astype(f32)
            filled = jnp.where(ids == 2 * i, hi, jnp.where(ids == 2 * i + 1, value - hi, filled))
        return filled.astype(bf16)

    pair_out[pl.ds(0, hd), :] = total[0, other_half, :].astype(bf16)
    pair_out[pl.ds(hd, hd), :] = total[1, other_half, :].astype(bf16)
    pair_out[pl.ds(2 * hd, RIM), :] = packed(log_f, log_b)

    def pair_copy(i):
        return pltpu.make_async_remote_copy(
            src_ref=(pair_out, back_out)[i],
            dst_ref=(pair_in, back_in)[i],
            send_sem=pair_send.at[i],
            recv_sem=pair_recv.at[i],
            device_id={"sp": me + 1 - 2 * odd},
            device_id_type=MESH,
        )

    def state_copy(d):
        peer = lax.rem(plane + d, planes)
        return pltpu.make_async_remote_copy(
            src_ref=msg.at[jnp.where(peer > plane, 0, 1)],
            dst_ref=inbox.at[plane],
            send_sem=st_send.at[d - 1],
            recv_sem=st_recv.at[d - 1],
            device_id={"sp": 2 * peer + odd},
            device_id_type=MESH,
        )

    def state_landed(source):
        d = lax.rem(plane - source + planes, planes)
        return pltpu.make_async_remote_copy(
            src_ref=msg.at[0],
            dst_ref=inbox.at[source],
            send_sem=st_send.at[d - 1],
            recv_sem=st_recv.at[d - 1],
            device_id={"sp": 2 * source + odd},
            device_id_type=MESH,
        )

    pair_copy(0).start()
    pump(PUMPS[0])
    pair_copy(0).wait_recv()
    even = odd == 0
    theirs_f = pair_in[pl.ds(0, hd), :].astype(f32)
    theirs_b = pair_in[pl.ds(hd, hd), :].astype(f32)
    tail = pair_in[pl.ds(2 * hd, RIM), :].astype(f32)
    peer_log_f, peer_log_b = tail[0:1] + tail[1:2], tail[2:3] + tail[3:4]
    mine_f, mine_b = total[0, my_half, :], total[1, my_half, :]
    late_f = jnp.exp(jnp.where(even, peer_log_f, log_f))
    late_b = jnp.exp(jnp.where(even, log_b, peer_log_b))
    msg[0, pl.ds(0, hd), :] = (
        late_f * jnp.where(even, mine_f, theirs_f) + jnp.where(even, theirs_f, mine_f)
    ).astype(bf16)
    msg[1, pl.ds(0, hd), :] = (
        late_b * jnp.where(even, theirs_b, mine_b) + jnp.where(even, mine_b, theirs_b)
    ).astype(bf16)
    msg[0, pl.ds(hd, RIM), :] = packed(log_f + peer_log_f)
    msg[1, pl.ds(hd, RIM), :] = packed(log_b + peer_log_b)
    for d in range(1, planes):
        state_copy(d).start()
    pump(PUMPS[1])

    def join(source, state):
        state_landed(source).wait_recv()
        tail = inbox[source, pl.ds(hd, RIM), :].astype(f32)
        log = tail[0:1, :] + tail[1:2, :]
        return jnp.exp(log) * state + inbox[source, pl.ds(0, hd), :].astype(f32)

    entry[0] = start[0].T
    entry[1] = start[1].T
    plane_f = lax.fori_loop(0, plane, join, entry[0, my_half, :])
    plane_b = lax.fori_loop(
        0, planes - 1 - plane, lambda i, st: join(planes - 1 - i, st), entry[1, my_half, :]
    )
    after_mine_f = jnp.exp(log_f) * plane_f + mine_f
    after_theirs_f = jnp.exp(peer_log_f) * plane_f + theirs_f
    after_mine_b = jnp.exp(log_b) * plane_b + mine_b
    after_theirs_b = jnp.exp(peer_log_b) * plane_b + theirs_b
    back_out[pl.ds(0, hd), :] = jnp.where(even, after_mine_f, plane_f).astype(bf16)
    back_out[pl.ds(hd, hd), :] = jnp.where(even, plane_b, after_mine_b).astype(bf16)
    pair_copy(1).start()
    entry[0, my_half, :] = jnp.where(even, plane_f, after_theirs_f)
    entry[1, my_half, :] = jnp.where(even, after_theirs_b, plane_b)

    pump_to((POOL, half, CHUNKS // 2 - 1))
    pbuf[pl.ds(RIM, seq), :] = nn(normed[...], wpl[...]).astype(bf16)

    def halo(side):
        src = pl.ds(seq, RIM) if side == 0 else pl.ds(RIM, RIM)
        dst = pl.ds(0, RIM) if side == 0 else pl.ds(RIM + seq, RIM)
        peer = jnp.minimum(me + 1, n - 1) if side == 0 else jnp.maximum(me - 1, 0)
        return pltpu.make_async_remote_copy(
            src_ref=pbuf.at[src],
            dst_ref=pbuf.at[dst],
            send_sem=halo_send.at[side],
            recv_sem=halo_recv.at[side],
            device_id={"sp": peer},
            device_id_type=MESH,
        )

    @pl.when(me < n - 1)
    def _():
        halo(0).start()

    @pl.when(me > 0)
    def _():
        halo(1).start()

    @pl.when(me == 0)
    def _():
        pbuf[pl.ds(0, RIM), :] = jnp.zeros((RIM, pc), bf16)

    @pl.when(me == n - 1)
    def _():
        pbuf[pl.ds(RIM + seq, RIM), :] = jnp.zeros((RIM, pc), bf16)

    pump(1)
    pair_copy(1).wait_recv()
    entry[0, other_half, :] = back_in[pl.ds(0, hd), :].astype(f32)
    entry[1, other_half, :] = back_in[pl.ds(hd, hd), :].astype(f32)
    state_f, state_b = entry[0], entry[1]
    for b in reversed(range(blocks)):
        before_b[b] = state_b
        state_b = jnp.exp(edges[b : b + 1, qc:]) * state_b + upd[b, :, qc:]
    for b in range(blocks):
        at = pl.ds(b * BLOCK, BLOCK)
        back = before_b[b]
        memory = jnp.concatenate(
            [
                jnp.concatenate([state_f * k0, back * k0], axis=1),
                jnp.concatenate([state_f * k1, back * k1], axis=1),
            ],
            axis=0,
        ).astype(bf16)
        joined = acc[at, :] + nt(qbuf[at, :], memory)
        for h in range(vc // DV):
            o = joined[:, h * DV : (h + 1) * DV]
            scale = lax.rsqrt(jnp.mean(o * o, axis=-1, keepdims=True) + eps_value)
            act[at, pc + h * DV : pc + (h + 1) * DV] = (o * scale).astype(bf16)
        if b + 1 < blocks:
            state_f = jnp.exp(edges[b : b + 1, :qc]) * state_f + upd[b, :, :qc]
    pump(1)

    @pl.when(me > 0)
    def _():
        halo(0).wait_recv()

    @pl.when(me < n - 1)
    def _():
        halo(1).wait_recv()

    window = jnp.left_shift(jnp.int32(2), tp)
    half_width = window // 2
    tile = 2 * BLOCK
    offset = (
        lax.broadcasted_iota(jnp.int32, (tile, tile + 2 * RIM), 1)
        - RIM
        - lax.broadcasted_iota(jnp.int32, (tile, tile + 2 * RIM), 0)
    )
    band = ((offset >= -half_width) & (offset < window - half_width)).astype(f32).astype(bf16)
    seq_length = seq * n
    for b in range(seq // tile):
        sums = nn(band, pbuf[pl.ds(b * tile, tile + 2 * RIM), :])
        position = me * seq + b * tile + lax.broadcasted_iota(jnp.int32, (tile, 1), 0)
        low_end = jnp.clip(position - half_width, 0, seq_length - 1)
        high_end = jnp.clip(position - half_width + window - 1, 0, seq_length - 1)
        counted = (high_end - low_end + 1).astype(f32)
        pooled = (sums / counted - pbuf[pl.ds(RIM + b * tile, tile), :].astype(f32)).astype(bf16)
        act[pl.ds(b * tile, tile), :pc] = nn(pooled, gmap[...]).astype(bf16)

    block_at = [0]
    for k in range(1, half):
        block_at += [-k, k]
    block_at.append(half)

    def rows_of(dest):
        return pl.ds(pl.multiple_of(dest * m, m), m)

    def sib_copy(i):
        return pltpu.make_async_remote_copy(
            src_ref=sib_out.at[i],
            dst_ref=sib_in.at[i],
            send_sem=sib_send.at[i],
            recv_sem=sib_recv.at[i],
            device_id={"tp": sibling},
            device_id_type=MESH,
        )

    def x_copy(i):
        return pltpu.make_async_remote_copy(
            src_ref=x_out.at[i],
            dst_ref=x_in.at[i],
            send_sem=x_send.at[i],
            recv_sem=x_recv.at[i],
            device_id={"tp": across},
            device_id_type=MESH,
        )

    def produce(i):
        weights = obuf[origins[block_at[i]]]
        sib_out[i, pl.ds(0, m)] = nn(act[rows_of(across_sibling), :], weights).astype(bf16)
        sib_out[i, pl.ds(m, m)] = nn(act[rows_of(sibling), :], weights).astype(bf16)
        sib_copy(i).start()
        x_part[i] = nn(act[rows_of(across), :], weights)
        own[i] = nn(act[rows_of(tp), :], weights)

    def cross(i):
        sib_copy(i).wait_recv()
        x_out[i] = (x_part[i] + sib_in[i, pl.ds(0, m)].astype(f32)).astype(bf16)
        x_copy(i).start()

    def finish(i):
        x_copy(i).wait_recv()
        at = pl.ds(pl.multiple_of(origins[block_at[i]] * ocols, ocols), ocols)
        result[:, at] = (
            own[i] + sib_in[i, pl.ds(m, m)].astype(f32) + x_in[i].astype(f32)
        ).astype(bf16)

    produce(0)
    for s in range(1, half):
        pump_to((OUT, s, CHUNKS - 1))
        produce(2 * s - 1)
        cross(2 * s - 2)
        produce(2 * s)
        cross(2 * s - 1)
        if s > 1:
            finish(2 * s - 4)
            finish(2 * s - 3)
    pump(len(order))
    produce(n - 1)
    cross(n - 2)
    cross(n - 1)
    for i in range(n - 4, n):
        finish(i)

    token_copy(0).wait_send()
    for c in range(TOK_CHUNKS):
        token_copy(1, c).wait_send()
        token_copy(2, c).wait_send()
    for group in range(3):
        for d in range(2):
            for c in range(CHUNKS):
                for s in range(hops_of(d, c)):
                    ring_copy(group, d, c, s, False).wait_send()

    @pl.when(me < n - 1)
    def _():
        halo(0).wait_send()

    @pl.when(me > 0)
    def _():
        halo(1).wait_send()

    for i in range(2):
        pair_copy(i).wait_send()
    for d in range(1, planes):
        state_copy(d).wait_send()
    for i in range(n):
        sib_copy(i).wait_send()
        x_copy(i).wait_send()


def event_order(half):
    lead, rest = range(CHUNKS // 2), range(CHUNKS // 2, CHUNKS)
    events = [(QKV, s, i) for s in range(half - 1) for i in range(CHUNKS)]
    events += [(QKV, half - 1, i) for i in lead]
    events += [(POOL, 0, i) for i in range(CHUNKS)]
    events += [(QKV, half - 1, i) for i in rest]
    events += [(QKV, half, i) for i in lead]
    events += [(OUT, 0, 0)]
    for s in range(1, half - 1):
        events += [(POOL, s, i) for i in range(CHUNKS)] + [(OUT, 0, s)] * (s < CHUNKS)
    events += [(POOL, half - 1, i) for i in lead]
    events += [(OUT, 0, i) for i in range(half - 1, CHUNKS)]
    events += [(POOL, half - 1, i) for i in rest]
    events += [(POOL, half, i) for i in lead]
    for s in range(1, half - 1):
        events += [(OUT, s, i) for i in range(CHUNKS)]
    events += [(OUT, half - 1, i) for i in range(CHUNKS)]
    events += [(OUT, half, i) for i in lead]
    return events


def one_kernel(
    n,
    tps,
    tokens,
    pooling_input_weight,
    query_matrix,
    key_matrix,
    value_matrix,
    decay_inner_weight,
    decay_outer_weight,
    channel_decay_bias,
    spike_log_decay,
    starting_state,
    pooling_group_map,
    pooling_output_weight,
    attention_output_weight,
):
    m, width = tokens.shape
    seq = m * tps
    pc, qc, vc = (a.shape[1] for a in (pooling_input_weight, query_matrix, value_matrix))
    ocols = pooling_output_weight.shape[1]
    blocks = seq // BLOCK
    f32, bf16 = jnp.float32, jnp.bfloat16
    vmem = pl.BlockSpec(memory_space=pltpu.VMEM)
    hbm = pl.BlockSpec(memory_space=pl.ANY)
    dma = pltpu.SemaphoreType.DMA
    return pl.pallas_call(
        functools.partial(fused, n),
        out_shape=pltpu.VMEM((m, n * ocols), bf16),
        in_specs=[hbm] * 13,
        out_specs=vmem,
        scratch_shapes=[
            pltpu.VMEM((decay_inner_weight.shape[1], width), bf16),
            pltpu.VMEM((2, RANK, decay_outer_weight.shape[2]), bf16),
            pltpu.VMEM(channel_decay_bias.shape, f32),
            pltpu.VMEM(spike_log_decay.shape, f32),
            pltpu.VMEM((2, qc, DV), f32),
            pltpu.VMEM((seq, width), bf16),
            pltpu.VMEM((seq, width), bf16),
            pltpu.VMEM((width, 2 * qc + vc), bf16),
            pltpu.VMEM((width, pc), bf16),
            pltpu.VMEM((n, pc + vc, ocols), bf16),
            pltpu.VMEM((seq + 2 * RIM, pc), bf16),
            pltpu.VMEM((seq, 2 * qc + vc), bf16),
            pltpu.VMEM((seq, 2 * qc), f32),
            pltpu.VMEM((seq, 2 * qc), bf16),
            pltpu.VMEM((blocks, DV, 2 * qc), f32),
            pltpu.VMEM((blocks, 2 * qc), f32),
            pltpu.VMEM((blocks, DV, qc), f32),
            pltpu.VMEM((seq, vc), f32),
            pltpu.VMEM((seq, pc + vc), bf16),
            pltpu.VMEM((2, DV, qc), f32),
            pltpu.VMEM((DV + RIM, qc), bf16),
            pltpu.VMEM((DV + RIM, qc), bf16),
            pltpu.VMEM((2, DV // 2 + RIM, qc), bf16),
            pltpu.VMEM((n // 2, DV // 2 + RIM, qc), bf16),
            pltpu.VMEM((DV, qc), bf16),
            pltpu.VMEM((DV, qc), bf16),
            pltpu.VMEM((2, DV, qc), f32),
            pltpu.VMEM((pc, pc), bf16),
            pltpu.VMEM((n, 2 * m, ocols), bf16),
            pltpu.VMEM((n, 2 * m, ocols), bf16),
            pltpu.VMEM((n, m, ocols), f32),
            pltpu.VMEM((n, m, ocols), bf16),
            pltpu.VMEM((n, m, ocols), bf16),
            pltpu.VMEM((n, m, ocols), f32),
            dma((13,)),
            dma((1 + 2 * TOK_CHUNKS,)),
            dma((1 + 2 * TOK_CHUNKS,)),
            dma((3, 2, CHUNKS, n // 2)),
            dma((3, 2, CHUNKS, n // 2)),
            dma((2,)),
            dma((2,)),
            dma((2,)),
            dma((2,)),
            dma((n // 2 - 1,)),
            dma((n // 2 - 1,)),
            dma((n,)),
            dma((n,)),
            dma((n,)),
            dma((n,)),
        ],
        compiler_params=pltpu.CompilerParams(
            collective_id=0, has_side_effects=True, vmem_limit_bytes=60 * 2**20
        ),
    )(
        tokens,
        pooling_input_weight,
        query_matrix,
        key_matrix,
        value_matrix,
        decay_inner_weight.T,
        decay_outer_weight,
        channel_decay_bias,
        spike_log_decay,
        starting_state.reshape(2, qc, DV),
        pooling_group_map,
        pooling_output_weight,
        attention_output_weight,
    )


def solution(mesh):
    in_specs = (
        P(("sp", "tp"), None),
        P("sp", "tp"),
        P("sp", "tp"),
        P("sp", "tp"),
        P("sp", "tp"),
        P(),
        P(),
        P(),
        P("tp", "sp"),
        P(None, "tp", None, None),
        P(),
        P("tp", "sp"),
        P("tp", "sp"),
    )
    out_specs = P(("sp", "tp"), None)
    n, tps = mesh.shape["sp"], mesh.shape["tp"]
    fits = n % 4 == 0 and n <= 16 and tps == 4
    local = functools.partial(one_kernel, n, tps) if fits else shards
    return jax.shard_map(local, mesh=mesh, in_specs=in_specs, out_specs=out_specs, check_vma=False)
```

```python
import functools

import jax
import jax.numpy as jnp
from jax import lax
from jax.experimental import pallas as pl
from jax.experimental.pallas import tpu as pltpu
from jax.sharding import PartitionSpec as P

KEY_CHANNELS = 64
DV = 128
RANK = 32
BLOCK = 64


eps_value = 1e-06
gate_norm_factor = 16.0
highest = lax.Precision.HIGHEST
rim_width = 8


def extended(value, sides, width):
    for axis, dim in sides:
        devices, length = (lax.axis_size(axis), value.shape[dim])
        up = [(i, (i + 1) % devices) for i in range(devices - 1)]
        down = [(j, i) for i, j in up]
        last = lax.slice_in_dim(value, length - width, length, axis=dim)
        leading = lax.slice_in_dim(value, 0, width, axis=dim)
        before = lax.ppermute(last, axis, up)
        after = lax.ppermute(leading, axis, down)
        value = jnp.concatenate([before, value, after], axis=dim)
    return value


def entering_2(value, axis, join, neutral, backward):
    count = lax.axis_size(axis)
    place = lax.axis_index(axis)
    ahead = count - 1 - place if backward else place
    gathered = jax.tree.map(
        lambda a, kind: lax.all_gather(a.astype(kind), axis),
        value,
        jax.tree.map(lambda a: jnp.bfloat16 if a.dtype == jnp.float32 else a.dtype, value),
    )
    state = jax.tree.map(lambda a, e: jnp.zeros_like(a) + jnp.asarray(e, a.dtype), value, neutral)

    def one(lap, state):
        source = count - 1 - lap if backward else lap
        return join(
            state,
            jax.tree.map(
                lambda a, own: lax.dynamic_index_in_dim(a, source, 0, False).astype(own.dtype),
                gathered,
                value,
            ),
        )

    return lax.fori_loop(0, ahead, one, state)


def normalize(token_rows):
    floats = token_rows.astype(jnp.float32)
    scaled = floats * lax.rsqrt(jnp.mean(floats * floats, axis=-1, keepdims=True) + eps_value)
    return scaled.astype(jnp.bfloat16)


def chain_combine(earlier, later):
    return (earlier[0] + later[0], jnp.exp(later[0])[..., None] * earlier[1] + later[1])


def local_chain(decays, updates, backward):

    def advance(carried, element):
        log_total, memory = carried
        decay_now, update_now = element
        return (
            (log_total + decay_now, jnp.exp(decay_now)[..., None] * memory + update_now),
            (log_total, memory),
        )

    begin = (jnp.zeros_like(decays[0]), jnp.zeros_like(updates[0]))
    return lax.scan(advance, begin, (decays, updates), reverse=backward)


def within_blocks(queries, cumulative, key_rows, value_rows, lower):
    row_ids = lax.broadcasted_iota(jnp.int32, (BLOCK, BLOCK), 0)
    col_ids = lax.broadcasted_iota(jnp.int32, (BLOCK, BLOCK), 1)
    allowed = col_ids <= row_ids if lower else col_ids > row_ids
    scaled_q = queries * jnp.exp(cumulative)
    scaled_k = key_rows * jnp.exp(-cumulative)
    scores = jnp.einsum("hnid,hnjd->hnij", scaled_q, scaled_k, precision=highest)
    scores = jnp.where(allowed, scores, 0.0)
    return (scaled_q, jnp.einsum("hnij,hnjv->hniv", scores, value_rows, precision=highest))


def block_updates(key_rows, value_rows, cumulative, edge):
    weighted = key_rows * jnp.exp(edge[:, :, None, :] - cumulative)
    return jnp.einsum("hncd,hncv->hndv", weighted, value_rows, precision=highest)


def carried_term(scaled_q, before, entering):
    log_before, memory_before = before
    block_memory = jnp.exp(log_before)[..., None] * entering[None] + memory_before
    return jnp.einsum("hnid,nhdv->hniv", scaled_q, block_memory, precision=highest)


def shards(
    tokens,
    pooling_input_weight,
    query_matrix,
    key_matrix,
    value_matrix,
    decay_inner_weight,
    decay_outer_weight,
    channel_decay_bias,
    spike_log_decay,
    starting_state,
    pooling_group_map,
    pooling_output_weight,
    attention_output_weight,
):
    sp_index = lax.axis_index("sp")
    tp_index = lax.axis_index("tp")
    normed = normalize(tokens)
    pool_cols = pooling_input_weight.shape[1]
    qk_cols = query_matrix.shape[1]
    value_cols = value_matrix.shape[1]
    local_weight = jnp.concatenate(
        [pooling_input_weight, query_matrix, key_matrix, value_matrix], axis=1
    )
    whole_weight = lax.all_gather(local_weight, "sp", axis=0, tiled=True)
    row_piece = lax.all_gather(normed, "tp", axis=0, tiled=True)
    main_part = jnp.dot(row_piece, whole_weight, preferred_element_type=jnp.float32).astype(
        jnp.bfloat16
    )
    rank_part = jnp.dot(row_piece, decay_inner_weight, preferred_element_type=jnp.float32).astype(
        jnp.bfloat16
    )
    projected = jnp.concatenate([main_part, rank_part], axis=1)
    sequence_length = projected.shape[0]
    blocks = sequence_length // BLOCK
    heads_here = qk_cols // KEY_CHANNELS
    pool_input = projected[:, :pool_cols]
    query_part = projected[:, pool_cols : pool_cols + qk_cols]
    key_part = projected[:, pool_cols + qk_cols : pool_cols + 2 * qk_cols]
    value_part = projected[:, pool_cols + 2 * qk_cols : pool_cols + 2 * qk_cols + value_cols]
    low_rank = projected[:, pool_cols + 2 * qk_cols + value_cols :]
    window = jnp.left_shift(jnp.int32(2), tp_index)
    half_width = window // 2
    padded = extended(pool_input, (("sp", 0),), rim_width)
    floats = padded.astype(jnp.float32)
    window_sum = jnp.zeros((sequence_length, pool_cols), jnp.float32)
    for offset in range(-rim_width, rim_width):
        inside = ((offset >= -half_width) & (offset < window - half_width)).astype(jnp.float32)
        window_sum = (
            window_sum + inside * floats[rim_width + offset : rim_width + offset + sequence_length]
        )
    seq_length = sequence_length * lax.axis_size("sp")
    position = sp_index * sequence_length + jnp.arange(sequence_length, dtype=jnp.int32)
    low_end = jnp.clip(position - half_width, 0, seq_length - 1)
    high_end = jnp.clip(position - half_width + window - 1, 0, seq_length - 1)
    counted = (high_end - low_end + 1).astype(jnp.float32)[:, None]
    pooled = (window_sum / counted - floats[rim_width : rim_width + sequence_length]).astype(
        jnp.bfloat16
    )
    mix_here = lax.dynamic_index_in_dim(pooling_group_map, tp_index, 0, keepdims=False)
    pool_output = jnp.dot(pooled, mix_here, preferred_element_type=jnp.float32).astype(jnp.bfloat16)

    def split_heads(token_level, width):
        return (
            token_level.astype(jnp.float32)
            .reshape(blocks, BLOCK, heads_here, width)
            .transpose(2, 0, 1, 3)
        )

    queries = split_heads(query_part, KEY_CHANNELS) * KEY_CHANNELS ** (-0.5)
    key_rows = split_heads(key_part, KEY_CHANNELS)
    value_rows = split_heads(value_part, DV)
    up_here = lax.dynamic_slice_in_dim(decay_outer_weight, tp_index * qk_cols, qk_cols, 2)
    bias_here = lax.dynamic_slice_in_dim(channel_decay_bias, tp_index * qk_cols, qk_cols, 1)
    spike_amounts = spike_log_decay.T[:, :, None]

    def log_decay(direction):
        preactivation = (
            jnp.dot(
                low_rank[:, direction * RANK : (direction + 1) * RANK],
                up_here[direction],
                preferred_element_type=jnp.float32,
            )
            + bias_here[direction]
        )
        token_level = (jax.nn.log_sigmoid(preactivation) / gate_norm_factor).reshape(
            sequence_length, heads_here, KEY_CHANNELS
        ) + spike_amounts
        return token_level.reshape(blocks, BLOCK, heads_here, KEY_CHANNELS).transpose(2, 0, 1, 3)

    cum_fwd = jnp.cumsum(log_decay(0), axis=2)
    cum_bwd = jnp.flip(jnp.cumsum(jnp.flip(log_decay(1), 2), axis=2), 2)
    scaled_fwd, inner_fwd = within_blocks(queries, cum_fwd, key_rows, value_rows, True)
    scaled_bwd, inner_bwd = within_blocks(queries, cum_bwd, key_rows, value_rows, False)
    edge_fwd = cum_fwd[:, :, -1, :]
    edge_bwd = cum_bwd[:, :, 0, :]
    updates_fwd = block_updates(key_rows, value_rows, cum_fwd, edge_fwd)
    updates_bwd = block_updates(key_rows, value_rows, cum_bwd, edge_bwd)
    total_fwd, before_fwd = local_chain(
        jnp.moveaxis(edge_fwd, 1, 0), jnp.moveaxis(updates_fwd, 1, 0), False
    )
    total_bwd, before_bwd = local_chain(
        jnp.moveaxis(edge_bwd, 1, 0), jnp.moveaxis(updates_bwd, 1, 0), True
    )
    neutral = (jnp.zeros_like(total_fwd[0]), jnp.zeros_like(total_fwd[1]))
    prefix_fwd = entering_2(total_fwd, "sp", chain_combine, neutral, False)
    prefix_bwd = entering_2(total_bwd, "sp", chain_combine, neutral, True)
    entering_fwd = jnp.exp(prefix_fwd[0])[..., None] * starting_state[0] + prefix_fwd[1]
    entering_bwd = jnp.exp(prefix_bwd[0])[..., None] * starting_state[1] + prefix_bwd[1]
    out_fwd = inner_fwd + carried_term(scaled_fwd, before_fwd, entering_fwd)
    out_bwd = inner_bwd + carried_term(scaled_bwd, before_bwd, entering_bwd)
    joined = out_fwd + out_bwd
    normal_scale = lax.rsqrt(jnp.mean(joined * joined, axis=-1, keepdims=True) + eps_value)
    attention_output = (
        (joined * normal_scale)
        .astype(jnp.bfloat16)
        .transpose(1, 2, 0, 3)
        .reshape(sequence_length, heads_here * DV)
    )
    whole_pool, whole_attention = (
        lax.all_gather(pooling_output_weight, "sp", axis=1, tiled=True),
        lax.all_gather(attention_output_weight, "sp", axis=1, tiled=True),
    )
    part_one = jnp.dot(pool_output, whole_pool, preferred_element_type=jnp.float32)
    part_two = jnp.dot(attention_output, whole_attention, preferred_element_type=jnp.float32)
    return lax.psum_scatter(
        (part_one + part_two).astype(jnp.bfloat16), "tp", scatter_dimension=0, tiled=True
    )


MESH = pl.DeviceIdType.MESH
CHUNKS = 4
TOK_CHUNKS = 8
RIM = 16
KV, QP, OUT = range(3)
PUMPS = (3, 7)


def nt(a, b):
    return lax.dot_general(a, b, (((1,), (1,)), ((), ())), preferred_element_type=jnp.float32)


def tn(a, b):
    return lax.dot_general(a, b, (((0,), (0,)), ((), ())), preferred_element_type=jnp.float32)


def nn(a, b):
    return jnp.dot(a, b, preferred_element_type=jnp.float32)


def fused(
    n,
    tokens,
    w_pool,
    w_query,
    w_key,
    w_value,
    inner_in,
    outer_in,
    bias_in,
    spikes_in,
    start_in,
    group_map,
    w_pool_out,
    w_att_out,
    result,
    inner,
    outer,
    bias,
    spikes,
    start,
    xraw,
    normed,
    wkv,
    wqp,
    obuf,
    pbuf,
    kv,
    ld,
    kbuf,
    upd,
    edges,
    before_b,
    act,
    total,
    pair_out,
    pair_in,
    msg,
    inbox,
    back_out,
    back_in,
    entry,
    gmap,
    sib_out,
    sib_in,
    x_part,
    x_out,
    x_in,
    own,
    local_sem,
    tok_send,
    tok_recv,
    ring_send,
    ring_recv,
    halo_send,
    halo_recv,
    pair_send,
    pair_recv,
    st_send,
    st_recv,
    sib_send,
    sib_recv,
    x_send,
    x_recv,
):
    me = lax.axis_index("sp")
    tp = lax.axis_index("tp")
    m = tokens.shape[0]
    tps = normed.shape[0] // m
    seq = normed.shape[0]
    rows = w_pool.shape[0]
    pc, qc, vc = w_pool.shape[1], w_query.shape[1], w_value.shape[1]
    ocols = obuf.shape[2]
    blocks = seq // BLOCK
    half = n // 2
    f32, bf16 = jnp.float32, jnp.bfloat16

    odd = lax.rem(me, 2)
    pos = jnp.where(odd == 0, me // 2, n - 1 - me // 2)

    def at_pos(p):
        p = lax.rem(p + 2 * n, n)
        return jnp.where(p < half, 2 * p, 2 * (n - 1 - p) + 1)

    nexts = (at_pos(pos + 1), at_pos(pos - 1))
    origins = {k: at_pos(pos + k) for k in range(-half, half + 1)}

    sibling = tp + 1 - 2 * lax.rem(tp, 2)
    across = lax.rem(tp + 2, tps)
    across_sibling = lax.rem(sibling + 2, tps)

    locals_ = []

    def local(src, dst):
        copy = pltpu.make_async_copy(src, dst, local_sem.at[len(locals_)])
        copy.start()
        locals_.append(copy)
        return copy

    barrier = pltpu.get_barrier_semaphore()
    for peer in nexts:
        pl.semaphore_signal(barrier, inc=1, device_id={"sp": peer}, device_id_type=MESH)
    for peer in (sibling, across):
        pl.semaphore_signal(barrier, inc=1, device_id={"tp": peer}, device_id_type=MESH)

    my_rows = pl.ds(pl.multiple_of(me * rows, rows), rows)
    my_tok = pl.ds(pl.multiple_of(tp * m, m), m)
    w_copies = [
        local(w_key, wkv.at[my_rows, pl.ds(0, qc)]),
        local(w_value, wkv.at[my_rows, pl.ds(qc, vc)]),
    ]
    t_copy = local(tokens, xraw.at[my_tok])
    late_copies = [
        local(w_query, wqp.at[my_rows, pl.ds(0, qc)]),
        local(w_pool, wqp.at[my_rows, pl.ds(qc, pc)]),
        local(w_pool_out, obuf.at[me, pl.ds(0, pc)]),
        local(w_att_out, obuf.at[me, pl.ds(pc, vc)]),
        local(group_map.at[tp], gmap),
        local(inner_in, inner),
        local(outer_in, outer),
        local(bias_in, bias),
        local(spikes_in, spikes),
        local(start_in, start),
    ]
    pl.semaphore_wait(barrier, 4)

    def hops_of(d, c):
        return half if (c < CHUNKS // 2) == (d == 0) else half - 1

    def ring_copy(group, d, c, s, landed):
        shift = s + 1 if landed else s
        origin = origins[-shift if d == 0 else shift]
        if group == OUT:
            step = (pc + vc) // CHUNKS
            part = obuf.at[origin, pl.ds(c * step, step)]
        else:
            step = rows // CHUNKS
            at = pl.ds(pl.multiple_of(origin * rows + c * step, step), step)
            part = wkv.at[at] if group == KV else wqp.at[at]
        return pltpu.make_async_remote_copy(
            src_ref=part,
            dst_ref=part,
            send_sem=ring_send.at[group, d, c, s],
            recv_sem=ring_recv.at[group, d, c, s],
            device_id={"sp": nexts[d]},
            device_id_type=MESH,
        )

    def ring_event(group, s, i):
        for d in range(2):
            c = i if d == 0 else (i + CHUNKS // 2) % CHUNKS
            hops = hops_of(d, c)
            if 0 < s <= hops:
                ring_copy(group, d, c, s - 1, True).wait_recv()
            if s < hops:
                ring_copy(group, d, c, s, False).start()

    order = event_order(half)
    done = 0

    def pump(count=1):
        nonlocal done
        for event in order[done : done + count]:
            ring_event(*event)
        done = min(done + count, len(order))

    def pump_to(event):
        pump(order.index(event) + 1 - done)

    def token_copy(kind, c=0):
        step = m // TOK_CHUNKS
        if kind == 0:
            slot, part, peer = 0, my_tok, sibling
        elif kind == 1:
            slot, peer = 1 + c, across
            part = pl.ds(pl.multiple_of(tp * m + c * step, step), step)
        else:
            slot, peer = 1 + TOK_CHUNKS + c, sibling
            part = pl.ds(pl.multiple_of(across * m + c * step, step), step)
        return pltpu.make_async_remote_copy(
            src_ref=xraw.at[part],
            dst_ref=xraw.at[part],
            send_sem=tok_send.at[slot],
            recv_sem=tok_recv.at[slot],
            device_id={"tp": peer},
            device_id_type=MESH,
        )

    def normalize_rows(source, c, count):
        piece = pl.ds(pl.multiple_of(source * m + c * count, count), count)
        floats = xraw[piece, :].astype(f32)
        scale = lax.rsqrt(jnp.mean(floats * floats, axis=-1, keepdims=True) + eps_value)
        normed[piece, :] = (floats * scale).astype(bf16)

    t_copy.wait()
    for c in range(TOK_CHUNKS):
        token_copy(1, c).start()
    token_copy(0).start()
    for copy in w_copies:
        copy.wait()
    pump(CHUNKS)
    for copy in late_copies:
        copy.wait()
    normalize_rows(tp, 0, m)
    token_copy(0).wait_recv()
    normalize_rows(sibling, 0, m)
    for c in range(TOK_CHUNKS):
        token_copy(1, c).wait_recv()
        token_copy(2, c).start()
        normalize_rows(across, c, m // TOK_CHUNKS)
        if c > 0:
            token_copy(2, c - 1).wait_recv()
            normalize_rows(across_sibling, c - 1, m // TOK_CHUNKS)
        pump(1)
    token_copy(2, TOK_CHUNKS - 1).wait_recv()
    normalize_rows(across_sibling, TOK_CHUNKS - 1, m // TOK_CHUNKS)
    pump(CHUNKS // 2 + CHUNKS)

    low = nt(normed[...], inner[...]).astype(bf16)
    cols = pl.ds(pl.multiple_of(tp * qc, qc), qc)
    lane2 = lax.broadcasted_iota(jnp.int32, (1, 2 * qc), 1)
    heads = spikes.shape[0]
    padded = jnp.concatenate([spikes[...], jnp.zeros((8 - heads, seq), f32)], axis=0)
    chosen = (
        lax.broadcasted_iota(jnp.int32, (8, qc), 1) // KEY_CHANNELS
        == lax.broadcasted_iota(jnp.int32, (8, qc), 0)
    ).astype(f32)
    spread = lax.dot_general(
        padded, chosen, (((0,), (0,)), ((), ())), precision=highest, preferred_element_type=f32
    )
    for direction in range(2):
        pre = nn(
            low[:, direction * RANK : (direction + 1) * RANK], outer[direction, :, cols]
        ) + bias[direction : direction + 1, cols]
        ld[:, direction * qc : (direction + 1) * qc] = (
            jnp.minimum(pre, 0.0) - jnp.log1p(jnp.exp(-jnp.abs(pre)))
        ) / gate_norm_factor + spread

    pump_to((KV, half, CHUNKS // 2 - 1))
    kv[...] = nn(normed[...], wkv[...]).astype(bf16)
    pump(1)

    row_ids = lax.broadcasted_iota(jnp.int32, (BLOCK, BLOCK), 0)
    col_ids = lax.broadcasted_iota(jnp.int32, (BLOCK, BLOCK), 1)
    lower = (col_ids <= row_ids).astype(f32)
    upper = (col_ids >= row_ids).astype(f32)
    first = lax.broadcasted_iota(jnp.int32, (1, qc), 1) < KEY_CHANNELS
    k0 = first.astype(f32)
    k1 = 1.0 - k0
    first2 = lax.rem(lane2, qc) < KEY_CHANNELS
    v0 = (lax.broadcasted_iota(jnp.int32, (1, vc), 1) < DV).astype(f32)
    v1 = 1.0 - v0
    allowed = (
        lax.rem(lax.broadcasted_iota(jnp.int32, (BLOCK, qc), 1), BLOCK)
        <= lax.broadcasted_iota(jnp.int32, (BLOCK, qc), 0)
    )

    for b in range(blocks):
        at = pl.ds(b * BLOCK, BLOCK)
        cum_f = jnp.dot(lower, ld[at, :qc], precision=highest, preferred_element_type=f32)
        cum_b = jnp.dot(upper, ld[at, qc:], precision=highest, preferred_element_type=f32)
        k = kv[at, :qc].astype(f32)
        edge_f = cum_f[BLOCK - 1 : BLOCK, :]
        edge_b = cum_b[0:1, :]
        ld[at, :qc] = cum_f
        ld[at, qc:] = cum_b
        kbuf[at, :qc] = (k * jnp.exp(-cum_f)).astype(bf16)
        kbuf[at, qc:] = (k * jnp.exp(-cum_b)).astype(bf16)
        edges[b : b + 1, :] = jnp.concatenate([edge_f, edge_b], axis=1)
        weighted = jnp.concatenate(
            [k * jnp.exp(edge_f - cum_f), k * jnp.exp(edge_b - cum_b)], axis=1
        ).astype(bf16)
        full = tn(kv[at, qc:], weighted)
        upd[b] = jnp.where(first2, full[:DV], full[DV:])
        if b % 4 == 3:
            pump(1)

    total_f = jnp.zeros((DV, qc), f32)
    total_b = jnp.zeros((DV, qc), f32)
    for b in range(blocks):
        total_f = jnp.exp(edges[b : b + 1, :qc]) * total_f + upd[b, :, :qc]
    for b in reversed(range(blocks)):
        total_b = jnp.exp(edges[b : b + 1, qc:]) * total_b + upd[b, :, qc:]
    logs = jnp.sum(edges[...], axis=0, keepdims=True)
    log_f, log_b = logs[:, :qc], logs[:, qc:]
    total[0] = total_f
    total[1] = total_b
    plane, planes = me // 2, n // 2
    hd = DV // 2
    my_half = pl.ds(pl.multiple_of(odd * hd, hd), hd)
    other_half = pl.ds(pl.multiple_of((1 - odd) * hd, hd), hd)
    ids = lax.broadcasted_iota(jnp.int32, (RIM, qc), 0)

    def packed(*values):
        filled = jnp.zeros((RIM, qc), f32)
        for i, value in enumerate(values):
            hi = value.astype(bf16).astype(f32)
            filled = jnp.where(ids == 2 * i, hi, jnp.where(ids == 2 * i + 1, value - hi, filled))
        return filled.astype(bf16)

    pair_out[pl.ds(0, hd), :] = total[0, other_half, :].astype(bf16)
    pair_out[pl.ds(hd, hd), :] = total[1, other_half, :].astype(bf16)
    pair_out[pl.ds(2 * hd, RIM), :] = packed(log_f, log_b)

    def pair_copy(i):
        return pltpu.make_async_remote_copy(
            src_ref=(pair_out, back_out)[i],
            dst_ref=(pair_in, back_in)[i],
            send_sem=pair_send.at[i],
            recv_sem=pair_recv.at[i],
            device_id={"sp": me + 1 - 2 * odd},
            device_id_type=MESH,
        )

    def state_copy(d):
        peer = lax.rem(plane + d, planes)
        return pltpu.make_async_remote_copy(
            src_ref=msg.at[jnp.where(peer > plane, 0, 1)],
            dst_ref=inbox.at[plane],
            send_sem=st_send.at[d - 1],
            recv_sem=st_recv.at[d - 1],
            device_id={"sp": 2 * peer + odd},
            device_id_type=MESH,
        )

    def state_landed(source):
        d = lax.rem(plane - source + planes, planes)
        return pltpu.make_async_remote_copy(
            src_ref=msg.at[0],
            dst_ref=inbox.at[source],
            send_sem=st_send.at[d - 1],
            recv_sem=st_recv.at[d - 1],
            device_id={"sp": 2 * source + odd},
            device_id_type=MESH,
        )

    pair_copy(0).start()
    pump(PUMPS[0])
    pair_copy(0).wait_recv()
    even = odd == 0
    theirs_f = pair_in[pl.ds(0, hd), :].astype(f32)
    theirs_b = pair_in[pl.ds(hd, hd), :].astype(f32)
    tail = pair_in[pl.ds(2 * hd, RIM), :].astype(f32)
    peer_log_f, peer_log_b = tail[0:1] + tail[1:2], tail[2:3] + tail[3:4]
    mine_f, mine_b = total[0, my_half, :], total[1, my_half, :]
    late_f = jnp.exp(jnp.where(even, peer_log_f, log_f))
    late_b = jnp.exp(jnp.where(even, log_b, peer_log_b))
    msg[0, pl.ds(0, hd), :] = (
        late_f * jnp.where(even, mine_f, theirs_f) + jnp.where(even, theirs_f, mine_f)
    ).astype(bf16)
    msg[1, pl.ds(0, hd), :] = (
        late_b * jnp.where(even, theirs_b, mine_b) + jnp.where(even, mine_b, theirs_b)
    ).astype(bf16)
    msg[0, pl.ds(hd, RIM), :] = packed(log_f + peer_log_f)
    msg[1, pl.ds(hd, RIM), :] = packed(log_b + peer_log_b)
    for d in range(1, planes):
        state_copy(d).start()
    pump(PUMPS[1])

    def join(source, state):
        state_landed(source).wait_recv()
        tail = inbox[source, pl.ds(hd, RIM), :].astype(f32)
        log = tail[0:1, :] + tail[1:2, :]
        return jnp.exp(log) * state + inbox[source, pl.ds(0, hd), :].astype(f32)

    entry[0] = start[0].T
    entry[1] = start[1].T
    plane_f = lax.fori_loop(0, plane, join, entry[0, my_half, :])
    plane_b = lax.fori_loop(
        0, planes - 1 - plane, lambda i, st: join(planes - 1 - i, st), entry[1, my_half, :]
    )
    after_mine_f = jnp.exp(log_f) * plane_f + mine_f
    after_theirs_f = jnp.exp(peer_log_f) * plane_f + theirs_f
    after_mine_b = jnp.exp(log_b) * plane_b + mine_b
    after_theirs_b = jnp.exp(peer_log_b) * plane_b + theirs_b
    back_out[pl.ds(0, hd), :] = jnp.where(even, after_mine_f, plane_f).astype(bf16)
    back_out[pl.ds(hd, hd), :] = jnp.where(even, plane_b, after_mine_b).astype(bf16)
    pair_copy(1).start()
    entry[0, my_half, :] = jnp.where(even, plane_f, after_theirs_f)
    entry[1, my_half, :] = jnp.where(even, after_theirs_b, plane_b)

    pump_to((QP, half, CHUNKS // 2 - 1))
    pbuf[pl.ds(RIM, seq), :] = nn(normed[...], wqp[:, qc:]).astype(bf16)

    def halo(side):
        src = pl.ds(seq, RIM) if side == 0 else pl.ds(RIM, RIM)
        dst = pl.ds(0, RIM) if side == 0 else pl.ds(RIM + seq, RIM)
        peer = jnp.minimum(me + 1, n - 1) if side == 0 else jnp.maximum(me - 1, 0)
        return pltpu.make_async_remote_copy(
            src_ref=pbuf.at[src],
            dst_ref=pbuf.at[dst],
            send_sem=halo_send.at[side],
            recv_sem=halo_recv.at[side],
            device_id={"sp": peer},
            device_id_type=MESH,
        )

    @pl.when(me < n - 1)
    def _():
        halo(0).start()

    @pl.when(me > 0)
    def _():
        halo(1).start()

    @pl.when(me == 0)
    def _():
        pbuf[pl.ds(0, RIM), :] = jnp.zeros((RIM, pc), bf16)

    @pl.when(me == n - 1)
    def _():
        pbuf[pl.ds(RIM + seq, RIM), :] = jnp.zeros((RIM, pc), bf16)

    query = nn(normed[...], wqp[:, :qc]).astype(bf16)
    pump(1)
    pair_copy(1).wait_recv()
    entry[0, other_half, :] = back_in[pl.ds(0, hd), :].astype(f32)
    entry[1, other_half, :] = back_in[pl.ds(hd, hd), :].astype(f32)
    state_f, state_b = entry[0], entry[1]
    for b in reversed(range(blocks)):
        before_b[b] = state_b
        state_b = jnp.exp(edges[b : b + 1, qc:]) * state_b + upd[b, :, qc:]
    for b in range(blocks):
        at = pl.ds(b * BLOCK, BLOCK)
        q = query[b * BLOCK : (b + 1) * BLOCK].astype(f32) * KEY_CHANNELS ** (-0.5)
        qf = (q * jnp.exp(ld[at, :qc])).astype(bf16)
        qb = (q * jnp.exp(ld[at, qc:])).astype(bf16)
        kf = kbuf[at, :qc].astype(f32)
        kb = kbuf[at, qc:].astype(f32)
        scores_f = nt(qf, jnp.concatenate([kf * k0, kf * k1], axis=0).astype(bf16))
        scores_b = nt(qb, jnp.concatenate([kb * k0, kb * k1], axis=0).astype(bf16))
        scores = jnp.where(allowed, scores_f, scores_b).astype(bf16)
        vf = kv[at, qc:].astype(f32)
        both = jnp.concatenate([vf * v0, vf * v1], axis=0).astype(bf16)
        back = before_b[b]
        memory = jnp.concatenate(
            [
                jnp.concatenate([state_f * k0, back * k0], axis=1),
                jnp.concatenate([state_f * k1, back * k1], axis=1),
            ],
            axis=0,
        ).astype(bf16)
        joined = nn(scores, both) + nt(jnp.concatenate([qf, qb], axis=1), memory)
        for h in range(vc // DV):
            o = joined[:, h * DV : (h + 1) * DV]
            scale = lax.rsqrt(jnp.mean(o * o, axis=-1, keepdims=True) + eps_value)
            act[at, pc + h * DV : pc + (h + 1) * DV] = (o * scale).astype(bf16)
        if b + 1 < blocks:
            state_f = jnp.exp(edges[b : b + 1, :qc]) * state_f + upd[b, :, :qc]
        if b % 4 == 3:
            pump(1)

    @pl.when(me > 0)
    def _():
        halo(0).wait_recv()

    @pl.when(me < n - 1)
    def _():
        halo(1).wait_recv()

    window = jnp.left_shift(jnp.int32(2), tp)
    half_width = window // 2
    tile = 2 * BLOCK
    offset = (
        lax.broadcasted_iota(jnp.int32, (tile, tile + 2 * RIM), 1)
        - RIM
        - lax.broadcasted_iota(jnp.int32, (tile, tile + 2 * RIM), 0)
    )
    band = ((offset >= -half_width) & (offset < window - half_width)).astype(f32).astype(bf16)
    seq_length = seq * n
    for b in range(seq // tile):
        sums = nn(band, pbuf[pl.ds(b * tile, tile + 2 * RIM), :])
        position = me * seq + b * tile + lax.broadcasted_iota(jnp.int32, (tile, 1), 0)
        low_end = jnp.clip(position - half_width, 0, seq_length - 1)
        high_end = jnp.clip(position - half_width + window - 1, 0, seq_length - 1)
        counted = (high_end - low_end + 1).astype(f32)
        pooled = (sums / counted - pbuf[pl.ds(RIM + b * tile, tile), :].astype(f32)).astype(bf16)
        act[pl.ds(b * tile, tile), :pc] = nn(pooled, gmap[...]).astype(bf16)

    block_at = [0]
    for k in range(1, half):
        block_at += [-k, k]
    block_at.append(half)

    def rows_of(dest):
        return pl.ds(pl.multiple_of(dest * m, m), m)

    def sib_copy(i):
        return pltpu.make_async_remote_copy(
            src_ref=sib_out.at[i],
            dst_ref=sib_in.at[i],
            send_sem=sib_send.at[i],
            recv_sem=sib_recv.at[i],
            device_id={"tp": sibling},
            device_id_type=MESH,
        )

    def x_copy(i):
        return pltpu.make_async_remote_copy(
            src_ref=x_out.at[i],
            dst_ref=x_in.at[i],
            send_sem=x_send.at[i],
            recv_sem=x_recv.at[i],
            device_id={"tp": across},
            device_id_type=MESH,
        )

    def produce(i):
        weights = obuf[origins[block_at[i]]]
        sib_out[i, pl.ds(0, m)] = nn(act[rows_of(across_sibling), :], weights).astype(bf16)
        sib_out[i, pl.ds(m, m)] = nn(act[rows_of(sibling), :], weights).astype(bf16)
        sib_copy(i).start()
        x_part[i] = nn(act[rows_of(across), :], weights)
        own[i] = nn(act[rows_of(tp), :], weights)

    def cross(i):
        sib_copy(i).wait_recv()
        x_out[i] = (x_part[i] + sib_in[i, pl.ds(0, m)].astype(f32)).astype(bf16)
        x_copy(i).start()

    def finish(i):
        x_copy(i).wait_recv()
        at = pl.ds(pl.multiple_of(origins[block_at[i]] * ocols, ocols), ocols)
        result[:, at] = (
            own[i] + sib_in[i, pl.ds(m, m)].astype(f32) + x_in[i].astype(f32)
        ).astype(bf16)

    produce(0)
    for s in range(1, half):
        pump_to((OUT, s, CHUNKS - 1))
        produce(2 * s - 1)
        cross(2 * s - 2)
        produce(2 * s)
        cross(2 * s - 1)
        if s > 1:
            finish(2 * s - 4)
            finish(2 * s - 3)
    pump(len(order))
    produce(n - 1)
    cross(n - 2)
    cross(n - 1)
    for i in range(n - 4, n):
        finish(i)

    token_copy(0).wait_send()
    for c in range(TOK_CHUNKS):
        token_copy(1, c).wait_send()
        token_copy(2, c).wait_send()
    for group in range(3):
        for d in range(2):
            for c in range(CHUNKS):
                for s in range(hops_of(d, c)):
                    ring_copy(group, d, c, s, False).wait_send()

    @pl.when(me < n - 1)
    def _():
        halo(0).wait_send()

    @pl.when(me > 0)
    def _():
        halo(1).wait_send()

    for i in range(2):
        pair_copy(i).wait_send()
    for d in range(1, planes):
        state_copy(d).wait_send()
    for i in range(n):
        sib_copy(i).wait_send()
        x_copy(i).wait_send()


def event_order(half):
    lead, rest = range(CHUNKS // 2), range(CHUNKS // 2, CHUNKS)
    events = []
    for group in (KV, QP, OUT):
        waits = events[-CHUNKS:] if events else []
        events = events[: len(events) - len(waits)]
        events += [(group, 0, i) for i in range(CHUNKS)] + waits
        for s in range(1, half - 1):
            events += [(group, s, i) for i in range(CHUNKS)]
        events += [(group, half - 1, i) for i in lead]
        events += [(group, half - 1, i) for i in rest] + [(group, half, i) for i in lead]
    return events


def one_kernel(
    n,
    tps,
    tokens,
    pooling_input_weight,
    query_matrix,
    key_matrix,
    value_matrix,
    decay_inner_weight,
    decay_outer_weight,
    channel_decay_bias,
    spike_log_decay,
    starting_state,
    pooling_group_map,
    pooling_output_weight,
    attention_output_weight,
):
    m, width = tokens.shape
    seq = m * tps
    pc, qc, vc = (a.shape[1] for a in (pooling_input_weight, query_matrix, value_matrix))
    ocols = pooling_output_weight.shape[1]
    blocks = seq // BLOCK
    f32, bf16 = jnp.float32, jnp.bfloat16
    vmem = pl.BlockSpec(memory_space=pltpu.VMEM)
    hbm = pl.BlockSpec(memory_space=pl.ANY)
    dma = pltpu.SemaphoreType.DMA
    return pl.pallas_call(
        functools.partial(fused, n),
        out_shape=pltpu.VMEM((m, n * ocols), bf16),
        in_specs=[hbm] * 13,
        out_specs=vmem,
        scratch_shapes=[
            pltpu.VMEM((decay_inner_weight.shape[1], width), bf16),
            pltpu.VMEM((2, RANK, decay_outer_weight.shape[2]), bf16),
            pltpu.VMEM(channel_decay_bias.shape, f32),
            pltpu.VMEM(spike_log_decay.shape, f32),
            pltpu.VMEM((2, qc, DV), f32),
            pltpu.VMEM((seq, width), bf16),
            pltpu.VMEM((seq, width), bf16),
            pltpu.VMEM((width, qc + vc), bf16),
            pltpu.VMEM((width, qc + pc), bf16),
            pltpu.VMEM((n, pc + vc, ocols), bf16),
            pltpu.VMEM((seq + 2 * RIM, pc), bf16),
            pltpu.VMEM((seq, qc + vc), bf16),
            pltpu.VMEM((seq, 2 * qc), f32),
            pltpu.VMEM((seq, 2 * qc), bf16),
            pltpu.VMEM((blocks, DV, 2 * qc), f32),
            pltpu.VMEM((blocks, 2 * qc), f32),
            pltpu.VMEM((blocks, DV, qc), f32),
            pltpu.VMEM((seq, pc + vc), bf16),
            pltpu.VMEM((2, DV, qc), f32),
            pltpu.VMEM((DV + RIM, qc), bf16),
            pltpu.VMEM((DV + RIM, qc), bf16),
            pltpu.VMEM((2, DV // 2 + RIM, qc), bf16),
            pltpu.VMEM((n // 2, DV // 2 + RIM, qc), bf16),
            pltpu.VMEM((DV, qc), bf16),
            pltpu.VMEM((DV, qc), bf16),
            pltpu.VMEM((2, DV, qc), f32),
            pltpu.VMEM((pc, pc), bf16),
            pltpu.VMEM((n, 2 * m, ocols), bf16),
            pltpu.VMEM((n, 2 * m, ocols), bf16),
            pltpu.VMEM((n, m, ocols), f32),
            pltpu.VMEM((n, m, ocols), bf16),
            pltpu.VMEM((n, m, ocols), bf16),
            pltpu.VMEM((n, m, ocols), f32),
            dma((13,)),
            dma((1 + 2 * TOK_CHUNKS,)),
            dma((1 + 2 * TOK_CHUNKS,)),
            dma((3, 2, CHUNKS, n // 2)),
            dma((3, 2, CHUNKS, n // 2)),
            dma((2,)),
            dma((2,)),
            dma((2,)),
            dma((2,)),
            dma((n // 2 - 1,)),
            dma((n // 2 - 1,)),
            dma((n,)),
            dma((n,)),
            dma((n,)),
            dma((n,)),
        ],
        compiler_params=pltpu.CompilerParams(
            collective_id=0, has_side_effects=True, vmem_limit_bytes=60 * 2**20
        ),
    )(
        tokens,
        pooling_input_weight,
        query_matrix,
        key_matrix,
        value_matrix,
        decay_inner_weight.T,
        decay_outer_weight,
        channel_decay_bias,
        spike_log_decay,
        starting_state.reshape(2, qc, DV),
        pooling_group_map,
        pooling_output_weight,
        attention_output_weight,
    )


def solution(mesh):
    in_specs = (
        P(("sp", "tp"), None),
        P("sp", "tp"),
        P("sp", "tp"),
        P("sp", "tp"),
        P("sp", "tp"),
        P(),
        P(),
        P(),
        P("tp", "sp"),
        P(None, "tp", None, None),
        P(),
        P("tp", "sp"),
        P("tp", "sp"),
    )
    out_specs = P(("sp", "tp"), None)
    n, tps = mesh.shape["sp"], mesh.shape["tp"]
    fits = n % 4 == 0 and n <= 16 and tps == 4
    local = functools.partial(one_kernel, n, tps) if fits else shards
    return jax.shard_map(local, mesh=mesh, in_specs=in_specs, out_specs=out_specs, check_vma=False)
```

```python
import functools

import jax
import jax.numpy as jnp
from jax import lax
from jax.experimental import pallas as pl
from jax.experimental.pallas import tpu as pltpu
from jax.sharding import PartitionSpec as P

KEY_CHANNELS = 64
DV = 128
RANK = 32
BLOCK = 64


eps_value = 1e-06
gate_norm_factor = 16.0
highest = lax.Precision.HIGHEST
rim_width = 8


def extended(value, sides, width):
    for axis, dim in sides:
        devices, length = (lax.axis_size(axis), value.shape[dim])
        up = [(i, (i + 1) % devices) for i in range(devices - 1)]
        down = [(j, i) for i, j in up]
        last = lax.slice_in_dim(value, length - width, length, axis=dim)
        leading = lax.slice_in_dim(value, 0, width, axis=dim)
        before = lax.ppermute(last, axis, up)
        after = lax.ppermute(leading, axis, down)
        value = jnp.concatenate([before, value, after], axis=dim)
    return value


def entering_2(value, axis, join, neutral, backward):
    count = lax.axis_size(axis)
    place = lax.axis_index(axis)
    ahead = count - 1 - place if backward else place
    gathered = jax.tree.map(
        lambda a, kind: lax.all_gather(a.astype(kind), axis),
        value,
        jax.tree.map(lambda a: jnp.bfloat16 if a.dtype == jnp.float32 else a.dtype, value),
    )
    state = jax.tree.map(lambda a, e: jnp.zeros_like(a) + jnp.asarray(e, a.dtype), value, neutral)

    def one(lap, state):
        source = count - 1 - lap if backward else lap
        return join(
            state,
            jax.tree.map(
                lambda a, own: lax.dynamic_index_in_dim(a, source, 0, False).astype(own.dtype),
                gathered,
                value,
            ),
        )

    return lax.fori_loop(0, ahead, one, state)


def normalize(token_rows):
    floats = token_rows.astype(jnp.float32)
    scaled = floats * lax.rsqrt(jnp.mean(floats * floats, axis=-1, keepdims=True) + eps_value)
    return scaled.astype(jnp.bfloat16)


def chain_combine(earlier, later):
    return (earlier[0] + later[0], jnp.exp(later[0])[..., None] * earlier[1] + later[1])


def local_chain(decays, updates, backward):

    def advance(carried, element):
        log_total, memory = carried
        decay_now, update_now = element
        return (
            (log_total + decay_now, jnp.exp(decay_now)[..., None] * memory + update_now),
            (log_total, memory),
        )

    begin = (jnp.zeros_like(decays[0]), jnp.zeros_like(updates[0]))
    return lax.scan(advance, begin, (decays, updates), reverse=backward)


def within_blocks(queries, cumulative, key_rows, value_rows, lower):
    row_ids = lax.broadcasted_iota(jnp.int32, (BLOCK, BLOCK), 0)
    col_ids = lax.broadcasted_iota(jnp.int32, (BLOCK, BLOCK), 1)
    allowed = col_ids <= row_ids if lower else col_ids > row_ids
    scaled_q = queries * jnp.exp(cumulative)
    scaled_k = key_rows * jnp.exp(-cumulative)
    scores = jnp.einsum("hnid,hnjd->hnij", scaled_q, scaled_k, precision=highest)
    scores = jnp.where(allowed, scores, 0.0)
    return (scaled_q, jnp.einsum("hnij,hnjv->hniv", scores, value_rows, precision=highest))


def block_updates(key_rows, value_rows, cumulative, edge):
    weighted = key_rows * jnp.exp(edge[:, :, None, :] - cumulative)
    return jnp.einsum("hncd,hncv->hndv", weighted, value_rows, precision=highest)


def carried_term(scaled_q, before, entering):
    log_before, memory_before = before
    block_memory = jnp.exp(log_before)[..., None] * entering[None] + memory_before
    return jnp.einsum("hnid,nhdv->hniv", scaled_q, block_memory, precision=highest)


def shards(
    tokens,
    pooling_input_weight,
    query_matrix,
    key_matrix,
    value_matrix,
    decay_inner_weight,
    decay_outer_weight,
    channel_decay_bias,
    spike_log_decay,
    starting_state,
    pooling_group_map,
    pooling_output_weight,
    attention_output_weight,
):
    sp_index = lax.axis_index("sp")
    tp_index = lax.axis_index("tp")
    normed = normalize(tokens)
    pool_cols = pooling_input_weight.shape[1]
    qk_cols = query_matrix.shape[1]
    value_cols = value_matrix.shape[1]
    local_weight = jnp.concatenate(
        [pooling_input_weight, query_matrix, key_matrix, value_matrix], axis=1
    )
    whole_weight = lax.all_gather(local_weight, "sp", axis=0, tiled=True)
    row_piece = lax.all_gather(normed, "tp", axis=0, tiled=True)
    main_part = jnp.dot(row_piece, whole_weight, preferred_element_type=jnp.float32).astype(
        jnp.bfloat16
    )
    rank_part = jnp.dot(row_piece, decay_inner_weight, preferred_element_type=jnp.float32).astype(
        jnp.bfloat16
    )
    projected = jnp.concatenate([main_part, rank_part], axis=1)
    sequence_length = projected.shape[0]
    blocks = sequence_length // BLOCK
    heads_here = qk_cols // KEY_CHANNELS
    pool_input = projected[:, :pool_cols]
    query_part = projected[:, pool_cols : pool_cols + qk_cols]
    key_part = projected[:, pool_cols + qk_cols : pool_cols + 2 * qk_cols]
    value_part = projected[:, pool_cols + 2 * qk_cols : pool_cols + 2 * qk_cols + value_cols]
    low_rank = projected[:, pool_cols + 2 * qk_cols + value_cols :]
    window = jnp.left_shift(jnp.int32(2), tp_index)
    half_width = window // 2
    padded = extended(pool_input, (("sp", 0),), rim_width)
    floats = padded.astype(jnp.float32)
    window_sum = jnp.zeros((sequence_length, pool_cols), jnp.float32)
    for offset in range(-rim_width, rim_width):
        inside = ((offset >= -half_width) & (offset < window - half_width)).astype(jnp.float32)
        window_sum = (
            window_sum + inside * floats[rim_width + offset : rim_width + offset + sequence_length]
        )
    seq_length = sequence_length * lax.axis_size("sp")
    position = sp_index * sequence_length + jnp.arange(sequence_length, dtype=jnp.int32)
    low_end = jnp.clip(position - half_width, 0, seq_length - 1)
    high_end = jnp.clip(position - half_width + window - 1, 0, seq_length - 1)
    counted = (high_end - low_end + 1).astype(jnp.float32)[:, None]
    pooled = (window_sum / counted - floats[rim_width : rim_width + sequence_length]).astype(
        jnp.bfloat16
    )
    mix_here = lax.dynamic_index_in_dim(pooling_group_map, tp_index, 0, keepdims=False)
    pool_output = jnp.dot(pooled, mix_here, preferred_element_type=jnp.float32).astype(jnp.bfloat16)

    def split_heads(token_level, width):
        return (
            token_level.astype(jnp.float32)
            .reshape(blocks, BLOCK, heads_here, width)
            .transpose(2, 0, 1, 3)
        )

    queries = split_heads(query_part, KEY_CHANNELS) * KEY_CHANNELS ** (-0.5)
    key_rows = split_heads(key_part, KEY_CHANNELS)
    value_rows = split_heads(value_part, DV)
    up_here = lax.dynamic_slice_in_dim(decay_outer_weight, tp_index * qk_cols, qk_cols, 2)
    bias_here = lax.dynamic_slice_in_dim(channel_decay_bias, tp_index * qk_cols, qk_cols, 1)
    spike_amounts = spike_log_decay.T[:, :, None]

    def log_decay(direction):
        preactivation = (
            jnp.dot(
                low_rank[:, direction * RANK : (direction + 1) * RANK],
                up_here[direction],
                preferred_element_type=jnp.float32,
            )
            + bias_here[direction]
        )
        token_level = (jax.nn.log_sigmoid(preactivation) / gate_norm_factor).reshape(
            sequence_length, heads_here, KEY_CHANNELS
        ) + spike_amounts
        return token_level.reshape(blocks, BLOCK, heads_here, KEY_CHANNELS).transpose(2, 0, 1, 3)

    cum_fwd = jnp.cumsum(log_decay(0), axis=2)
    cum_bwd = jnp.flip(jnp.cumsum(jnp.flip(log_decay(1), 2), axis=2), 2)
    scaled_fwd, inner_fwd = within_blocks(queries, cum_fwd, key_rows, value_rows, True)
    scaled_bwd, inner_bwd = within_blocks(queries, cum_bwd, key_rows, value_rows, False)
    edge_fwd = cum_fwd[:, :, -1, :]
    edge_bwd = cum_bwd[:, :, 0, :]
    updates_fwd = block_updates(key_rows, value_rows, cum_fwd, edge_fwd)
    updates_bwd = block_updates(key_rows, value_rows, cum_bwd, edge_bwd)
    total_fwd, before_fwd = local_chain(
        jnp.moveaxis(edge_fwd, 1, 0), jnp.moveaxis(updates_fwd, 1, 0), False
    )
    total_bwd, before_bwd = local_chain(
        jnp.moveaxis(edge_bwd, 1, 0), jnp.moveaxis(updates_bwd, 1, 0), True
    )
    neutral = (jnp.zeros_like(total_fwd[0]), jnp.zeros_like(total_fwd[1]))
    prefix_fwd = entering_2(total_fwd, "sp", chain_combine, neutral, False)
    prefix_bwd = entering_2(total_bwd, "sp", chain_combine, neutral, True)
    entering_fwd = jnp.exp(prefix_fwd[0])[..., None] * starting_state[0] + prefix_fwd[1]
    entering_bwd = jnp.exp(prefix_bwd[0])[..., None] * starting_state[1] + prefix_bwd[1]
    out_fwd = inner_fwd + carried_term(scaled_fwd, before_fwd, entering_fwd)
    out_bwd = inner_bwd + carried_term(scaled_bwd, before_bwd, entering_bwd)
    joined = out_fwd + out_bwd
    normal_scale = lax.rsqrt(jnp.mean(joined * joined, axis=-1, keepdims=True) + eps_value)
    attention_output = (
        (joined * normal_scale)
        .astype(jnp.bfloat16)
        .transpose(1, 2, 0, 3)
        .reshape(sequence_length, heads_here * DV)
    )
    whole_pool, whole_attention = (
        lax.all_gather(pooling_output_weight, "sp", axis=1, tiled=True),
        lax.all_gather(attention_output_weight, "sp", axis=1, tiled=True),
    )
    part_one = jnp.dot(pool_output, whole_pool, preferred_element_type=jnp.float32)
    part_two = jnp.dot(attention_output, whole_attention, preferred_element_type=jnp.float32)
    return lax.psum_scatter(
        (part_one + part_two).astype(jnp.bfloat16), "tp", scatter_dimension=0, tiled=True
    )


MESH = pl.DeviceIdType.MESH
CHUNKS = 4
TOK_CHUNKS = 8
RIM = 16
KV, QP, OUT = range(3)
PUMPS = (3, 7)
TOK_PUMPS = (3, 0, 1, 2, 0, 2, 1, 5)
LAG = 3


def nt(a, b):
    return lax.dot_general(a, b, (((1,), (1,)), ((), ())), preferred_element_type=jnp.float32)


def tn(a, b):
    return lax.dot_general(a, b, (((0,), (0,)), ((), ())), preferred_element_type=jnp.float32)


def nn(a, b):
    return jnp.dot(a, b, preferred_element_type=jnp.float32)


def fused(
    n,
    tokens,
    w_pool,
    w_query,
    w_key,
    w_value,
    inner_in,
    outer_in,
    bias_in,
    spikes_in,
    start_in,
    group_map,
    w_pool_out,
    w_att_out,
    result,
    inner,
    outer,
    bias,
    spikes,
    start,
    xraw,
    normed,
    wkv,
    wqp,
    obuf,
    pbuf,
    kv,
    ld,
    kbuf,
    upd,
    edges,
    before_b,
    act,
    total,
    pair_out,
    pair_in,
    msg,
    inbox,
    back_out,
    back_in,
    entry,
    gmap,
    sib_out,
    sib_in,
    x_part,
    x_out,
    x_in,
    own,
    d_out,
    d_in,
    local_sem,
    tok_send,
    tok_recv,
    ring_send,
    ring_recv,
    halo_send,
    halo_recv,
    pair_send,
    pair_recv,
    st_send,
    st_recv,
    sib_send,
    sib_recv,
    x_send,
    x_recv,
    d_send,
    d_recv,
):
    me = lax.axis_index("sp")
    tp = lax.axis_index("tp")
    m = tokens.shape[0]
    tps = normed.shape[0] // m
    seq = normed.shape[0]
    rows = w_pool.shape[0]
    pc, qc, vc = w_pool.shape[1], w_query.shape[1], w_value.shape[1]
    hcols = obuf.shape[3]
    ocols = 2 * hcols
    blocks = seq // BLOCK
    half = n // 2
    f32, bf16 = jnp.float32, jnp.bfloat16

    odd = lax.rem(me, 2)
    pos = jnp.where(odd == 0, me // 2, n - 1 - me // 2)

    def at_pos(p):
        p = lax.rem(p + 2 * n, n)
        return jnp.where(p < half, 2 * p, 2 * (n - 1 - p) + 1)

    nexts = (at_pos(pos + 1), at_pos(pos - 1))
    origins = {k: at_pos(pos + k) for k in range(-half, half + 1)}

    sibling = tp + 1 - 2 * lax.rem(tp, 2)
    across = lax.rem(tp + 2, tps)
    across_sibling = lax.rem(sibling + 2, tps)

    locals_ = []

    def local(src, dst):
        copy = pltpu.make_async_copy(src, dst, local_sem.at[len(locals_)])
        copy.start()
        locals_.append(copy)
        return copy

    barrier = pltpu.get_barrier_semaphore()
    for peer in nexts:
        pl.semaphore_signal(barrier, inc=1, device_id={"sp": peer}, device_id_type=MESH)
    for peer in (sibling, across):
        pl.semaphore_signal(barrier, inc=1, device_id={"tp": peer}, device_id_type=MESH)

    my_rows = pl.ds(pl.multiple_of(me * rows, rows), rows)
    my_tok = pl.ds(pl.multiple_of(tp * m, m), m)
    w_copies = [
        local(w_key, wkv.at[my_rows, pl.ds(0, qc)]),
        local(w_value, wkv.at[my_rows, pl.ds(qc, vc)]),
    ]
    t_copy = local(tokens, xraw.at[my_tok])
    late_copies = [
        local(w_query, wqp.at[my_rows, pl.ds(0, qc)]),
        local(w_pool, wqp.at[my_rows, pl.ds(qc, pc)]),
        local(w_pool_out.at[:, pl.ds(0, hcols)], obuf.at[me, 0, pl.ds(0, pc)]),
        local(w_pool_out.at[:, pl.ds(hcols, hcols)], obuf.at[me, 1, pl.ds(0, pc)]),
        local(w_att_out.at[:, pl.ds(0, hcols)], obuf.at[me, 0, pl.ds(pc, vc)]),
        local(w_att_out.at[:, pl.ds(hcols, hcols)], obuf.at[me, 1, pl.ds(pc, vc)]),
        local(group_map.at[tp], gmap),
        local(inner_in, inner),
        local(outer_in, outer),
        local(bias_in, bias),
        local(spikes_in, spikes),
        local(start_in, start),
    ]
    pl.semaphore_wait(barrier, 4)

    def hops_of(d, c):
        return half if (c < CHUNKS // 2) == (d == 0) else half - 1

    def ring_copy(group, d, c, s, landed):
        shift = s + 1 if landed else s
        origin = origins[-shift if d == 0 else shift]
        if group == OUT:
            per = CHUNKS // 2
            step = (pc + vc) // per
            part = obuf.at[origin, c // per, pl.ds(c % per * step, step)]
        else:
            step = rows // CHUNKS
            at = pl.ds(pl.multiple_of(origin * rows + c * step, step), step)
            part = wkv.at[at] if group == KV else wqp.at[at]
        return pltpu.make_async_remote_copy(
            src_ref=part,
            dst_ref=part,
            send_sem=ring_send.at[group, d, c, s],
            recv_sem=ring_recv.at[group, d, c, s],
            device_id={"sp": nexts[d]},
            device_id_type=MESH,
        )

    def ring_event(group, s, i):
        for d in range(2):
            c = i if d == 0 else (i + CHUNKS // 2) % CHUNKS
            hops = hops_of(d, c)
            if 0 < s <= hops:
                ring_copy(group, d, c, s - 1, True).wait_recv()
            if s < hops:
                ring_copy(group, d, c, s, False).start()

    order = event_order(half)
    done = 0

    def pump(count=1):
        nonlocal done
        for event in order[done : done + count]:
            ring_event(*event)
        done = min(done + count, len(order))

    def pump_to(event):
        pump(order.index(event) + 1 - done)

    def token_copy(kind, c=0):
        step = m // TOK_CHUNKS
        if kind == 0:
            slot, part, peer = 0, my_tok, sibling
        elif kind == 1:
            slot, peer = 1 + c, across
            part = pl.ds(pl.multiple_of(tp * m + c * step, step), step)
        else:
            slot, peer = 1 + TOK_CHUNKS + c, sibling
            part = pl.ds(pl.multiple_of(across * m + c * step, step), step)
        return pltpu.make_async_remote_copy(
            src_ref=xraw.at[part],
            dst_ref=xraw.at[part],
            send_sem=tok_send.at[slot],
            recv_sem=tok_recv.at[slot],
            device_id={"tp": peer},
            device_id_type=MESH,
        )

    def normalize_rows(source, c, count):
        piece = pl.ds(pl.multiple_of(source * m + c * count, count), count)
        floats = xraw[piece, :].astype(f32)
        scale = lax.rsqrt(jnp.mean(floats * floats, axis=-1, keepdims=True) + eps_value)
        normed[piece, :] = (floats * scale).astype(bf16)

    t_copy.wait()
    for c in range(TOK_CHUNKS):
        token_copy(1, c).start()
    token_copy(0).start()
    for copy in w_copies:
        copy.wait()
    pump(CHUNKS)
    for copy in late_copies:
        copy.wait()
    normalize_rows(tp, 0, m)
    token_copy(0).wait_recv()
    normalize_rows(sibling, 0, m)
    part = m // TOK_CHUNKS

    def relayed(c):
        token_copy(2, c).wait_recv()
        normalize_rows(across_sibling, c, part)

    for c in range(TOK_CHUNKS):
        pump(TOK_PUMPS[c])
        token_copy(1, c).wait_recv()
        token_copy(2, c).start()
        normalize_rows(across, c, part)
        if c >= LAG:
            relayed(c - LAG)
    for c in range(TOK_CHUNKS - LAG, TOK_CHUNKS):
        relayed(c)

    low = nt(normed[...], inner[...]).astype(bf16)
    cols = pl.ds(pl.multiple_of(tp * qc, qc), qc)
    lane2 = lax.broadcasted_iota(jnp.int32, (1, 2 * qc), 1)
    heads = spikes.shape[0]
    padded = jnp.concatenate([spikes[...], jnp.zeros((8 - heads, seq), f32)], axis=0)
    chosen = (
        lax.broadcasted_iota(jnp.int32, (8, qc), 1) // KEY_CHANNELS
        == lax.broadcasted_iota(jnp.int32, (8, qc), 0)
    ).astype(f32)
    spread = lax.dot_general(
        padded, chosen, (((0,), (0,)), ((), ())), precision=highest, preferred_element_type=f32
    )
    for direction in range(2):
        pre = nn(
            low[:, direction * RANK : (direction + 1) * RANK], outer[direction, :, cols]
        ) + bias[direction : direction + 1, cols]
        ld[:, direction * qc : (direction + 1) * qc] = (
            jnp.minimum(pre, 0.0) - jnp.log1p(jnp.exp(-jnp.abs(pre)))
        ) / gate_norm_factor + spread

    pump_to((KV, half, CHUNKS // 2 - 1))
    kv[...] = nn(normed[...], wkv[...]).astype(bf16)
    pump(1)

    row_ids = lax.broadcasted_iota(jnp.int32, (BLOCK, BLOCK), 0)
    col_ids = lax.broadcasted_iota(jnp.int32, (BLOCK, BLOCK), 1)
    lower = (col_ids <= row_ids).astype(f32)
    upper = (col_ids >= row_ids).astype(f32)
    first = lax.broadcasted_iota(jnp.int32, (1, qc), 1) < KEY_CHANNELS
    k0 = first.astype(f32)
    k1 = 1.0 - k0
    first2 = lax.rem(lane2, qc) < KEY_CHANNELS
    v0 = (lax.broadcasted_iota(jnp.int32, (1, vc), 1) < DV).astype(f32)
    v1 = 1.0 - v0
    allowed = (
        lax.rem(lax.broadcasted_iota(jnp.int32, (BLOCK, qc), 1), BLOCK)
        <= lax.broadcasted_iota(jnp.int32, (BLOCK, qc), 0)
    )

    for b in range(blocks):
        at = pl.ds(b * BLOCK, BLOCK)
        cum_f = jnp.dot(lower, ld[at, :qc], precision=highest, preferred_element_type=f32)
        cum_b = jnp.dot(upper, ld[at, qc:], precision=highest, preferred_element_type=f32)
        k = kv[at, :qc].astype(f32)
        edge_f = cum_f[BLOCK - 1 : BLOCK, :]
        edge_b = cum_b[0:1, :]
        ld[at, :qc] = cum_f
        ld[at, qc:] = cum_b
        kbuf[at, :qc] = (k * jnp.exp(-cum_f)).astype(bf16)
        kbuf[at, qc:] = (k * jnp.exp(-cum_b)).astype(bf16)
        edges[b : b + 1, :] = jnp.concatenate([edge_f, edge_b], axis=1)
        weighted = jnp.concatenate(
            [k * jnp.exp(edge_f - cum_f), k * jnp.exp(edge_b - cum_b)], axis=1
        ).astype(bf16)
        full = tn(kv[at, qc:], weighted)
        upd[b] = jnp.where(first2, full[:DV], full[DV:])
        if b % 4 == 3:
            pump(1)

    total_f = jnp.zeros((DV, qc), f32)
    total_b = jnp.zeros((DV, qc), f32)
    for b in range(blocks):
        total_f = jnp.exp(edges[b : b + 1, :qc]) * total_f + upd[b, :, :qc]
    for b in reversed(range(blocks)):
        total_b = jnp.exp(edges[b : b + 1, qc:]) * total_b + upd[b, :, qc:]
    logs = jnp.sum(edges[...], axis=0, keepdims=True)
    log_f, log_b = logs[:, :qc], logs[:, qc:]
    total[0] = total_f
    total[1] = total_b
    plane, planes = me // 2, n // 2
    hd = DV // 2
    my_half = pl.ds(pl.multiple_of(odd * hd, hd), hd)
    other_half = pl.ds(pl.multiple_of((1 - odd) * hd, hd), hd)
    ids = lax.broadcasted_iota(jnp.int32, (RIM, qc), 0)

    def packed(*values):
        filled = jnp.zeros((RIM, qc), f32)
        for i, value in enumerate(values):
            hi = value.astype(bf16).astype(f32)
            filled = jnp.where(ids == 2 * i, hi, jnp.where(ids == 2 * i + 1, value - hi, filled))
        return filled.astype(bf16)

    pair_out[pl.ds(0, hd), :] = total[0, other_half, :].astype(bf16)
    pair_out[pl.ds(hd, hd), :] = total[1, other_half, :].astype(bf16)
    pair_out[pl.ds(2 * hd, RIM), :] = packed(log_f, log_b)

    def pair_copy(i):
        return pltpu.make_async_remote_copy(
            src_ref=(pair_out, back_out)[i],
            dst_ref=(pair_in, back_in)[i],
            send_sem=pair_send.at[i],
            recv_sem=pair_recv.at[i],
            device_id={"sp": me + 1 - 2 * odd},
            device_id_type=MESH,
        )

    def state_copy(d):
        peer = lax.rem(plane + d, planes)
        return pltpu.make_async_remote_copy(
            src_ref=msg.at[jnp.where(peer > plane, 0, 1)],
            dst_ref=inbox.at[plane],
            send_sem=st_send.at[d - 1],
            recv_sem=st_recv.at[d - 1],
            device_id={"sp": 2 * peer + odd},
            device_id_type=MESH,
        )

    def state_landed(source):
        d = lax.rem(plane - source + planes, planes)
        return pltpu.make_async_remote_copy(
            src_ref=msg.at[0],
            dst_ref=inbox.at[source],
            send_sem=st_send.at[d - 1],
            recv_sem=st_recv.at[d - 1],
            device_id={"sp": 2 * source + odd},
            device_id_type=MESH,
        )

    pair_copy(0).start()
    pump(PUMPS[0])
    pair_copy(0).wait_recv()
    even = odd == 0
    theirs_f = pair_in[pl.ds(0, hd), :].astype(f32)
    theirs_b = pair_in[pl.ds(hd, hd), :].astype(f32)
    tail = pair_in[pl.ds(2 * hd, RIM), :].astype(f32)
    peer_log_f, peer_log_b = tail[0:1] + tail[1:2], tail[2:3] + tail[3:4]
    mine_f, mine_b = total[0, my_half, :], total[1, my_half, :]
    late_f = jnp.exp(jnp.where(even, peer_log_f, log_f))
    late_b = jnp.exp(jnp.where(even, log_b, peer_log_b))
    msg[0, pl.ds(0, hd), :] = (
        late_f * jnp.where(even, mine_f, theirs_f) + jnp.where(even, theirs_f, mine_f)
    ).astype(bf16)
    msg[1, pl.ds(0, hd), :] = (
        late_b * jnp.where(even, theirs_b, mine_b) + jnp.where(even, mine_b, theirs_b)
    ).astype(bf16)
    msg[0, pl.ds(hd, RIM), :] = packed(log_f + peer_log_f)
    msg[1, pl.ds(hd, RIM), :] = packed(log_b + peer_log_b)
    for d in range(1, planes):
        state_copy(d).start()
    pump(PUMPS[1])

    def join(source, state):
        state_landed(source).wait_recv()
        tail = inbox[source, pl.ds(hd, RIM), :].astype(f32)
        log = tail[0:1, :] + tail[1:2, :]
        return jnp.exp(log) * state + inbox[source, pl.ds(0, hd), :].astype(f32)

    entry[0] = start[0].T
    entry[1] = start[1].T
    plane_f = lax.fori_loop(0, plane, join, entry[0, my_half, :])
    plane_b = lax.fori_loop(
        0, planes - 1 - plane, lambda i, st: join(planes - 1 - i, st), entry[1, my_half, :]
    )
    after_mine_f = jnp.exp(log_f) * plane_f + mine_f
    after_theirs_f = jnp.exp(peer_log_f) * plane_f + theirs_f
    after_mine_b = jnp.exp(log_b) * plane_b + mine_b
    after_theirs_b = jnp.exp(peer_log_b) * plane_b + theirs_b
    back_out[pl.ds(0, hd), :] = jnp.where(even, after_mine_f, plane_f).astype(bf16)
    back_out[pl.ds(hd, hd), :] = jnp.where(even, plane_b, after_mine_b).astype(bf16)
    pair_copy(1).start()
    entry[0, my_half, :] = jnp.where(even, plane_f, after_theirs_f)
    entry[1, my_half, :] = jnp.where(even, after_theirs_b, plane_b)

    pump_to((QP, half, CHUNKS // 2 - 1))
    pbuf[pl.ds(RIM, seq), :] = nn(normed[...], wqp[:, qc:]).astype(bf16)

    def halo(side):
        src = pl.ds(seq, RIM) if side == 0 else pl.ds(RIM, RIM)
        dst = pl.ds(0, RIM) if side == 0 else pl.ds(RIM + seq, RIM)
        peer = jnp.minimum(me + 1, n - 1) if side == 0 else jnp.maximum(me - 1, 0)
        return pltpu.make_async_remote_copy(
            src_ref=pbuf.at[src],
            dst_ref=pbuf.at[dst],
            send_sem=halo_send.at[side],
            recv_sem=halo_recv.at[side],
            device_id={"sp": peer},
            device_id_type=MESH,
        )

    @pl.when(me < n - 1)
    def _():
        halo(0).start()

    @pl.when(me > 0)
    def _():
        halo(1).start()

    @pl.when(me == 0)
    def _():
        pbuf[pl.ds(0, RIM), :] = jnp.zeros((RIM, pc), bf16)

    @pl.when(me == n - 1)
    def _():
        pbuf[pl.ds(RIM + seq, RIM), :] = jnp.zeros((RIM, pc), bf16)

    query = nn(normed[...], wqp[:, :qc]).astype(bf16)
    pump(1)
    pair_copy(1).wait_recv()
    entry[0, other_half, :] = back_in[pl.ds(0, hd), :].astype(f32)
    entry[1, other_half, :] = back_in[pl.ds(hd, hd), :].astype(f32)
    state_f, state_b = entry[0], entry[1]
    for b in reversed(range(blocks)):
        before_b[b] = state_b
        state_b = jnp.exp(edges[b : b + 1, qc:]) * state_b + upd[b, :, qc:]
    for b in range(blocks):
        at = pl.ds(b * BLOCK, BLOCK)
        q = query[b * BLOCK : (b + 1) * BLOCK].astype(f32) * KEY_CHANNELS ** (-0.5)
        qf = (q * jnp.exp(ld[at, :qc])).astype(bf16)
        qb = (q * jnp.exp(ld[at, qc:])).astype(bf16)
        kf = kbuf[at, :qc].astype(f32)
        kb = kbuf[at, qc:].astype(f32)
        scores_f = nt(qf, jnp.concatenate([kf * k0, kf * k1], axis=0).astype(bf16))
        scores_b = nt(qb, jnp.concatenate([kb * k0, kb * k1], axis=0).astype(bf16))
        scores = jnp.where(allowed, scores_f, scores_b).astype(bf16)
        vf = kv[at, qc:].astype(f32)
        both = jnp.concatenate([vf * v0, vf * v1], axis=0).astype(bf16)
        back = before_b[b]
        memory = jnp.concatenate(
            [
                jnp.concatenate([state_f * k0, back * k0], axis=1),
                jnp.concatenate([state_f * k1, back * k1], axis=1),
            ],
            axis=0,
        ).astype(bf16)
        joined = nn(scores, both) + nt(jnp.concatenate([qf, qb], axis=1), memory)
        for h in range(vc // DV):
            o = joined[:, h * DV : (h + 1) * DV]
            scale = lax.rsqrt(jnp.mean(o * o, axis=-1, keepdims=True) + eps_value)
            act[at, pc + h * DV : pc + (h + 1) * DV] = (o * scale).astype(bf16)
        if b + 1 < blocks:
            state_f = jnp.exp(edges[b : b + 1, :qc]) * state_f + upd[b, :, :qc]
        if b % 4 == 3:
            pump(1)

    @pl.when(me > 0)
    def _():
        halo(0).wait_recv()

    @pl.when(me < n - 1)
    def _():
        halo(1).wait_recv()

    window = jnp.left_shift(jnp.int32(2), tp)
    half_width = window // 2
    tile = 2 * BLOCK
    offset = (
        lax.broadcasted_iota(jnp.int32, (tile, tile + 2 * RIM), 1)
        - RIM
        - lax.broadcasted_iota(jnp.int32, (tile, tile + 2 * RIM), 0)
    )
    band = ((offset >= -half_width) & (offset < window - half_width)).astype(f32).astype(bf16)
    seq_length = seq * n
    for b in range(seq // tile):
        sums = nn(band, pbuf[pl.ds(b * tile, tile + 2 * RIM), :])
        position = me * seq + b * tile + lax.broadcasted_iota(jnp.int32, (tile, 1), 0)
        low_end = jnp.clip(position - half_width, 0, seq_length - 1)
        high_end = jnp.clip(position - half_width + window - 1, 0, seq_length - 1)
        counted = (high_end - low_end + 1).astype(f32)
        pooled = (sums / counted - pbuf[pl.ds(RIM + b * tile, tile), :].astype(f32)).astype(bf16)
        act[pl.ds(b * tile, tile), :pc] = nn(pooled, gmap[...]).astype(bf16)

    units = [(0, None)]
    for k in range(1, half - 1):
        units += [(-k, None), (k, None)]
    units += [(1 - half, 0), (half - 1, 1), (1 - half, 1), (half - 1, 0), (half, 0), (half, 1)]
    direct = len(units) - 2

    def lanes(i):
        return pl.ds(0, ocols if units[i][1] is None else hcols)

    def rows_of(dest):
        return pl.ds(pl.multiple_of(dest * m, m), m)

    def sib_copy(i, part):
        at = (i, pl.ds(part * m, m), lanes(i))
        return pltpu.make_async_remote_copy(
            src_ref=sib_out.at[at],
            dst_ref=sib_in.at[at],
            send_sem=sib_send.at[i, part],
            recv_sem=sib_recv.at[i, part],
            device_id={"tp": sibling},
            device_id_type=MESH,
        )

    def x_copy(i):
        at = (i, slice(None), lanes(i))
        return pltpu.make_async_remote_copy(
            src_ref=x_out.at[at],
            dst_ref=x_in.at[at],
            send_sem=x_send.at[i],
            recv_sem=x_recv.at[i],
            device_id={"tp": across},
            device_id_type=MESH,
        )

    def direct_copy():
        return pltpu.make_async_remote_copy(
            src_ref=d_out,
            dst_ref=d_in,
            send_sem=d_send.at[0],
            recv_sem=d_recv.at[0],
            device_id={"tp": across_sibling},
            device_id_type=MESH,
        )

    def produce(i):
        offset, side = units[i]
        source = origins[offset]
        if side is None:
            weights = jnp.concatenate([obuf[source, 0], obuf[source, 1]], axis=1)
        else:
            weights = obuf[source, side]
        far = nn(act[rows_of(across_sibling), :], weights).astype(bf16)
        if i == direct:
            d_out[...] = far
            direct_copy().start()
            x_out[i, :, lanes(i)] = nn(act[rows_of(across), :], weights).astype(bf16)
            x_copy(i).start()
        else:
            sib_out[i, pl.ds(0, m), lanes(i)] = far
            sib_copy(i, 0).start()
            x_part[i, :, lanes(i)] = nn(act[rows_of(across), :], weights)
        sib_out[i, pl.ds(m, m), lanes(i)] = nn(act[rows_of(sibling), :], weights).astype(bf16)
        sib_copy(i, 1).start()
        own[i, :, lanes(i)] = nn(act[rows_of(tp), :], weights)

    def cross(i):
        sib_copy(i, 0).wait_recv()
        x_out[i, :, lanes(i)] = (
            x_part[i, :, lanes(i)] + sib_in[i, pl.ds(0, m), lanes(i)].astype(f32)
        ).astype(bf16)
        x_copy(i).start()

    def finish(i):
        offset, side = units[i]
        sib_copy(i, 1).wait_recv()
        x_copy(i).wait_recv()
        summed = (
            own[i, :, lanes(i)]
            + sib_in[i, pl.ds(m, m), lanes(i)].astype(f32)
            + x_in[i, :, lanes(i)].astype(f32)
        )
        if i == direct:
            direct_copy().wait_recv()
            summed = summed + d_in[...].astype(f32)
        begin = origins[offset] * ocols + (side or 0) * hcols
        width = ocols if side is None else hcols
        result[:, pl.ds(pl.multiple_of(begin, width), width)] = summed.astype(bf16)

    def send_waits():
        token_copy(0).wait_send()
        for c in range(TOK_CHUNKS):
            token_copy(1, c).wait_send()
            token_copy(2, c).wait_send()
        for group in range(2):
            for d in range(2):
                for c in range(CHUNKS):
                    for s in range(hops_of(d, c)):
                        ring_copy(group, d, c, s, False).wait_send()

        @pl.when(me < n - 1)
        def _():
            halo(0).wait_send()

        @pl.when(me > 0)
        def _():
            halo(1).wait_send()

        for i in range(2):
            pair_copy(i).wait_send()
        for d in range(1, planes):
            state_copy(d).wait_send()

    last = len(units)
    whole = last - 6
    pump(1)
    produce(0)
    for s in range(1, half - 1):
        pump_to((OUT, s, CHUNKS - 1))
        produce(2 * s - 1)
        cross(2 * s - 2)
        if s == 1:
            pump(1)
        produce(2 * s)
        cross(2 * s - 1)
    pump_to((OUT, half - 1, CHUNKS // 2 - 1))
    cross(whole - 1)
    produce(whole)
    produce(whole + 1)
    for i in range(whole - 1):
        finish(i)
    cross(whole)
    cross(whole + 1)
    pump_to((OUT, half - 1, CHUNKS - 1))
    produce(whole + 2)
    produce(whole + 3)
    send_waits()
    finish(whole - 1)
    cross(whole + 2)
    cross(whole + 3)
    pump(len(order))
    produce(direct)
    produce(direct + 1)
    finish(whole)
    finish(whole + 1)
    cross(direct + 1)
    for i in range(whole + 2, last):
        finish(i)

    for d in range(2):
        for c in range(CHUNKS):
            for s in range(hops_of(d, c)):
                ring_copy(OUT, d, c, s, False).wait_send()
    for i in range(last):
        if i == direct:
            direct_copy().wait_send()
        else:
            sib_copy(i, 0).wait_send()
        sib_copy(i, 1).wait_send()
        x_copy(i).wait_send()


def event_order(half):
    lead, rest = range(CHUNKS // 2), range(CHUNKS // 2, CHUNKS)
    events = []
    for group in (KV, QP, OUT):
        waits = events[-CHUNKS:] if events else []
        events = events[: len(events) - len(waits)]
        events += [(group, 0, i) for i in range(CHUNKS)] + waits
        for s in range(1, half - 1):
            events += [(group, s, i) for i in range(CHUNKS)]
        events += [(group, half - 1, i) for i in lead]
        events += [(group, half - 1, i) for i in rest] + [(group, half, i) for i in lead]
    return events


def one_kernel(
    n,
    tps,
    tokens,
    pooling_input_weight,
    query_matrix,
    key_matrix,
    value_matrix,
    decay_inner_weight,
    decay_outer_weight,
    channel_decay_bias,
    spike_log_decay,
    starting_state,
    pooling_group_map,
    pooling_output_weight,
    attention_output_weight,
):
    m, width = tokens.shape
    seq = m * tps
    pc, qc, vc = (a.shape[1] for a in (pooling_input_weight, query_matrix, value_matrix))
    ocols = pooling_output_weight.shape[1]
    blocks = seq // BLOCK
    units = n + 3
    f32, bf16 = jnp.float32, jnp.bfloat16
    vmem = pl.BlockSpec(memory_space=pltpu.VMEM)
    hbm = pl.BlockSpec(memory_space=pl.ANY)
    dma = pltpu.SemaphoreType.DMA
    return pl.pallas_call(
        functools.partial(fused, n),
        out_shape=pltpu.VMEM((m, n * ocols), bf16),
        in_specs=[hbm] * 13,
        out_specs=vmem,
        scratch_shapes=[
            pltpu.VMEM((decay_inner_weight.shape[1], width), bf16),
            pltpu.VMEM((2, RANK, decay_outer_weight.shape[2]), bf16),
            pltpu.VMEM(channel_decay_bias.shape, f32),
            pltpu.VMEM(spike_log_decay.shape, f32),
            pltpu.VMEM((2, qc, DV), f32),
            pltpu.VMEM((seq, width), bf16),
            pltpu.VMEM((seq, width), bf16),
            pltpu.VMEM((width, qc + vc), bf16),
            pltpu.VMEM((width, qc + pc), bf16),
            pltpu.VMEM((n, 2, pc + vc, ocols // 2), bf16),
            pltpu.VMEM((seq + 2 * RIM, pc), bf16),
            pltpu.VMEM((seq, qc + vc), bf16),
            pltpu.VMEM((seq, 2 * qc), f32),
            pltpu.VMEM((seq, 2 * qc), bf16),
            pltpu.VMEM((blocks, DV, 2 * qc), f32),
            pltpu.VMEM((blocks, 2 * qc), f32),
            pltpu.VMEM((blocks, DV, qc), f32),
            pltpu.VMEM((seq, pc + vc), bf16),
            pltpu.VMEM((2, DV, qc), f32),
            pltpu.VMEM((DV + RIM, qc), bf16),
            pltpu.VMEM((DV + RIM, qc), bf16),
            pltpu.VMEM((2, DV // 2 + RIM, qc), bf16),
            pltpu.VMEM((n // 2, DV // 2 + RIM, qc), bf16),
            pltpu.VMEM((DV, qc), bf16),
            pltpu.VMEM((DV, qc), bf16),
            pltpu.VMEM((2, DV, qc), f32),
            pltpu.VMEM((pc, pc), bf16),
            pltpu.VMEM((units, 2 * m, ocols), bf16),
            pltpu.VMEM((units, 2 * m, ocols), bf16),
            pltpu.VMEM((units, m, ocols), f32),
            pltpu.VMEM((units, m, ocols), bf16),
            pltpu.VMEM((units, m, ocols), bf16),
            pltpu.VMEM((units, m, ocols), f32),
            pltpu.VMEM((m, ocols // 2), bf16),
            pltpu.VMEM((m, ocols // 2), bf16),
            dma((15,)),
            dma((1 + 2 * TOK_CHUNKS,)),
            dma((1 + 2 * TOK_CHUNKS,)),
            dma((3, 2, CHUNKS, n // 2)),
            dma((3, 2, CHUNKS, n // 2)),
            dma((2,)),
            dma((2,)),
            dma((2,)),
            dma((2,)),
            dma((n // 2 - 1,)),
            dma((n // 2 - 1,)),
            dma((units, 2)),
            dma((units, 2)),
            dma((units,)),
            dma((units,)),
            dma((1,)),
            dma((1,)),
        ],
        compiler_params=pltpu.CompilerParams(
            collective_id=0, has_side_effects=True, vmem_limit_bytes=60 * 2**20
        ),
    )(
        tokens,
        pooling_input_weight,
        query_matrix,
        key_matrix,
        value_matrix,
        decay_inner_weight.T,
        decay_outer_weight,
        channel_decay_bias,
        spike_log_decay,
        starting_state.reshape(2, qc, DV),
        pooling_group_map,
        pooling_output_weight,
        attention_output_weight,
    )


def solution(mesh):
    in_specs = (
        P(("sp", "tp"), None),
        P("sp", "tp"),
        P("sp", "tp"),
        P("sp", "tp"),
        P("sp", "tp"),
        P(),
        P(),
        P(),
        P("tp", "sp"),
        P(None, "tp", None, None),
        P(),
        P("tp", "sp"),
        P("tp", "sp"),
    )
    out_specs = P(("sp", "tp"), None)
    n, tps = mesh.shape["sp"], mesh.shape["tp"]
    fits = n % 4 == 0 and n <= 16 and tps == 4
    local = functools.partial(one_kernel, n, tps) if fits else shards
    return jax.shard_map(local, mesh=mesh, in_specs=in_specs, out_specs=out_specs, check_vma=False)
```

```python
import functools

import jax
import jax.numpy as jnp
from jax import lax
from jax.experimental import pallas as pl
from jax.experimental.pallas import tpu as pltpu
from jax.sharding import PartitionSpec as P

KEY_CHANNELS = 64
DV = 128
RANK = 32
BLOCK = 64


eps_value = 1e-06
gate_norm_factor = 16.0
highest = lax.Precision.HIGHEST
rim_width = 8


def extended(value, sides, width):
    for axis, dim in sides:
        devices, length = (lax.axis_size(axis), value.shape[dim])
        up = [(i, (i + 1) % devices) for i in range(devices - 1)]
        down = [(j, i) for i, j in up]
        last = lax.slice_in_dim(value, length - width, length, axis=dim)
        leading = lax.slice_in_dim(value, 0, width, axis=dim)
        before = lax.ppermute(last, axis, up)
        after = lax.ppermute(leading, axis, down)
        value = jnp.concatenate([before, value, after], axis=dim)
    return value


def entering_2(value, axis, join, neutral, backward):
    count = lax.axis_size(axis)
    place = lax.axis_index(axis)
    ahead = count - 1 - place if backward else place
    gathered = jax.tree.map(
        lambda a, kind: lax.all_gather(a.astype(kind), axis),
        value,
        jax.tree.map(lambda a: jnp.bfloat16 if a.dtype == jnp.float32 else a.dtype, value),
    )
    state = jax.tree.map(lambda a, e: jnp.zeros_like(a) + jnp.asarray(e, a.dtype), value, neutral)

    def one(lap, state):
        source = count - 1 - lap if backward else lap
        return join(
            state,
            jax.tree.map(
                lambda a, own: lax.dynamic_index_in_dim(a, source, 0, False).astype(own.dtype),
                gathered,
                value,
            ),
        )

    return lax.fori_loop(0, ahead, one, state)


def normalize(token_rows):
    floats = token_rows.astype(jnp.float32)
    scaled = floats * lax.rsqrt(jnp.mean(floats * floats, axis=-1, keepdims=True) + eps_value)
    return scaled.astype(jnp.bfloat16)


def chain_combine(earlier, later):
    return (earlier[0] + later[0], jnp.exp(later[0])[..., None] * earlier[1] + later[1])


def local_chain(decays, updates, backward):

    def advance(carried, element):
        log_total, memory = carried
        decay_now, update_now = element
        return (
            (log_total + decay_now, jnp.exp(decay_now)[..., None] * memory + update_now),
            (log_total, memory),
        )

    begin = (jnp.zeros_like(decays[0]), jnp.zeros_like(updates[0]))
    return lax.scan(advance, begin, (decays, updates), reverse=backward)


def within_blocks(queries, cumulative, key_rows, value_rows, lower):
    row_ids = lax.broadcasted_iota(jnp.int32, (BLOCK, BLOCK), 0)
    col_ids = lax.broadcasted_iota(jnp.int32, (BLOCK, BLOCK), 1)
    allowed = col_ids <= row_ids if lower else col_ids > row_ids
    scaled_q = queries * jnp.exp(cumulative)
    scaled_k = key_rows * jnp.exp(-cumulative)
    scores = jnp.einsum("hnid,hnjd->hnij", scaled_q, scaled_k, precision=highest)
    scores = jnp.where(allowed, scores, 0.0)
    return (scaled_q, jnp.einsum("hnij,hnjv->hniv", scores, value_rows, precision=highest))


def block_updates(key_rows, value_rows, cumulative, edge):
    weighted = key_rows * jnp.exp(edge[:, :, None, :] - cumulative)
    return jnp.einsum("hncd,hncv->hndv", weighted, value_rows, precision=highest)


def carried_term(scaled_q, before, entering):
    log_before, memory_before = before
    block_memory = jnp.exp(log_before)[..., None] * entering[None] + memory_before
    return jnp.einsum("hnid,nhdv->hniv", scaled_q, block_memory, precision=highest)


def shards(
    tokens,
    pooling_input_weight,
    query_matrix,
    key_matrix,
    value_matrix,
    decay_inner_weight,
    decay_outer_weight,
    channel_decay_bias,
    spike_log_decay,
    starting_state,
    pooling_group_map,
    pooling_output_weight,
    attention_output_weight,
):
    sp_index = lax.axis_index("sp")
    tp_index = lax.axis_index("tp")
    normed = normalize(tokens)
    pool_cols = pooling_input_weight.shape[1]
    qk_cols = query_matrix.shape[1]
    value_cols = value_matrix.shape[1]
    local_weight = jnp.concatenate(
        [pooling_input_weight, query_matrix, key_matrix, value_matrix], axis=1
    )
    whole_weight = lax.all_gather(local_weight, "sp", axis=0, tiled=True)
    row_piece = lax.all_gather(normed, "tp", axis=0, tiled=True)
    main_part = jnp.dot(row_piece, whole_weight, preferred_element_type=jnp.float32).astype(
        jnp.bfloat16
    )
    rank_part = jnp.dot(row_piece, decay_inner_weight, preferred_element_type=jnp.float32).astype(
        jnp.bfloat16
    )
    projected = jnp.concatenate([main_part, rank_part], axis=1)
    sequence_length = projected.shape[0]
    blocks = sequence_length // BLOCK
    heads_here = qk_cols // KEY_CHANNELS
    pool_input = projected[:, :pool_cols]
    query_part = projected[:, pool_cols : pool_cols + qk_cols]
    key_part = projected[:, pool_cols + qk_cols : pool_cols + 2 * qk_cols]
    value_part = projected[:, pool_cols + 2 * qk_cols : pool_cols + 2 * qk_cols + value_cols]
    low_rank = projected[:, pool_cols + 2 * qk_cols + value_cols :]
    window = jnp.left_shift(jnp.int32(2), tp_index)
    half_width = window // 2
    padded = extended(pool_input, (("sp", 0),), rim_width)
    floats = padded.astype(jnp.float32)
    window_sum = jnp.zeros((sequence_length, pool_cols), jnp.float32)
    for offset in range(-rim_width, rim_width):
        inside = ((offset >= -half_width) & (offset < window - half_width)).astype(jnp.float32)
        window_sum = (
            window_sum + inside * floats[rim_width + offset : rim_width + offset + sequence_length]
        )
    seq_length = sequence_length * lax.axis_size("sp")
    position = sp_index * sequence_length + jnp.arange(sequence_length, dtype=jnp.int32)
    low_end = jnp.clip(position - half_width, 0, seq_length - 1)
    high_end = jnp.clip(position - half_width + window - 1, 0, seq_length - 1)
    counted = (high_end - low_end + 1).astype(jnp.float32)[:, None]
    pooled = (window_sum / counted - floats[rim_width : rim_width + sequence_length]).astype(
        jnp.bfloat16
    )
    mix_here = lax.dynamic_index_in_dim(pooling_group_map, tp_index, 0, keepdims=False)
    pool_output = jnp.dot(pooled, mix_here, preferred_element_type=jnp.float32).astype(jnp.bfloat16)

    def split_heads(token_level, width):
        return (
            token_level.astype(jnp.float32)
            .reshape(blocks, BLOCK, heads_here, width)
            .transpose(2, 0, 1, 3)
        )

    queries = split_heads(query_part, KEY_CHANNELS) * KEY_CHANNELS ** (-0.5)
    key_rows = split_heads(key_part, KEY_CHANNELS)
    value_rows = split_heads(value_part, DV)
    up_here = lax.dynamic_slice_in_dim(decay_outer_weight, tp_index * qk_cols, qk_cols, 2)
    bias_here = lax.dynamic_slice_in_dim(channel_decay_bias, tp_index * qk_cols, qk_cols, 1)
    spike_amounts = spike_log_decay.T[:, :, None]

    def log_decay(direction):
        preactivation = (
            jnp.dot(
                low_rank[:, direction * RANK : (direction + 1) * RANK],
                up_here[direction],
                preferred_element_type=jnp.float32,
            )
            + bias_here[direction]
        )
        token_level = (jax.nn.log_sigmoid(preactivation) / gate_norm_factor).reshape(
            sequence_length, heads_here, KEY_CHANNELS
        ) + spike_amounts
        return token_level.reshape(blocks, BLOCK, heads_here, KEY_CHANNELS).transpose(2, 0, 1, 3)

    cum_fwd = jnp.cumsum(log_decay(0), axis=2)
    cum_bwd = jnp.flip(jnp.cumsum(jnp.flip(log_decay(1), 2), axis=2), 2)
    scaled_fwd, inner_fwd = within_blocks(queries, cum_fwd, key_rows, value_rows, True)
    scaled_bwd, inner_bwd = within_blocks(queries, cum_bwd, key_rows, value_rows, False)
    edge_fwd = cum_fwd[:, :, -1, :]
    edge_bwd = cum_bwd[:, :, 0, :]
    updates_fwd = block_updates(key_rows, value_rows, cum_fwd, edge_fwd)
    updates_bwd = block_updates(key_rows, value_rows, cum_bwd, edge_bwd)
    total_fwd, before_fwd = local_chain(
        jnp.moveaxis(edge_fwd, 1, 0), jnp.moveaxis(updates_fwd, 1, 0), False
    )
    total_bwd, before_bwd = local_chain(
        jnp.moveaxis(edge_bwd, 1, 0), jnp.moveaxis(updates_bwd, 1, 0), True
    )
    neutral = (jnp.zeros_like(total_fwd[0]), jnp.zeros_like(total_fwd[1]))
    prefix_fwd = entering_2(total_fwd, "sp", chain_combine, neutral, False)
    prefix_bwd = entering_2(total_bwd, "sp", chain_combine, neutral, True)
    entering_fwd = jnp.exp(prefix_fwd[0])[..., None] * starting_state[0] + prefix_fwd[1]
    entering_bwd = jnp.exp(prefix_bwd[0])[..., None] * starting_state[1] + prefix_bwd[1]
    out_fwd = inner_fwd + carried_term(scaled_fwd, before_fwd, entering_fwd)
    out_bwd = inner_bwd + carried_term(scaled_bwd, before_bwd, entering_bwd)
    joined = out_fwd + out_bwd
    normal_scale = lax.rsqrt(jnp.mean(joined * joined, axis=-1, keepdims=True) + eps_value)
    attention_output = (
        (joined * normal_scale)
        .astype(jnp.bfloat16)
        .transpose(1, 2, 0, 3)
        .reshape(sequence_length, heads_here * DV)
    )
    whole_pool, whole_attention = (
        lax.all_gather(pooling_output_weight, "sp", axis=1, tiled=True),
        lax.all_gather(attention_output_weight, "sp", axis=1, tiled=True),
    )
    part_one = jnp.dot(pool_output, whole_pool, preferred_element_type=jnp.float32)
    part_two = jnp.dot(attention_output, whole_attention, preferred_element_type=jnp.float32)
    return lax.psum_scatter(
        (part_one + part_two).astype(jnp.bfloat16), "tp", scatter_dimension=0, tiled=True
    )


MESH = pl.DeviceIdType.MESH
CHUNKS = 4
TOK_CHUNKS = 8
RIM = 16
KV, QP, OUT = range(3)
PUMPS = (3, 7)
TOK_PUMPS = (3, 0, 1, 2, 0, 2, 1, 5)
LAG = 3


def nt(a, b):
    return lax.dot_general(a, b, (((1,), (1,)), ((), ())), preferred_element_type=jnp.float32)


def tn(a, b):
    return lax.dot_general(a, b, (((0,), (0,)), ((), ())), preferred_element_type=jnp.float32)


def nn(a, b):
    return jnp.dot(a, b, preferred_element_type=jnp.float32)


def fused(
    n,
    tokens,
    w_pool,
    w_query,
    w_key,
    w_value,
    inner_in,
    outer_in,
    bias_in,
    spikes_in,
    start_in,
    group_map,
    w_pool_out,
    w_att_out,
    result,
    inner,
    outer,
    bias,
    spikes,
    start,
    xraw,
    normed,
    wkv,
    wqp,
    obuf,
    pbuf,
    kv,
    ld,
    kbuf,
    upd,
    edges,
    before_b,
    act,
    total,
    pair_out,
    pair_in,
    msg,
    inbox,
    back_out,
    back_in,
    entry,
    gmap,
    sib_out,
    sib_in,
    x_part,
    x_out,
    x_in,
    own,
    d_out,
    d_in,
    local_sem,
    tok_send,
    tok_recv,
    ring_send,
    ring_recv,
    halo_send,
    halo_recv,
    pair_send,
    pair_recv,
    st_send,
    st_recv,
    sib_send,
    sib_recv,
    x_send,
    x_recv,
    d_send,
    d_recv,
):
    me = lax.axis_index("sp")
    tp = lax.axis_index("tp")
    m = tokens.shape[0]
    tps = normed.shape[0] // m
    seq = normed.shape[0]
    rows = w_pool.shape[0]
    pc, qc, vc = w_pool.shape[1], w_query.shape[1], w_value.shape[1]
    hcols = obuf.shape[3]
    ocols = 2 * hcols
    blocks = seq // BLOCK
    half = n // 2
    f32, bf16 = jnp.float32, jnp.bfloat16

    odd = lax.rem(me, 2)
    pos = jnp.where(odd == 0, me // 2, n - 1 - me // 2)

    def at_pos(p):
        p = lax.rem(p + 2 * n, n)
        return jnp.where(p < half, 2 * p, 2 * (n - 1 - p) + 1)

    nexts = (at_pos(pos + 1), at_pos(pos - 1))
    origins = {k: at_pos(pos + k) for k in range(-half, half + 1)}

    sibling = tp + 1 - 2 * lax.rem(tp, 2)
    across = lax.rem(tp + 2, tps)
    across_sibling = lax.rem(sibling + 2, tps)

    locals_ = []

    def local(src, dst):
        copy = pltpu.make_async_copy(src, dst, local_sem.at[len(locals_)])
        copy.start()
        locals_.append(copy)
        return copy

    barrier = pltpu.get_barrier_semaphore()
    for peer in nexts:
        pl.semaphore_signal(barrier, inc=1, device_id={"sp": peer}, device_id_type=MESH)
    for peer in (sibling, across):
        pl.semaphore_signal(barrier, inc=1, device_id={"tp": peer}, device_id_type=MESH)

    my_rows = pl.ds(pl.multiple_of(me * rows, rows), rows)
    my_tok = pl.ds(pl.multiple_of(tp * m, m), m)
    w_copies = [
        local(w_key, wkv.at[my_rows, pl.ds(0, qc)]),
        local(w_value, wkv.at[my_rows, pl.ds(qc, vc)]),
    ]
    t_copy = local(tokens, xraw.at[my_tok])
    late_copies = [
        local(w_query, wqp.at[my_rows, pl.ds(0, qc)]),
        local(w_pool, wqp.at[my_rows, pl.ds(qc, pc)]),
        local(w_pool_out.at[:, pl.ds(0, hcols)], obuf.at[me, 0, pl.ds(0, pc)]),
        local(w_pool_out.at[:, pl.ds(hcols, hcols)], obuf.at[me, 1, pl.ds(0, pc)]),
        local(w_att_out.at[:, pl.ds(0, hcols)], obuf.at[me, 0, pl.ds(pc, vc)]),
        local(w_att_out.at[:, pl.ds(hcols, hcols)], obuf.at[me, 1, pl.ds(pc, vc)]),
        local(group_map.at[tp], gmap),
        local(inner_in, inner),
        local(outer_in, outer),
        local(bias_in, bias),
        local(spikes_in, spikes),
        local(start_in, start),
    ]
    pl.semaphore_wait(barrier, 4)

    def hops_of(d, c):
        return half if (c < CHUNKS // 2) == (d == 0) else half - 1

    def ring_copy(group, d, c, s, landed):
        shift = s + 1 if landed else s
        origin = origins[-shift if d == 0 else shift]
        if group == OUT:
            per = CHUNKS // 2
            step = (pc + vc) // per
            part = obuf.at[origin, c // per, pl.ds(c % per * step, step)]
        else:
            step = rows // CHUNKS
            at = pl.ds(pl.multiple_of(origin * rows + c * step, step), step)
            part = wkv.at[at] if group == KV else wqp.at[at]
        return pltpu.make_async_remote_copy(
            src_ref=part,
            dst_ref=part,
            send_sem=ring_send.at[group, d, c, s],
            recv_sem=ring_recv.at[group, d, c, s],
            device_id={"sp": nexts[d]},
            device_id_type=MESH,
        )

    def ring_event(group, s, i):
        for d in range(2):
            c = i if d == 0 else (i + CHUNKS // 2) % CHUNKS
            hops = hops_of(d, c)
            if 0 < s <= hops:
                ring_copy(group, d, c, s - 1, True).wait_recv()
            if s < hops:
                ring_copy(group, d, c, s, False).start()

    order = event_order(half)
    done = 0

    def pump(count=1):
        nonlocal done
        for event in order[done : done + count]:
            ring_event(*event)
        done = min(done + count, len(order))

    def pump_to(event):
        pump(max(order.index(event) + 1 - done, 0))

    def token_copy(kind, c=0):
        step = m // TOK_CHUNKS
        if kind == 0:
            slot, part, peer = 0, my_tok, sibling
        elif kind == 1:
            slot, peer = 1 + c, across
            part = pl.ds(pl.multiple_of(tp * m + c * step, step), step)
        else:
            slot, peer = 1 + TOK_CHUNKS + c, sibling
            part = pl.ds(pl.multiple_of(across * m + c * step, step), step)
        return pltpu.make_async_remote_copy(
            src_ref=xraw.at[part],
            dst_ref=xraw.at[part],
            send_sem=tok_send.at[slot],
            recv_sem=tok_recv.at[slot],
            device_id={"tp": peer},
            device_id_type=MESH,
        )

    def normalize_rows(source, c, count):
        piece = pl.ds(pl.multiple_of(source * m + c * count, count), count)
        floats = xraw[piece, :].astype(f32)
        scale = lax.rsqrt(jnp.mean(floats * floats, axis=-1, keepdims=True) + eps_value)
        normed[piece, :] = (floats * scale).astype(bf16)

    for copy in w_copies:
        copy.wait()
    pump(CHUNKS)
    t_copy.wait()
    for c in range(TOK_CHUNKS):
        token_copy(1, c).start()
    token_copy(0).start()
    for copy in late_copies:
        copy.wait()
    normalize_rows(tp, 0, m)
    token_copy(0).wait_recv()
    normalize_rows(sibling, 0, m)
    part = m // TOK_CHUNKS

    def relayed(c):
        token_copy(2, c).wait_recv()
        normalize_rows(across_sibling, c, part)

    for c in range(TOK_CHUNKS):
        pump(TOK_PUMPS[c])
        token_copy(1, c).wait_recv()
        token_copy(2, c).start()
        normalize_rows(across, c, part)
        if c >= LAG:
            relayed(c - LAG)
    for c in range(TOK_CHUNKS - LAG, TOK_CHUNKS):
        relayed(c)

    low = nt(normed[...], inner[...]).astype(bf16)
    cols = pl.ds(pl.multiple_of(tp * qc, qc), qc)
    lane2 = lax.broadcasted_iota(jnp.int32, (1, 2 * qc), 1)
    heads = spikes.shape[0]
    padded = jnp.concatenate([spikes[...], jnp.zeros((8 - heads, seq), f32)], axis=0)
    chosen = (
        lax.broadcasted_iota(jnp.int32, (8, qc), 1) // KEY_CHANNELS
        == lax.broadcasted_iota(jnp.int32, (8, qc), 0)
    ).astype(f32)
    spread = lax.dot_general(
        padded, chosen, (((0,), (0,)), ((), ())), precision=highest, preferred_element_type=f32
    )
    for direction in range(2):
        pre = nn(
            low[:, direction * RANK : (direction + 1) * RANK], outer[direction, :, cols]
        ) + bias[direction : direction + 1, cols]
        ld[:, direction * qc : (direction + 1) * qc] = (
            jnp.minimum(pre, 0.0) - jnp.log1p(jnp.exp(-jnp.abs(pre)))
        ) / gate_norm_factor + spread

    pump_to((KV, half, CHUNKS // 2 - 1))
    kv[...] = nn(normed[...], wkv[...]).astype(bf16)
    pump(1)

    row_ids = lax.broadcasted_iota(jnp.int32, (BLOCK, BLOCK), 0)
    col_ids = lax.broadcasted_iota(jnp.int32, (BLOCK, BLOCK), 1)
    lower = (col_ids <= row_ids).astype(f32)
    upper = (col_ids >= row_ids).astype(f32)
    first = lax.broadcasted_iota(jnp.int32, (1, qc), 1) < KEY_CHANNELS
    k0 = first.astype(f32)
    k1 = 1.0 - k0
    first2 = lax.rem(lane2, qc) < KEY_CHANNELS
    v0 = (lax.broadcasted_iota(jnp.int32, (1, vc), 1) < DV).astype(f32)
    v1 = 1.0 - v0
    allowed = (
        lax.rem(lax.broadcasted_iota(jnp.int32, (BLOCK, qc), 1), BLOCK)
        <= lax.broadcasted_iota(jnp.int32, (BLOCK, qc), 0)
    )

    for b in range(blocks):
        at = pl.ds(b * BLOCK, BLOCK)
        cum_f = jnp.dot(lower, ld[at, :qc], precision=highest, preferred_element_type=f32)
        cum_b = jnp.dot(upper, ld[at, qc:], precision=highest, preferred_element_type=f32)
        k = kv[at, :qc].astype(f32)
        edge_f = cum_f[BLOCK - 1 : BLOCK, :]
        edge_b = cum_b[0:1, :]
        ld[at, :qc] = cum_f
        ld[at, qc:] = cum_b
        kbuf[at, :qc] = (k * jnp.exp(-cum_f)).astype(bf16)
        kbuf[at, qc:] = (k * jnp.exp(-cum_b)).astype(bf16)
        edges[b : b + 1, :] = jnp.concatenate([edge_f, edge_b], axis=1)
        weighted = jnp.concatenate(
            [k * jnp.exp(edge_f - cum_f), k * jnp.exp(edge_b - cum_b)], axis=1
        ).astype(bf16)
        full = tn(kv[at, qc:], weighted)
        upd[b] = jnp.where(first2, full[:DV], full[DV:])
        if b % 4 == 3:
            pump(1)

    total_f = jnp.zeros((DV, qc), f32)
    total_b = jnp.zeros((DV, qc), f32)
    for b in range(blocks):
        total_f = jnp.exp(edges[b : b + 1, :qc]) * total_f + upd[b, :, :qc]
    for b in reversed(range(blocks)):
        total_b = jnp.exp(edges[b : b + 1, qc:]) * total_b + upd[b, :, qc:]
    logs = jnp.sum(edges[...], axis=0, keepdims=True)
    log_f, log_b = logs[:, :qc], logs[:, qc:]
    total[0] = total_f
    total[1] = total_b
    plane, planes = me // 2, n // 2
    hd = DV // 2
    my_half = pl.ds(pl.multiple_of(odd * hd, hd), hd)
    other_half = pl.ds(pl.multiple_of((1 - odd) * hd, hd), hd)
    ids = lax.broadcasted_iota(jnp.int32, (RIM, qc), 0)

    def packed(*values):
        filled = jnp.zeros((RIM, qc), f32)
        for i, value in enumerate(values):
            hi = value.astype(bf16).astype(f32)
            filled = jnp.where(ids == 2 * i, hi, jnp.where(ids == 2 * i + 1, value - hi, filled))
        return filled.astype(bf16)

    pair_out[pl.ds(0, hd), :] = total[0, other_half, :].astype(bf16)
    pair_out[pl.ds(hd, hd), :] = total[1, other_half, :].astype(bf16)
    pair_out[pl.ds(2 * hd, RIM), :] = packed(log_f, log_b)

    def pair_copy(i):
        return pltpu.make_async_remote_copy(
            src_ref=(pair_out, back_out)[i],
            dst_ref=(pair_in, back_in)[i],
            send_sem=pair_send.at[i],
            recv_sem=pair_recv.at[i],
            device_id={"sp": me + 1 - 2 * odd},
            device_id_type=MESH,
        )

    def state_copy(d):
        peer = lax.rem(plane + d, planes)
        return pltpu.make_async_remote_copy(
            src_ref=msg.at[jnp.where(peer > plane, 0, 1)],
            dst_ref=inbox.at[plane],
            send_sem=st_send.at[d - 1],
            recv_sem=st_recv.at[d - 1],
            device_id={"sp": 2 * peer + odd},
            device_id_type=MESH,
        )

    def state_landed(source):
        d = lax.rem(plane - source + planes, planes)
        return pltpu.make_async_remote_copy(
            src_ref=msg.at[0],
            dst_ref=inbox.at[source],
            send_sem=st_send.at[d - 1],
            recv_sem=st_recv.at[d - 1],
            device_id={"sp": 2 * source + odd},
            device_id_type=MESH,
        )

    pair_copy(0).start()
    pump(PUMPS[0])
    pair_copy(0).wait_recv()
    even = odd == 0
    theirs_f = pair_in[pl.ds(0, hd), :].astype(f32)
    theirs_b = pair_in[pl.ds(hd, hd), :].astype(f32)
    tail = pair_in[pl.ds(2 * hd, RIM), :].astype(f32)
    peer_log_f, peer_log_b = tail[0:1] + tail[1:2], tail[2:3] + tail[3:4]
    mine_f, mine_b = total[0, my_half, :], total[1, my_half, :]
    late_f = jnp.exp(jnp.where(even, peer_log_f, log_f))
    late_b = jnp.exp(jnp.where(even, log_b, peer_log_b))
    msg[0, pl.ds(0, hd), :] = (
        late_f * jnp.where(even, mine_f, theirs_f) + jnp.where(even, theirs_f, mine_f)
    ).astype(bf16)
    msg[1, pl.ds(0, hd), :] = (
        late_b * jnp.where(even, theirs_b, mine_b) + jnp.where(even, mine_b, theirs_b)
    ).astype(bf16)
    msg[0, pl.ds(hd, RIM), :] = packed(log_f + peer_log_f)
    msg[1, pl.ds(hd, RIM), :] = packed(log_b + peer_log_b)
    for d in range(1, planes):
        state_copy(d).start()
    pump(PUMPS[1])

    def join(source, state):
        state_landed(source).wait_recv()
        tail = inbox[source, pl.ds(hd, RIM), :].astype(f32)
        log = tail[0:1, :] + tail[1:2, :]
        return jnp.exp(log) * state + inbox[source, pl.ds(0, hd), :].astype(f32)

    entry[0] = start[0].T
    entry[1] = start[1].T
    plane_f = lax.fori_loop(0, plane, join, entry[0, my_half, :])
    plane_b = lax.fori_loop(
        0, planes - 1 - plane, lambda i, st: join(planes - 1 - i, st), entry[1, my_half, :]
    )
    after_mine_f = jnp.exp(log_f) * plane_f + mine_f
    after_theirs_f = jnp.exp(peer_log_f) * plane_f + theirs_f
    after_mine_b = jnp.exp(log_b) * plane_b + mine_b
    after_theirs_b = jnp.exp(peer_log_b) * plane_b + theirs_b
    back_out[pl.ds(0, hd), :] = jnp.where(even, after_mine_f, plane_f).astype(bf16)
    back_out[pl.ds(hd, hd), :] = jnp.where(even, plane_b, after_mine_b).astype(bf16)
    pair_copy(1).start()
    entry[0, my_half, :] = jnp.where(even, plane_f, after_theirs_f)
    entry[1, my_half, :] = jnp.where(even, after_theirs_b, plane_b)

    pump_to((QP, half, CHUNKS // 2 - 1))
    pbuf[pl.ds(RIM, seq), :] = nn(normed[...], wqp[:, qc:]).astype(bf16)

    def halo(side):
        src = pl.ds(seq, RIM) if side == 0 else pl.ds(RIM, RIM)
        dst = pl.ds(0, RIM) if side == 0 else pl.ds(RIM + seq, RIM)
        peer = jnp.minimum(me + 1, n - 1) if side == 0 else jnp.maximum(me - 1, 0)
        return pltpu.make_async_remote_copy(
            src_ref=pbuf.at[src],
            dst_ref=pbuf.at[dst],
            send_sem=halo_send.at[side],
            recv_sem=halo_recv.at[side],
            device_id={"sp": peer},
            device_id_type=MESH,
        )

    @pl.when(me < n - 1)
    def _():
        halo(0).start()

    @pl.when(me > 0)
    def _():
        halo(1).start()

    @pl.when(me == 0)
    def _():
        pbuf[pl.ds(0, RIM), :] = jnp.zeros((RIM, pc), bf16)

    @pl.when(me == n - 1)
    def _():
        pbuf[pl.ds(RIM + seq, RIM), :] = jnp.zeros((RIM, pc), bf16)

    query = nn(normed[...], wqp[:, :qc]).astype(bf16)
    pump(1)
    pair_copy(1).wait_recv()
    entry[0, other_half, :] = back_in[pl.ds(0, hd), :].astype(f32)
    entry[1, other_half, :] = back_in[pl.ds(hd, hd), :].astype(f32)
    state_f, state_b = entry[0], entry[1]
    for b in reversed(range(blocks)):
        before_b[b] = state_b
        state_b = jnp.exp(edges[b : b + 1, qc:]) * state_b + upd[b, :, qc:]
    for b in range(blocks):
        at = pl.ds(b * BLOCK, BLOCK)
        q = query[b * BLOCK : (b + 1) * BLOCK].astype(f32) * KEY_CHANNELS ** (-0.5)
        qf = (q * jnp.exp(ld[at, :qc])).astype(bf16)
        qb = (q * jnp.exp(ld[at, qc:])).astype(bf16)
        kf = kbuf[at, :qc].astype(f32)
        kb = kbuf[at, qc:].astype(f32)
        scores_f = nt(qf, jnp.concatenate([kf * k0, kf * k1], axis=0).astype(bf16))
        scores_b = nt(qb, jnp.concatenate([kb * k0, kb * k1], axis=0).astype(bf16))
        scores = jnp.where(allowed, scores_f, scores_b).astype(bf16)
        vf = kv[at, qc:].astype(f32)
        both = jnp.concatenate([vf * v0, vf * v1], axis=0).astype(bf16)
        back = before_b[b]
        memory = jnp.concatenate(
            [
                jnp.concatenate([state_f * k0, back * k0], axis=1),
                jnp.concatenate([state_f * k1, back * k1], axis=1),
            ],
            axis=0,
        ).astype(bf16)
        joined = nn(scores, both) + nt(jnp.concatenate([qf, qb], axis=1), memory)
        for h in range(vc // DV):
            o = joined[:, h * DV : (h + 1) * DV]
            scale = lax.rsqrt(jnp.mean(o * o, axis=-1, keepdims=True) + eps_value)
            act[at, pc + h * DV : pc + (h + 1) * DV] = (o * scale).astype(bf16)
        if b + 1 < blocks:
            state_f = jnp.exp(edges[b : b + 1, :qc]) * state_f + upd[b, :, :qc]
        if b % 4 == 3:
            pump(1)

    @pl.when(me > 0)
    def _():
        halo(0).wait_recv()

    @pl.when(me < n - 1)
    def _():
        halo(1).wait_recv()

    window = jnp.left_shift(jnp.int32(2), tp)
    half_width = window // 2
    tile = 2 * BLOCK
    offset = (
        lax.broadcasted_iota(jnp.int32, (tile, tile + 2 * RIM), 1)
        - RIM
        - lax.broadcasted_iota(jnp.int32, (tile, tile + 2 * RIM), 0)
    )
    band = ((offset >= -half_width) & (offset < window - half_width)).astype(f32).astype(bf16)
    seq_length = seq * n
    for b in range(seq // tile):
        sums = nn(band, pbuf[pl.ds(b * tile, tile + 2 * RIM), :])
        position = me * seq + b * tile + lax.broadcasted_iota(jnp.int32, (tile, 1), 0)
        low_end = jnp.clip(position - half_width, 0, seq_length - 1)
        high_end = jnp.clip(position - half_width + window - 1, 0, seq_length - 1)
        counted = (high_end - low_end + 1).astype(f32)
        pooled = (sums / counted - pbuf[pl.ds(RIM + b * tile, tile), :].astype(f32)).astype(bf16)
        act[pl.ds(b * tile, tile), :pc] = nn(pooled, gmap[...]).astype(bf16)

    units = [(0, None)]
    for k in range(1, half - 1):
        units += [(-k, None), (k, None)]
    units += [(1 - half, 0), (half - 1, 1), (1 - half, 1), (half - 1, 0), (half, 0), (half, 1)]
    direct = len(units) - 2

    def lanes(i):
        return pl.ds(0, ocols if units[i][1] is None else hcols)

    def rows_of(dest):
        return pl.ds(pl.multiple_of(dest * m, m), m)

    def sib_copy(i, part):
        at = (i, pl.ds(part * m, m), lanes(i))
        return pltpu.make_async_remote_copy(
            src_ref=sib_out.at[at],
            dst_ref=sib_in.at[at],
            send_sem=sib_send.at[i, part],
            recv_sem=sib_recv.at[i, part],
            device_id={"tp": sibling},
            device_id_type=MESH,
        )

    def x_copy(i):
        at = (i, slice(None), lanes(i))
        return pltpu.make_async_remote_copy(
            src_ref=x_out.at[at],
            dst_ref=x_in.at[at],
            send_sem=x_send.at[i],
            recv_sem=x_recv.at[i],
            device_id={"tp": across},
            device_id_type=MESH,
        )

    def direct_copy():
        return pltpu.make_async_remote_copy(
            src_ref=d_out,
            dst_ref=d_in,
            send_sem=d_send.at[0],
            recv_sem=d_recv.at[0],
            device_id={"tp": across_sibling},
            device_id_type=MESH,
        )

    def weights_of(i):
        offset, side = units[i]
        source = origins[offset]
        if side is None:
            return jnp.concatenate([obuf[source, 0], obuf[source, 1]], axis=1)
        return obuf[source, side]

    def produce_far(i):
        weights = weights_of(i)
        far = nn(act[rows_of(across_sibling), :], weights).astype(bf16)
        if i == direct:
            d_out[...] = far
            direct_copy().start()
            x_out[i, :, lanes(i)] = nn(act[rows_of(across), :], weights).astype(bf16)
            x_copy(i).start()
        else:
            sib_out[i, pl.ds(0, m), lanes(i)] = far
            sib_copy(i, 0).start()
            x_part[i, :, lanes(i)] = nn(act[rows_of(across), :], weights)

    def produce_near(i):
        weights = weights_of(i)
        sib_out[i, pl.ds(m, m), lanes(i)] = nn(act[rows_of(sibling), :], weights).astype(bf16)
        sib_copy(i, 1).start()
        own[i, :, lanes(i)] = nn(act[rows_of(tp), :], weights)

    def produce(i):
        produce_far(i)
        produce_near(i)

    def cross(i):
        sib_copy(i, 0).wait_recv()
        x_out[i, :, lanes(i)] = (
            x_part[i, :, lanes(i)] + sib_in[i, pl.ds(0, m), lanes(i)].astype(f32)
        ).astype(bf16)
        x_copy(i).start()

    def finish(i):
        offset, side = units[i]
        sib_copy(i, 1).wait_recv()
        x_copy(i).wait_recv()
        summed = (
            own[i, :, lanes(i)]
            + sib_in[i, pl.ds(m, m), lanes(i)].astype(f32)
            + x_in[i, :, lanes(i)].astype(f32)
        )
        if i == direct:
            direct_copy().wait_recv()
            summed = summed + d_in[...].astype(f32)
        begin = origins[offset] * ocols + (side or 0) * hcols
        width = ocols if side is None else hcols
        result[:, pl.ds(pl.multiple_of(begin, width), width)] = summed.astype(bf16)

    def send_waits():
        token_copy(0).wait_send()
        for c in range(TOK_CHUNKS):
            token_copy(1, c).wait_send()
            token_copy(2, c).wait_send()
        for group in range(2):
            for d in range(2):
                for c in range(CHUNKS):
                    for s in range(hops_of(d, c)):
                        ring_copy(group, d, c, s, False).wait_send()

        @pl.when(me < n - 1)
        def _():
            halo(0).wait_send()

        @pl.when(me > 0)
        def _():
            halo(1).wait_send()

        for i in range(2):
            pair_copy(i).wait_send()
        for d in range(1, planes):
            state_copy(d).wait_send()

    last = len(units)
    whole = last - 6
    pump(1)
    produce(0)
    for s in range(1, half - 1):
        pump_to((OUT, s, CHUNKS - 1))
        produce(2 * s - 1)
        cross(2 * s - 2)
        if s == 1:
            pump(1)
        produce(2 * s)
        cross(2 * s - 1)
    pump_to((OUT, half - 1, CHUNKS // 2 - 1))
    cross(whole - 1)
    produce(whole)
    produce(whole + 1)
    for i in range(whole - 1):
        finish(i)
    cross(whole)
    cross(whole + 1)
    pump_to((OUT, half - 1, CHUNKS - 1))
    produce(whole + 2)
    produce(whole + 3)
    send_waits()
    finish(whole - 1)
    cross(whole + 2)
    cross(whole + 3)
    pump(len(order))
    produce_far(direct + 1)
    produce_far(direct)
    produce_near(direct + 1)
    produce_near(direct)
    cross(direct + 1)
    finish(whole)
    finish(whole + 1)
    for i in range(whole + 2, last):
        finish(i)

    for d in range(2):
        for c in range(CHUNKS):
            for s in range(hops_of(d, c)):
                ring_copy(OUT, d, c, s, False).wait_send()
    for i in range(last):
        if i == direct:
            direct_copy().wait_send()
        else:
            sib_copy(i, 0).wait_send()
        sib_copy(i, 1).wait_send()
        x_copy(i).wait_send()


def event_order(half):
    lead, rest = range(CHUNKS // 2), range(CHUNKS // 2, CHUNKS)
    events = []
    for group in (KV, QP, OUT):
        waits = events[-CHUNKS:] if events else []
        events = events[: len(events) - len(waits)]
        events += [(group, 0, i) for i in range(CHUNKS)] + waits
        for s in range(1, half - 1):
            events += [(group, s, i) for i in range(CHUNKS)]
        events += [(group, half - 1, i) for i in lead]
        events += [(group, half - 1, i) for i in rest] + [(group, half, i) for i in lead]
    return events


def one_kernel(
    n,
    tps,
    tokens,
    pooling_input_weight,
    query_matrix,
    key_matrix,
    value_matrix,
    decay_inner_weight,
    decay_outer_weight,
    channel_decay_bias,
    spike_log_decay,
    starting_state,
    pooling_group_map,
    pooling_output_weight,
    attention_output_weight,
):
    m, width = tokens.shape
    seq = m * tps
    pc, qc, vc = (a.shape[1] for a in (pooling_input_weight, query_matrix, value_matrix))
    ocols = pooling_output_weight.shape[1]
    blocks = seq // BLOCK
    units = n + 3
    f32, bf16 = jnp.float32, jnp.bfloat16
    vmem = pl.BlockSpec(memory_space=pltpu.VMEM)
    hbm = pl.BlockSpec(memory_space=pl.ANY)
    dma = pltpu.SemaphoreType.DMA
    return pl.pallas_call(
        functools.partial(fused, n),
        out_shape=pltpu.VMEM((m, n * ocols), bf16),
        in_specs=[hbm] * 13,
        out_specs=vmem,
        scratch_shapes=[
            pltpu.VMEM((decay_inner_weight.shape[1], width), bf16),
            pltpu.VMEM((2, RANK, decay_outer_weight.shape[2]), bf16),
            pltpu.VMEM(channel_decay_bias.shape, f32),
            pltpu.VMEM(spike_log_decay.shape, f32),
            pltpu.VMEM((2, qc, DV), f32),
            pltpu.VMEM((seq, width), bf16),
            pltpu.VMEM((seq, width), bf16),
            pltpu.VMEM((width, qc + vc), bf16),
            pltpu.VMEM((width, qc + pc), bf16),
            pltpu.VMEM((n, 2, pc + vc, ocols // 2), bf16),
            pltpu.VMEM((seq + 2 * RIM, pc), bf16),
            pltpu.VMEM((seq, qc + vc), bf16),
            pltpu.VMEM((seq, 2 * qc), f32),
            pltpu.VMEM((seq, 2 * qc), bf16),
            pltpu.VMEM((blocks, DV, 2 * qc), f32),
            pltpu.VMEM((blocks, 2 * qc), f32),
            pltpu.VMEM((blocks, DV, qc), f32),
            pltpu.VMEM((seq, pc + vc), bf16),
            pltpu.VMEM((2, DV, qc), f32),
            pltpu.VMEM((DV + RIM, qc), bf16),
            pltpu.VMEM((DV + RIM, qc), bf16),
            pltpu.VMEM((2, DV // 2 + RIM, qc), bf16),
            pltpu.VMEM((n // 2, DV // 2 + RIM, qc), bf16),
            pltpu.VMEM((DV, qc), bf16),
            pltpu.VMEM((DV, qc), bf16),
            pltpu.VMEM((2, DV, qc), f32),
            pltpu.VMEM((pc, pc), bf16),
            pltpu.VMEM((units, 2 * m, ocols), bf16),
            pltpu.VMEM((units, 2 * m, ocols), bf16),
            pltpu.VMEM((units, m, ocols), f32),
            pltpu.VMEM((units, m, ocols), bf16),
            pltpu.VMEM((units, m, ocols), bf16),
            pltpu.VMEM((units, m, ocols), f32),
            pltpu.VMEM((m, ocols // 2), bf16),
            pltpu.VMEM((m, ocols // 2), bf16),
            dma((15,)),
            dma((1 + 2 * TOK_CHUNKS,)),
            dma((1 + 2 * TOK_CHUNKS,)),
            dma((3, 2, CHUNKS, n // 2)),
            dma((3, 2, CHUNKS, n // 2)),
            dma((2,)),
            dma((2,)),
            dma((2,)),
            dma((2,)),
            dma((n // 2 - 1,)),
            dma((n // 2 - 1,)),
            dma((units, 2)),
            dma((units, 2)),
            dma((units,)),
            dma((units,)),
            dma((1,)),
            dma((1,)),
        ],
        compiler_params=pltpu.CompilerParams(
            collective_id=0, has_side_effects=True, vmem_limit_bytes=60 * 2**20,
        ),
    )(
        tokens,
        pooling_input_weight,
        query_matrix,
        key_matrix,
        value_matrix,
        decay_inner_weight.T,
        decay_outer_weight,
        channel_decay_bias,
        spike_log_decay,
        starting_state.reshape(2, qc, DV),
        pooling_group_map,
        pooling_output_weight,
        attention_output_weight,
    )


def solution(mesh):
    in_specs = (
        P(("sp", "tp"), None),
        P("sp", "tp"),
        P("sp", "tp"),
        P("sp", "tp"),
        P("sp", "tp"),
        P(),
        P(),
        P(),
        P("tp", "sp"),
        P(None, "tp", None, None),
        P(),
        P("tp", "sp"),
        P("tp", "sp"),
    )
    out_specs = P(("sp", "tp"), None)
    n, tps = mesh.shape["sp"], mesh.shape["tp"]
    fits = n % 4 == 0 and n <= 16 and tps == 4
    local = functools.partial(one_kernel, n, tps) if fits else shards
    return jax.shard_map(local, mesh=mesh, in_specs=in_specs, out_specs=out_specs, check_vma=False)
```
